32 devices in a mesh: sp: 4 (over z), fs: 4 (over y, x), tp: 2 (over core).
Axes of the slice: x: 2, y: 2, z: 4, core: 2. Of those that a mesh axis runs over, the one named last changes fastest.
Arguments:
- tokens: bfloat16 [2048, 2048], P(('fs', 'sp')), parts along dimension 0, may hold values from -6 to 6
- norm_gain: bfloat16 [2048], replicated, may hold values from 0.099609375 to 1.8984375
- query_down: bfloat16 [2048, 512], P('sp'), may hold values from -0.125 to 0.125
- query_gain: bfloat16 [512], replicated, may hold values from 0.099609375 to 1.8984375
- latent_down: bfloat16 [2048, 256], replicated, may hold values from -0.125 to 0.125
- latent_gain: bfloat16 [256], replicated, may hold values from 0.099609375 to 1.8984375
- rope_down: bfloat16 [2048, 64], replicated, may hold values from -30 to 30
- query_up: bfloat16 [512, 1536], P(None, 'tp'), may hold values from -0.25 to 0.25
- key_up: bfloat16 [256, 1024], P(None, 'tp'), may hold values from -0.75 to 0.75
- value_up: bfloat16 [256, 1024], P(None, 'tp'), may hold values from -0.375 to 0.375
- glu_value: bfloat16 [2048, 1024], P('sp', 'tp'), may hold values from -0.125 to 0.125
- glu_gate: bfloat16 [2048, 1024], P('sp', 'tp'), may hold values from -0.125 to 0.125
- conv_taps: bfloat16 [31, 1024], P(None, 'tp'), may hold values from -1 to 1
- group_gain: bfloat16 [1024], P('tp'), may hold values from 0.099609375 to 1.8984375
- head_proj: bfloat16 [1024, 2048], P('tp', 'sp'), may hold values from -0.75 to 0.75
- channel_proj: bfloat16 [1024, 2048], P('tp', 'sp'), may hold values from -0.1875 to 0.1875
Outputs:
- mixed_out: bfloat16 [2048, 2048], P(('fs', 'sp'), 'tp'), parts along dimension 0
- log_weight: float32 [8, 2048], P('tp', ('fs', 'sp')), parts along dimension 1
The draws below stay inside these ranges and needn't reach their ends.
There are 4 independent parts, one for each index of `fs`. The reference program is written for one: setup_inputs(seed, part) draws one part's arguments, and reference() takes and returns one part's arrays. A program takes and returns all parts, laid end to end along the dimension named above; an argument that names none is the same for every part. Nothing has to cross between parts.
All inputs are finite; a program needn't handle non-finite values.
Results may differ from the reference program's by a relative error of at most 0.015.
The reference program's roundings to bfloat16 on the way count: a program that leaves them out, or rounds other values in their place, can miss the bound.
Values may be sent and summed in bfloat16 or wider, within the bound.
A program may use at most 128 MiB of HBM per device.

```python
import jax
import jax.numpy as jnp
from jax import lax

D = 2048
HEADS = 8
NOPE = 128
ROPE = 64
VDIM = 128
QR = 512
KVR = 256
CH = 1024
GROUPS = 8
WIDTH = 31
GRID_W = 64
TOK_DEV = 128
LENGTH = 512
N_TP = 2


def draw_rope_down(key, part):
    base_key = jax.random.fold_in(jax.random.fold_in(key, 11), 0)
    entries = jax.random.normal(base_key, (D, ROPE), jnp.float32) * D ** (-0.5)
    return jnp.clip(entries, -30.0, 30.0).astype(jnp.bfloat16)


def steps_of(key, extent, cuts, least, high):
    factor_of, own = 1.0, jax.random.fold_in(key, 6)
    for position, blocks in cuts:
        steps = jnp.exp(jax.random.uniform(jax.random.fold_in(own, position), (blocks,), jnp.float32, least / len(cuts), high / len(cuts)))
        factor_of = factor_of * jnp.repeat(steps, extent[position] // blocks).reshape([-1 if axis == position else 1 for axis in range(len(extent))])
    return factor_of


def bell_draw(stream_key, extent, width, bound, cuts=(), held_as=jnp.bfloat16):
    loudness = steps_of(stream_key, extent, cuts, -0.22, 0.18) if cuts else 1.0
    drawn = jax.random.normal(stream_key, extent, jnp.float32) * width * loudness
    return jnp.minimum(jnp.maximum(drawn, -bound), bound).astype(held_as)


def setup_inputs(seed: int = 0, part: int = 0) -> dict:
    arg_keys = jax.random.split(jax.random.key(seed), 17)
    part_splits = jax.random.split(jax.random.fold_in(arg_keys[16], part), 17)
    tokens = bell_draw(part_splits[0], (LENGTH, D), 1.0, 6.0, ((0, 4),))
    norm_gain = jnp.clip(1.0 + 0.18 * jax.random.normal(arg_keys[1], (D,), jnp.float32), 0.099609375, 1.8984375).astype(jnp.bfloat16)
    query_down = bell_draw(arg_keys[2], (D, QR), D ** -0.5, 0.125, ((0, 4),))
    query_gain = jnp.clip(1.0 + 0.18 * jax.random.normal(arg_keys[3], (QR,), jnp.float32), 0.099609375, 1.8984375).astype(jnp.bfloat16)
    latent_down = bell_draw(arg_keys[4], (D, KVR), D ** -0.5, 0.125)
    latent_gain = jnp.clip(1.0 + 0.18 * jax.random.normal(arg_keys[5], (KVR,), jnp.float32), 0.099609375, 1.8984375).astype(jnp.bfloat16)
    rope_down = draw_rope_down(jax.random.fold_in(arg_keys[16], 71), part)
    query_up = bell_draw(arg_keys[7], (QR, HEADS * (NOPE + ROPE)), QR ** -0.5, 0.25, ((1, 2),))
    key_up = bell_draw(arg_keys[8], (KVR, HEADS * NOPE), 0.125, 0.75, ((1, 2),))
    value_up = bell_draw(arg_keys[9], (KVR, HEADS * VDIM), KVR ** -0.5, 0.375, ((1, 2),))
    glu_value = bell_draw(arg_keys[10], (D, CH), D ** -0.5, 0.125, ((0, 4), (1, 2)))
    glu_gate = bell_draw(arg_keys[11], (D, CH), D ** -0.5, 0.125, ((0, 4), (1, 2)))
    conv_taps = bell_draw(arg_keys[12], (WIDTH, CH), WIDTH ** -0.5, 1.0, ((1, 2),))
    group_gain = jnp.clip(1.0 + 0.18 * jax.random.normal(arg_keys[13], (CH,), jnp.float32), 0.099609375, 1.8984375).astype(jnp.bfloat16)
    head_proj = bell_draw(arg_keys[14], (HEADS * VDIM, D), (HEADS * VDIM // 16) ** -0.5, 0.75, ((0, 2), (1, 4)))
    channel_proj = bell_draw(arg_keys[15], (CH, D), CH ** -0.5, 0.1875, ((0, 2), (1, 4)))
    return {"tokens": tokens, "norm_gain": norm_gain, "query_down": query_down, "query_gain": query_gain, "latent_down": latent_down, "latent_gain": latent_gain, "rope_down": rope_down, "query_up": query_up, "key_up": key_up, "value_up": value_up, "glu_value": glu_value, "glu_gate": glu_gate, "conv_taps": conv_taps, "group_gain": group_gain, "head_proj": head_proj, "channel_proj": channel_proj}


norm_eps = 1e-06
rope_base = 10000.0

def rounded(values):
    return lax.optimization_barrier(values.astype(jnp.bfloat16))

def rms_scale(values, scale_gain):
    inv_rms = lax.rsqrt(lax.optimization_barrier(jnp.mean(values * values, axis=-1, keepdims=True)) + norm_eps)
    return values * inv_rms * scale_gain.astype(jnp.float32)

def angles_for(positions, rope_size):
    quarter = rope_size // 4
    inverse = rope_base ** (-jnp.arange(quarter, dtype=jnp.float32) / quarter)
    grid_row = (positions // GRID_W).astype(jnp.float32)
    grid_col = (positions % GRID_W).astype(jnp.float32)
    return jnp.concatenate([grid_row[:, None] * inverse, grid_col[:, None] * inverse], axis=-1)

def rotate(values, angles):
    half_size = values.shape[-1] // 2
    front_half = values[..., :half_size]
    back_half = values[..., half_size:]
    cosine = jnp.cos(angles)
    sine_part = jnp.sin(angles)
    return jnp.concatenate([front_half * cosine - back_half * sine_part, back_half * cosine + front_half * sine_part], axis=-1)

def reference(tokens, norm_gain, query_down, query_gain, latent_down, latent_gain, rope_down, query_up, key_up, value_up, glu_value, glu_gate, conv_taps, group_gain, head_proj, channel_proj):
    normed = rounded(rms_scale(tokens.astype(jnp.float32), norm_gain))
    positions = jnp.arange(LENGTH, dtype=jnp.int32)
    angles = angles_for(positions, ROPE)
    latent_query = rounded(rms_scale(jnp.dot(normed, query_down, preferred_element_type=jnp.float32), query_gain))
    query_all = jnp.dot(latent_query, query_up, preferred_element_type=jnp.float32).reshape(LENGTH, HEADS, NOPE + ROPE)
    query_plain = rounded(query_all[:, :, :NOPE])
    query_rope = rounded(rotate(query_all[:, :, NOPE:], angles[:, None, :]))
    absorbed = rounded(jnp.einsum('thd,rhd->htr', query_plain.astype(jnp.float32), key_up.astype(jnp.float32).reshape(KVR, HEADS, NOPE)))
    queries = jnp.concatenate([absorbed, jnp.transpose(query_rope, (1, 0, 2))], axis=-1).astype(jnp.float32)
    latent = rounded(rms_scale(jnp.dot(normed, latent_down, preferred_element_type=jnp.float32), latent_gain))
    rope_key = rounded(rotate(jnp.dot(normed, rope_down, preferred_element_type=jnp.float32), angles))
    keys = jnp.concatenate([latent, rope_key], axis=1).astype(jnp.float32)
    latent_wide = latent.astype(jnp.float32)
    score_scale = (NOPE + ROPE) ** (-0.5)
    block_count = LENGTH // TOK_DEV
    query_blocks = jnp.transpose(queries.reshape(HEADS, block_count, TOK_DEV, KVR + ROPE), (1, 0, 2, 3))

    def attend_block(query_block):
        scores = jnp.einsum('hqc,kc->hqk', query_block, keys) * score_scale
        row_max = lax.optimization_barrier(jnp.max(scores, axis=-1))
        weights = jnp.exp(scores - row_max[:, :, None])
        row_sum = lax.optimization_barrier(jnp.sum(weights, axis=-1))
        summed = jnp.einsum('hqk,kr->hqr', rounded(weights).astype(jnp.float32), latent_wide)
        return (rounded(summed / row_sum[:, :, None]), row_max + jnp.log(row_sum))
    attended, log_blocks = lax.map(attend_block, query_blocks)
    attended = jnp.transpose(attended, (1, 0, 2, 3)).reshape(HEADS, LENGTH, KVR)
    log_weight = jnp.transpose(log_blocks, (1, 0, 2)).reshape(HEADS, LENGTH)
    head_out = jnp.einsum('htr,rhv->thv', attended.astype(jnp.float32), value_up.astype(jnp.float32).reshape(KVR, HEADS, VDIM))
    head_out = rounded(head_out.reshape(LENGTH, HEADS * VDIM))
    value_in = jnp.dot(normed, glu_value, preferred_element_type=jnp.float32)
    gate_in = jnp.dot(normed, glu_gate, preferred_element_type=jnp.float32)
    gated_rows = rounded(value_in * jax.nn.sigmoid(gate_in))
    reach_rows = WIDTH // 2
    padded = jnp.pad(gated_rows.astype(jnp.float32), ((reach_rows, reach_rows), (0, 0)))
    filtered = padded[0:LENGTH] * conv_taps[0].astype(jnp.float32)
    for tap_index in range(1, WIDTH):
        filtered = filtered + padded[tap_index:tap_index + LENGTH] * conv_taps[tap_index].astype(jnp.float32)
    grouped = filtered.reshape(LENGTH, GROUPS, CH // GROUPS)
    centred = grouped - lax.optimization_barrier(jnp.mean(grouped, axis=-1, keepdims=True))
    spread = lax.optimization_barrier(jnp.mean(centred * centred, axis=-1, keepdims=True))
    normal_groups = (centred * lax.rsqrt(spread + norm_eps)).reshape(LENGTH, CH)
    conv_branch = rounded(jax.nn.silu(normal_groups * group_gain.astype(jnp.float32)))
    head_part = HEADS * VDIM // N_TP
    channel_part = CH // N_TP
    mixed_total = jnp.zeros((LENGTH, D), jnp.float32)
    for group_index in range(N_TP):
        head_lo = group_index * head_part
        chan_lo = group_index * channel_part
        partial_value = jnp.dot(head_out[:, head_lo:head_lo + head_part], head_proj[head_lo:head_lo + head_part], preferred_element_type=jnp.float32)
        partial_value = partial_value + jnp.dot(conv_branch[:, chan_lo:chan_lo + channel_part], channel_proj[chan_lo:chan_lo + channel_part], preferred_element_type=jnp.float32)
        mixed_total = mixed_total + rounded(partial_value).astype(jnp.float32)
    return (mixed_total.astype(jnp.bfloat16), log_weight)
```

```python
import functools

import jax
import jax.numpy as jnp
import numpy as np
from jax import lax
from jax.experimental import pallas as pl
from jax.experimental.pallas import tpu as pltpu
from jax.sharding import PartitionSpec as P

NOPE = 128
ROPE = 64
VDIM = 128
KVR = 256
CH = 1024
GROUPS = 8
GRID_W = 64


norm_eps = 1e-06
rope_base = 10000.0
far_below = -1e30


def padded_2(block, sides, width):
    for axis, dim in sides:
        count = lax.axis_size(axis)
        forward = [(i, i + 1) for i in range(count - 1)]
        backward = [(target, source) for source, target in forward]
        low = lax.ppermute(
            lax.slice_in_dim(block, block.shape[dim] - width, None, axis=dim), axis, forward
        )
        high = lax.ppermute(lax.slice_in_dim(block, 0, width, axis=dim), axis, backward)
        block = jnp.concatenate([low, block, high], axis=dim)
    return block


def rms_scale(values, scale_gain):
    inv_rms = lax.rsqrt(jnp.mean(values * values, axis=-1, keepdims=True) + norm_eps)
    return values * inv_rms * scale_gain.astype(jnp.float32)


def angles_for(positions, rope_size):
    quarter = rope_size // 4
    inverse = rope_base ** (-jnp.arange(quarter, dtype=jnp.float32) / quarter)
    grid_row = (positions // GRID_W).astype(jnp.float32)
    grid_col = (positions % GRID_W).astype(jnp.float32)
    return jnp.concatenate([grid_row[:, None] * inverse, grid_col[:, None] * inverse], axis=-1)


def rotate(values, angles):
    half_size = values.shape[-1] // 2
    front_half = values[..., :half_size]
    back_half = values[..., half_size:]
    cosine = jnp.cos(angles)
    sine_part = jnp.sin(angles)
    return jnp.concatenate(
        [front_half * cosine - back_half * sine_part, back_half * cosine + front_half * sine_part],
        axis=-1,
    )


def key_block(normed, latent_down, latent_gain, rope_down, positions):
    latent = jnp.dot(normed, latent_down, preferred_element_type=jnp.float32)
    latent = rms_scale(latent, latent_gain).astype(jnp.bfloat16)
    rope_key = jnp.dot(normed, rope_down, preferred_element_type=jnp.float32)
    rope_key = rotate(rope_key, angles_for(positions, rope_key.shape[-1])).astype(jnp.bfloat16)
    return jnp.concatenate([latent, rope_key], axis=1)


def per_device(
    tokens,
    norm_gain,
    query_down,
    query_gain,
    latent_down,
    latent_gain,
    rope_down,
    query_up,
    key_up,
    value_up,
    glu_value,
    glu_gate,
    conv_taps,
    group_gain,
    head_proj,
    channel_proj,
):
    tok_count = tokens.shape[0]
    reach_rows = conv_taps.shape[0] // 2
    head_count = key_up.shape[1] // NOPE
    normed = rms_scale(tokens.astype(jnp.float32), norm_gain).astype(jnp.bfloat16)
    offsets = lax.axis_index("sp") * tok_count + jnp.arange(tok_count, dtype=jnp.int32)
    query_latent = jnp.dot(
        normed,
        lax.all_gather(query_down, "sp", axis=0, tiled=True),
        preferred_element_type=jnp.float32,
    )
    value_in = jnp.dot(
        normed,
        lax.all_gather(glu_value, "sp", axis=0, tiled=True),
        preferred_element_type=jnp.float32,
    )
    gate_in = jnp.dot(
        normed,
        lax.all_gather(glu_gate, "sp", axis=0, tiled=True),
        preferred_element_type=jnp.float32,
    )
    latent_query = rms_scale(query_latent, query_gain).astype(jnp.bfloat16)
    query_all = jnp.dot(latent_query, query_up, preferred_element_type=jnp.float32).reshape(
        tok_count, head_count, NOPE + ROPE
    )
    query_plain = query_all[:, :, :NOPE].astype(jnp.bfloat16)
    query_rope = rotate(query_all[:, :, NOPE:], angles_for(offsets, ROPE)[:, None, :]).astype(
        jnp.bfloat16
    )
    absorbed = jnp.einsum(
        "thd,rhd->htr",
        query_plain,
        key_up.reshape(KVR, head_count, NOPE),
        preferred_element_type=jnp.float32,
    ).astype(jnp.bfloat16)
    queries = jnp.concatenate([absorbed, jnp.transpose(query_rope, (1, 0, 2))], axis=-1)
    score_scale = (NOPE + ROPE) ** (-0.5)
    half_rows = tok_count // lax.axis_size("tp")
    first_row = lax.axis_index("tp") * half_rows
    own_rows = lax.dynamic_slice_in_dim(normed, first_row, half_rows, 0)
    own_positions = lax.dynamic_slice_in_dim(offsets, first_row, half_rows, 0)
    own_keys = key_block(own_rows, latent_down, latent_gain, rope_down, own_positions)
    block_keys = lax.all_gather(own_keys, ("sp", "tp"), axis=0, tiled=True)
    row_max = jnp.full((head_count, tok_count), far_below, jnp.float32)
    scores = (
        jnp.einsum("hqc,kc->hqk", queries, block_keys, preferred_element_type=jnp.float32)
        * score_scale
    )
    new_max = jnp.maximum(row_max, jnp.max(scores, axis=2))
    weights = jnp.exp(scores - new_max[:, :, None])
    new_sum = jnp.sum(weights, axis=2)
    added = jnp.einsum(
        "hqk,kr->hqr",
        weights.astype(jnp.bfloat16),
        block_keys[:, :KVR],
        preferred_element_type=jnp.float32,
    )
    gated_rows = (value_in * jax.nn.sigmoid(gate_in)).astype(jnp.bfloat16)
    padded = padded_2(gated_rows, (("sp", 0),), reach_rows)
    filtered = padded[0:tok_count].astype(jnp.float32) * conv_taps[0].astype(jnp.float32)
    for tap_index in range(1, conv_taps.shape[0]):
        filtered = filtered + padded[tap_index : tap_index + tok_count].astype(
            jnp.float32
        ) * conv_taps[tap_index].astype(jnp.float32)
    grouped = filtered.reshape(tok_count, -1, CH // GROUPS)
    centred = grouped - jnp.mean(grouped, axis=-1, keepdims=True)
    spread = jnp.mean(centred * centred, axis=-1, keepdims=True)
    normal_groups = (centred * lax.rsqrt(spread + norm_eps)).reshape(tok_count, -1)
    conv_branch = jax.nn.silu(normal_groups * group_gain.astype(jnp.float32)).astype(jnp.bfloat16)
    attended = (added / new_sum[:, :, None]).astype(jnp.bfloat16)
    log_weight = new_max + jnp.log(new_sum)
    head_out = jnp.einsum(
        "htr,rhv->thv",
        attended,
        value_up.reshape(KVR, head_count, VDIM),
        preferred_element_type=jnp.float32,
    )
    head_out = head_out.reshape(tok_count, head_count * VDIM).astype(jnp.bfloat16)
    mixed_in = jnp.concatenate([head_out, conv_branch], axis=1)
    out_weight = jnp.concatenate([head_proj, channel_proj], axis=0)
    partial_terms = jnp.dot(
        mixed_in,
        lax.all_gather(out_weight, "sp", axis=1, tiled=True),
        preferred_element_type=jnp.float32,
    )
    mixed_out = lax.psum_scatter(
        partial_terms.astype(jnp.bfloat16), "tp", scatter_dimension=1, tiled=True
    )
    return (mixed_out, log_weight)


LANES = 128
MESH = pl.DeviceIdType.MESH
F32 = jnp.float32
BF16 = jnp.bfloat16
LOW, HIGH, FWD = range(3)
Q, K, V, W, H, C = range(6)


def rope_tables(length):
    quarter = ROPE // 4
    inverse = np.float32(rope_base) ** (-np.arange(quarter, dtype=np.float32) / np.float32(quarter))
    positions = np.arange(length)
    row = (positions // GRID_W).astype(np.float32)[:, None] * inverse
    col = (positions % GRID_W).astype(np.float32)[:, None] * inverse
    angles = np.concatenate([row, col], axis=1).astype(np.float32)
    cosine, sine = np.cos(angles), np.sin(angles)
    tables = np.zeros((3, length, LANES), np.float32)
    half = ROPE // 2
    tables[0, :, :half] = cosine
    tables[0, :, half:ROPE] = cosine
    tables[1, :, :half] = -sine
    tables[2, :, half:ROPE] = sine
    return tables


def dot(a, b):
    return jnp.dot(a, b, preferred_element_type=F32)


def row_of(ref):
    return ref[...].reshape(1, -1)


def dot_nt(a, b):
    return lax.dot_general(a, b, (((1,), (1,)), ((), ())), preferred_element_type=F32)


def fused_kernel(
    n_sp,
    tokens, norm_gain, query_down, query_gain, latent_down, latent_gain, rope_down, query_up,
    key_up, value_up, glu_value, glu_gate, conv_taps, group_gain, head_proj, channel_proj, tables,
    out, log_out,
    w_q, w_g, w_o, tok_v, lat_v, rope_v, qup_v, kup_v, vup_v, tab_v,
    normed, keys, key_tmp, q_out, q_lat, q_scr, g_acc, gated, low_rows, high_rows, padded,
    mixed, parts, peer_parts, final, out_v,
    load_sem, z_recv, z_send, pair_recv, pair_send, n_recv, n_send, np_recv, np_send, q_recv, q_send,
    head_recv, head_send, halo_recv, halo_send, conv_recv, conv_send, p_recv, p_send, fin_recv, fin_send,
    corner_sem,
):
    z = lax.axis_index("sp")
    c = lax.axis_index("fs")
    t = lax.axis_index("tp")
    peer = 1 - t
    c_x = c + 1 - 2 * (c % 2)
    c_y = (c + 2) % 4
    c_d = 3 - c
    others = (c_x, c_y, c_d)
    n_fs = normed.shape[0]
    n_tp = 2
    rows, width = tokens.shape
    depth, q_cols = w_q.shape[1:]
    cols = w_g.shape[2] // 2
    heads = key_up.shape[1] // NOPE
    head_rows = head_proj.shape[0]
    out_rows, out_cols = w_o.shape[1:]
    half_width = width // n_tp
    per_core = n_fs // n_tp
    half_sp = n_sp // n_tp

    def lanes_at(index, size):
        return pl.ds(pl.multiple_of(index * size, LANES), size)

    loads = {}

    def load(name, src, dst):
        copy = pltpu.make_async_copy(src, dst, load_sem.at[len(loads)])
        copy.start()
        loads[name] = copy

    load("tok", tokens, tok_v)
    load("wq", query_down.at[:, lanes_at(c, q_cols)], w_q.at[z])
    load("wv", glu_value.at[:, lanes_at(c, cols)], w_g.at[z, :, pl.ds(0, cols)])
    load("wt", glu_gate.at[:, lanes_at(c, cols)], w_g.at[z, :, pl.ds(cols, cols)])
    load("lat", latent_down, lat_v)
    load("rope", rope_down, rope_v)
    load("tab", tables.at[:, pl.ds(pl.multiple_of(z * rows, LANES), rows), :], tab_v)
    load("hp", head_proj.at[:, lanes_at(c, out_cols)], w_o.at[z, pl.ds(0, head_rows), :])
    load("cp", channel_proj.at[:, lanes_at(c, out_cols)], w_o.at[z, pl.ds(head_rows, out_rows - head_rows), :])
    load("qup", query_up, qup_v)
    load("kup", key_up, kup_v)
    load("vup", value_up, vup_v)

    barrier = pltpu.get_barrier_semaphore()
    sides = [{"fs": c_x}, {"fs": c_y}, {"tp": peer}]
    for partner in sides:
        pl.semaphore_signal(barrier, inc=1, device_id=partner, device_id_type=MESH)

    @pl.when(z > 0)
    def _():
        pl.semaphore_signal(barrier, inc=1, device_id={"sp": z - 1}, device_id_type=MESH)

    @pl.when(z < n_sp - 1)
    def _():
        pl.semaphore_signal(barrier, inc=1, device_id={"sp": z + 1}, device_id_type=MESH)

    loads["tok"].wait()
    values = tok_v[...].astype(F32)
    normed[c] = rms_scale(values, row_of(norm_gain)).astype(BF16)
    for name in ("wq", "wv", "wt"):
        loads[name].wait()

    ends = (z == 0).astype(jnp.int32) + (z == n_sp - 1).astype(jnp.int32)
    pl.semaphore_wait(barrier, len(sides) + 2 - ends)
    pl.semaphore_signal(corner_sem, inc=1, device_id={"fs": c_x}, device_id_type=MESH)

    def remote(src, dst, send_sem, recv_sem, device):
        return pltpu.make_async_remote_copy(
            src_ref=src, dst_ref=dst, send_sem=send_sem, recv_sem=recv_sem,
            device_id=device, device_id_type=MESH,
        )

    q_half = depth // n_tp
    g_half = depth // 2
    k_half = rows // n_tp

    def half(first, size):
        return pl.ds(pl.multiple_of(first * size, 16), size)

    def block(u, shard, side=t):
        if u == Q:
            return w_q.at[shard, half(side, q_half), :]
        if u == K:
            return keys.at[shard, half(side, k_half), :]
        if u == V:
            return w_g.at[shard, pl.ds(0, g_half), :]
        if u == W:
            return w_g.at[shard, pl.ds(g_half, depth - g_half), :]
        if u == H:
            return w_o.at[shard, pl.ds(0, head_rows), :]
        return w_o.at[shard, pl.ds(head_rows, out_rows - head_rows), :]

    def z_copy(u, shard, kind, target):
        ref = block(u, shard)
        return remote(ref, ref, z_send.at[u, shard, kind], z_recv.at[u, shard], {"sp": target})

    def own(u, action):
        @pl.when(z > 0)
        def _():
            action(z_copy(u, z, LOW, z - 1))

        @pl.when(z < n_sp - 1)
        def _():
            action(z_copy(u, z, HIGH, z + 1))

    def send_own(u):
        own(u, lambda copy: copy.start())

    nearest = jnp.minimum(z, n_sp - 1 - z)
    arrivals = []
    for k in range(n_sp - 1):
        both = k < 2 * nearest
        distance = jnp.where(both, k // 2 + 1, k - nearest + 1)
        from_low = jnp.where(both, 1 - k % 2, (2 * z > n_sp - 1).astype(jnp.int32))
        arrivals.append((z - distance * (2 * from_low - 1), z + 2 * from_low - 1))

    def forwards(k):
        target = arrivals[k][1]
        return (target >= 0) & (target < n_sp)

    def relay(u, k):
        shard, target = arrivals[k]

        @pl.when(forwards(k))
        def _():
            copy = z_copy(u, shard, FWD, target)
            copy.wait_recv()
            copy.start()

    def settle(u, k):
        @pl.when(jnp.logical_not(forwards(k)))
        def _():
            z_copy(u, arrivals[k][0], FWD, jnp.where(z > 0, z - 1, z + 1)).wait_recv()

    def pair(u, shard, side):
        ref = block(u, shard, side)
        return remote(ref, ref, pair_send.at[u, shard], pair_recv.at[u, shard], {"tp": peer})

    def share(u, k):
        settle(u, k)
        pair(u, arrivals[k][0], t).start()

    def n_copy(i):
        ref = normed.at[c, :, lanes_at(t, half_width)]
        return remote(ref, ref, n_send.at[i], n_recv.at[i], {"fs": others[i]})

    def n_pair(i, side):
        ref = normed.at[others[i], :, lanes_at(side, half_width)]
        return remote(ref, ref, np_send.at[i], np_recv.at[i], {"tp": peer})

    def share_normed(i):
        n_copy(i).wait_recv()
        n_pair(i, t).start()

    send_own(Q)
    send_own(V)
    n_copy(0).start()
    n_copy(1).start()
    pl.semaphore_wait(corner_sem, 1)
    n_copy(2).start()

    def rotate_lanes(v):
        step = ROPE // 2
        return (
            v * tab_v[0] + pltpu.roll(v, LANES - step, 1) * tab_v[1] + pltpu.roll(v, step, 1) * tab_v[2]
        )

    loads["lat"].wait()
    own_normed = normed[c]
    latent = rms_scale(dot(own_normed, lat_v[...]), row_of(latent_gain))
    keys[z, :, 0:KVR] = latent.astype(BF16)
    loads["rope"].wait()
    loads["tab"].wait()
    key_tmp[...] = jnp.zeros_like(key_tmp)
    key_tmp[:, 0:ROPE] = dot_nt(own_normed, rope_v[...])
    keys[z, :, KVR : KVR + LANES] = rotate_lanes(key_tmp[...]).astype(BF16)
    send_own(K)

    last = n_sp - 2
    for u in (Q, K):
        for k in range(last):
            relay(u, k)
    send_own(W)
    share(Q, 0)
    share(K, 0)
    for k in range(last):
        relay(V, k)
    share_normed(0)
    share_normed(1)
    for u in (Q, K):
        relay(u, last)
    for k in range(1, last):
        share(Q, k)
        share(K, k)
    for k in range(last):
        relay(W, k)
    share_normed(2)
    share(Q, last)
    share(K, last)
    relay(V, last)

    for i in range(len(others)):
        n_pair(i, peer).wait_recv()
    for k in range(n_sp - 1):
        pair(Q, arrivals[k][0], peer).wait_recv()
    seqs = normed[pl.ds(per_core * t, per_core)].reshape(per_core * rows, width)
    q_out[...] = dot(seqs, w_q[...].reshape(n_sp * depth, q_cols)).reshape(per_core, rows, q_cols)

    def q_copies(i):
        seq = per_core * t + i
        return seq, [
            remote(q_out.at[i], q_lat.at[c], q_send.at[i, j], q_recv.at[c], {"fs": seq, "tp": core})
            for j, core in enumerate((t, peer))
        ]

    for i in range(per_core):
        seq, (same, other) = q_copies(i)
        other.start()

        @pl.when(seq != c)
        def _():
            same.start()

        @pl.when(seq == c)
        def _():
            q_lat[c] = q_out[i]

    def add_shard(shard, first=False):
        rows_in = normed[:, :, lanes_at(shard, depth)].reshape(n_fs * rows, depth)
        term = dot(rows_in, w_g[shard])
        g_acc[...] = term if first else g_acc[...] + term

    add_shard(z, True)
    relay(W, last)
    for name in ("hp", "cp", "qup", "kup", "vup"):
        loads[name].wait()
    send_own(H)
    send_own(C)
    for u in (V, W):
        settle(u, 0)
    add_shard(arrivals[0][0])

    for source in range(n_fs):
        @pl.when((c != source) | (t != c // per_core))
        def _():
            remote(q_out.at[0], q_lat.at[source], q_send.at[0, 0], q_recv.at[source], {"tp": peer}).wait_recv()

    whole_q = jnp.concatenate([q_lat[i] for i in range(n_fs)], axis=1)
    latent_query = rms_scale(whole_q, row_of(query_gain)).astype(BF16)
    q_scr[...] = dot(latent_query, qup_v[...])
    for k in range(n_sp - 1):
        pair(K, arrivals[k][0], peer).wait_recv()

    def attend(h, shifted):
        start = h * (NOPE + ROPE)
        source = q_scr[...]
        if start % LANES:
            source, start = shifted, start - ROPE
        plain = source[:, start : start + NOPE].astype(BF16)
        rope_part = rotate_lanes(source[:, start + NOPE : start + NOPE + LANES]).astype(BF16)
        absorbed = dot_nt(plain, kup_v[:, h * NOPE : (h + 1) * NOPE]).astype(BF16)
        query = jnp.concatenate([absorbed, rope_part], axis=1)
        all_keys = keys[...].reshape(n_sp * rows, KVR + LANES)
        scores = dot_nt(query, all_keys) * (NOPE + ROPE) ** (-0.5)
        row_max = jnp.max(scores, axis=1, keepdims=True)
        weights = jnp.exp(scores - row_max)
        total = jnp.sum(weights, axis=1, keepdims=True)
        added = dot(weights.astype(BF16), all_keys[:, 0:KVR])
        attended = (added / total).astype(BF16)
        head_out = dot(attended, vup_v[:, h * VDIM : (h + 1) * VDIM])
        mixed[c, :, h * VDIM : (h + 1) * VDIM] = head_out.astype(BF16)
        return row_max + jnp.log(total)

    def head_copy(h, i):
        ref = mixed.at[c, :, pl.ds(h * VDIM, VDIM)]
        return remote(ref, ref, head_send.at[h, i], head_recv.at[h, i], {"fs": others[i]})

    whole = q_scr[...]
    shifted = pltpu.roll(whole, whole.shape[1] - ROPE, 1)
    lane = lax.broadcasted_iota(jnp.int32, (rows, LANES), 1)
    logs = jnp.zeros((rows, LANES), F32)
    relays = {1: [(H, 0)], 2: [(H, 1), (C, 0)], 3: [(C, 1)]}
    for h in range(heads):
        logs = jnp.where(lane == h, attend(h, shifted), logs)
        for i in range(len(others)):
            head_copy(h, i).start()
        for u, k in relays.get(h, []):
            relay(u, k)
    log_out[...] = jnp.transpose(logs)[0:heads, :]

    for k in range(1, n_sp - 1):
        for u in (V, W):
            settle(u, k)
        add_shard(arrivals[k][0])

    halo = low_rows.shape[1]
    reach = conv_taps.shape[0] // 2
    acc = g_acc[...]
    gated[...] = (acc[:, 0:cols] * jax.nn.sigmoid(acc[:, cols : 2 * cols])).astype(BF16).reshape(n_fs, rows, cols)
    up_copy = remote(
        gated.at[:, pl.ds(rows - halo, halo), :], low_rows, halo_send.at[0], halo_recv.at[0], {"sp": z + 1}
    )
    down_copy = remote(
        gated.at[:, pl.ds(0, halo), :], high_rows, halo_send.at[1], halo_recv.at[1], {"sp": z - 1}
    )

    @pl.when(z < n_sp - 1)
    def _():
        up_copy.start()

    @pl.when(z > 0)
    def _():
        down_copy.start()

    padded[:, halo : halo + rows, :] = gated[...].astype(F32)
    relay(H, last)

    @pl.when(z > 0)
    def _():
        up_copy.wait_recv()
        padded[:, 0:halo, :] = low_rows[...].astype(F32)

    @pl.when(z == 0)
    def _():
        padded[:, 0:halo, :] = jnp.zeros((n_fs, halo, cols), F32)

    @pl.when(z < n_sp - 1)
    def _():
        down_copy.wait_recv()
        padded[:, halo + rows : 2 * halo + rows, :] = high_rows[...].astype(F32)

    @pl.when(z == n_sp - 1)
    def _():
        padded[:, halo + rows : 2 * halo + rows, :] = jnp.zeros((n_fs, halo, cols), F32)

    def conv_copy(s, i):
        ref = mixed.at[s, :, pl.ds(pl.multiple_of(head_rows + c * cols, LANES), cols)]
        return remote(ref, ref, conv_send.at[s, i], conv_recv.at[s, i], {"fs": others[i]})

    own_lanes = lanes_at(c, cols)
    taps = conv_taps[:, own_lanes].astype(F32)
    all_gains = row_of(group_gain).astype(F32)
    gains = all_gains[:, 0:cols]
    for i in range(1, n_fs):
        gains = jnp.where(c == i, all_gains[:, i * cols : (i + 1) * cols], gains)
    for s in range(n_fs):
        filtered = jnp.zeros((rows, cols), F32)
        for j in range(conv_taps.shape[0]):
            first = halo - reach + j
            filtered = filtered + padded[s, first : first + rows, :] * taps[j : j + 1, :]
        centred = filtered - jnp.mean(filtered, axis=1, keepdims=True)
        spread = jnp.mean(centred * centred, axis=1, keepdims=True)
        branch = centred * lax.rsqrt(spread + norm_eps) * gains
        branch = branch * jax.nn.sigmoid(branch)
        mixed[s, :, pl.ds(pl.multiple_of(head_rows + c * cols, LANES), cols)] = branch.astype(BF16)
        for i in range(len(others)):
            conv_copy(s, i).start()
        if s == 1:
            relay(C, last)

    for i in range(len(others)):
        for h in range(heads):
            head_copy(h, i).wait_recv()
    for s in range(n_fs):
        for i in range(len(others)):
            conv_copy(s, i).wait_recv()

    def p_copy(i):
        return remote(
            parts.at[peer * half_sp + i], peer_parts.at[i], p_send.at[i], p_recv.at[i], {"tp": peer}
        )

    def fin_copy(i, j):
        return remote(
            final.at[i, pl.ds(pl.multiple_of(others[j] * rows, LANES), rows), :],
            out_v.at[:, pl.ds(pl.multiple_of(i * n_fs * out_cols + c * out_cols, LANES), out_cols)],
            fin_send.at[i, j], fin_recv.at[i, j], {"fs": others[j]},
        )

    def add_part(shard):
        part = dot(mixed[...].reshape(n_fs * rows, out_rows), w_o[shard])
        parts[shard] = part.astype(BF16)
        for i in range(half_sp):
            @pl.when(shard == peer * half_sp + i)
            def _():
                p_copy(i).start()

    def finish(shard):
        for i in range(half_sp):
            @pl.when(shard == t * half_sp + i)
            def _():
                p_copy(i).wait_recv()
                total = parts[t * half_sp + i].astype(F32) + peer_parts[i].astype(F32)
                final[i] = total.astype(BF16)
                for j in range(len(others)):
                    fin_copy(i, j).start()
                out_v[:, pl.ds(pl.multiple_of(i * n_fs * out_cols + c * out_cols, LANES), out_cols)] = final[
                    i, pl.ds(pl.multiple_of(c * rows, LANES), rows), :
                ]

    shards = [z] + [shard for shard, _ in arrivals]
    for k, shard in enumerate(shards):
        if k:
            settle(H, k - 1)
            settle(C, k - 1)
        add_part(shard)
        if k:
            finish(shards[k - 1])
    finish(shards[-1])

    for u in (Q, K, V, W, H, C):
        own(u, lambda copy: copy.wait_send())
        for k in range(n_sp - 1):
            shard, target = arrivals[k]

            @pl.when(forwards(k))
            def _():
                z_copy(u, shard, FWD, target).wait_send()

            if u in (Q, K):
                pair(u, shard, t).wait_send()
    for i in range(len(others)):
        n_copy(i).wait_send()
        n_pair(i, t).wait_send()
        for h in range(heads):
            head_copy(h, i).wait_send()
        for s in range(n_fs):
            conv_copy(s, i).wait_send()
    for i in range(per_core):
        seq, (same, other) = q_copies(i)
        other.wait_send()

        @pl.when(seq != c)
        def _():
            same.wait_send()

    @pl.when(z < n_sp - 1)
    def _():
        up_copy.wait_send()

    @pl.when(z > 0)
    def _():
        down_copy.wait_send()

    for i in range(half_sp):
        p_copy(i).wait_send()
        for j in range(len(others)):
            fin_copy(i, j).wait()
    out[...] = out_v[...]


def fused_device(n_sp, n_fs, *args):
    (tokens, norm_gain, query_down, query_gain, latent_down, latent_gain, rope_down, query_up,
     key_up, value_up, glu_value, glu_gate, conv_taps, group_gain, head_proj, channel_proj) = args
    rows, width = tokens.shape
    depth, q_rank = query_down.shape
    cols = glu_value.shape[1] // n_fs
    heads = key_up.shape[1] // NOPE
    out_rows = head_proj.shape[0] + channel_proj.shape[0]
    out_cols = head_proj.shape[1] // n_fs
    q_cols = q_rank // n_fs
    halo = (conv_taps.shape[0] // 2 + 15) // 16 * 16
    tables = jnp.asarray(rope_tables(n_sp * rows))
    vmem = pl.BlockSpec(memory_space=pltpu.VMEM)
    hbm = pl.BlockSpec(memory_space=pltpu.HBM)
    operands = [
        (tokens, hbm), (norm_gain, vmem), (query_down, hbm), (query_gain, vmem),
        (latent_down, hbm), (latent_gain, vmem), (rope_down.T, hbm), (query_up, hbm),
        (key_up, hbm), (value_up, hbm), (glu_value, hbm), (glu_gate, hbm), (conv_taps, vmem),
        (group_gain, vmem), (head_proj, hbm), (channel_proj, hbm), (tables, hbm),
    ]
    like = lambda a: pltpu.VMEM(a.shape, a.dtype)
    dma = pltpu.SemaphoreType.DMA
    half_sp = n_sp // 2
    scratch = [
        pltpu.VMEM((n_sp, depth, q_cols), BF16),
        pltpu.VMEM((n_sp, depth, 2 * cols), BF16),
        pltpu.VMEM((n_sp, out_rows, out_cols), BF16),
        like(tokens), like(latent_down), pltpu.VMEM(rope_down.shape[::-1], BF16), like(query_up), like(key_up), like(value_up),
        pltpu.VMEM((3, rows, LANES), F32),
        pltpu.VMEM((n_fs, rows, width), BF16),
        pltpu.VMEM((n_sp, rows, KVR + LANES), BF16),
        pltpu.VMEM((rows, LANES), F32),
        pltpu.VMEM((n_fs // 2, rows, q_cols), F32),
        pltpu.VMEM((n_fs, rows, q_cols), F32),
        pltpu.VMEM((rows, query_up.shape[1]), F32),
        pltpu.VMEM((n_fs * rows, 2 * cols), F32),
        pltpu.VMEM((n_fs, rows, cols), BF16),
        pltpu.VMEM((n_fs, halo, cols), BF16),
        pltpu.VMEM((n_fs, halo, cols), BF16),
        pltpu.VMEM((n_fs, rows + 2 * halo, cols), F32),
        pltpu.VMEM((n_fs, rows, out_rows), BF16),
        pltpu.VMEM((n_sp, n_fs * rows, out_cols), BF16),
        pltpu.VMEM((half_sp, n_fs * rows, out_cols), BF16),
        pltpu.VMEM((half_sp, n_fs * rows, out_cols), BF16),
        pltpu.VMEM((rows, half_sp * n_fs * out_cols), BF16),
        dma((12,)), dma((6, n_sp)), dma((6, n_sp, 3)), dma((2, n_sp)), dma((2, n_sp)),
        dma((3,)), dma((3,)), dma((3,)), dma((3,)), dma((n_fs,)), dma((n_fs // 2, 2)),
        dma((heads, 3)), dma((heads, 3)), dma((2,)), dma((2,)), dma((n_fs, 3)), dma((n_fs, 3)),
        dma((half_sp,)), dma((half_sp,)), dma((half_sp, 3)), dma((half_sp, 3)),
        pltpu.SemaphoreType.REGULAR,
    ]
    return pl.pallas_call(
        functools.partial(fused_kernel, n_sp),
        out_shape=(
            jax.ShapeDtypeStruct((rows, half_sp * n_fs * out_cols), BF16),
            jax.ShapeDtypeStruct((heads, rows), F32),
        ),
        in_specs=[spec for _, spec in operands],
        out_specs=(vmem, vmem),
        scratch_shapes=scratch,
        compiler_params=pltpu.CompilerParams(
            collective_id=0, has_side_effects=True, vmem_limit_bytes=63 * 1024 * 1024
        ),
        name="fused_layer",
    )(*[value for value, _ in operands])


def solution(mesh):
    in_specs = (
        P(("fs", "sp"), None),
        P(),
        P("sp", None),
        P(),
        P(),
        P(),
        P(),
        P(None, "tp"),
        P(None, "tp"),
        P(None, "tp"),
        P("sp", "tp"),
        P("sp", "tp"),
        P(None, "tp"),
        P("tp"),
        P("tp", "sp"),
        P("tp", "sp"),
    )
    out_specs = (P(("fs", "sp"), "tp"), P("tp", ("fs", "sp")))
    body = per_device
    if mesh.shape["fs"] == 4 and mesh.shape["tp"] == 2 and mesh.shape["sp"] == 4:
        body = functools.partial(fused_device, mesh.shape["sp"], mesh.shape["fs"])
    return jax.shard_map(
        body, mesh=mesh, in_specs=in_specs, out_specs=out_specs, check_vma=False
    )
```

```python
import functools

import jax
import jax.numpy as jnp
import numpy as np
from jax import lax
from jax.experimental import pallas as pl
from jax.experimental.pallas import tpu as pltpu
from jax.sharding import PartitionSpec as P

NOPE = 128
ROPE = 64
VDIM = 128
KVR = 256
CH = 1024
GROUPS = 8
GRID_W = 64


norm_eps = 1e-06
rope_base = 10000.0
far_below = -1e30


def padded_2(block, sides, width):
    for axis, dim in sides:
        count = lax.axis_size(axis)
        forward = [(i, i + 1) for i in range(count - 1)]
        backward = [(target, source) for source, target in forward]
        low = lax.ppermute(
            lax.slice_in_dim(block, block.shape[dim] - width, None, axis=dim), axis, forward
        )
        high = lax.ppermute(lax.slice_in_dim(block, 0, width, axis=dim), axis, backward)
        block = jnp.concatenate([low, block, high], axis=dim)
    return block


def rms_scale(values, scale_gain):
    inv_rms = lax.rsqrt(jnp.mean(values * values, axis=-1, keepdims=True) + norm_eps)
    return values * inv_rms * scale_gain.astype(jnp.float32)


def angles_for(positions, rope_size):
    quarter = rope_size // 4
    inverse = rope_base ** (-jnp.arange(quarter, dtype=jnp.float32) / quarter)
    grid_row = (positions // GRID_W).astype(jnp.float32)
    grid_col = (positions % GRID_W).astype(jnp.float32)
    return jnp.concatenate([grid_row[:, None] * inverse, grid_col[:, None] * inverse], axis=-1)


def rotate(values, angles):
    half_size = values.shape[-1] // 2
    front_half = values[..., :half_size]
    back_half = values[..., half_size:]
    cosine = jnp.cos(angles)
    sine_part = jnp.sin(angles)
    return jnp.concatenate(
        [front_half * cosine - back_half * sine_part, back_half * cosine + front_half * sine_part],
        axis=-1,
    )


def key_block(normed, latent_down, latent_gain, rope_down, positions):
    latent = jnp.dot(normed, latent_down, preferred_element_type=jnp.float32)
    latent = rms_scale(latent, latent_gain).astype(jnp.bfloat16)
    rope_key = jnp.dot(normed, rope_down, preferred_element_type=jnp.float32)
    rope_key = rotate(rope_key, angles_for(positions, rope_key.shape[-1])).astype(jnp.bfloat16)
    return jnp.concatenate([latent, rope_key], axis=1)


def per_device(
    tokens,
    norm_gain,
    query_down,
    query_gain,
    latent_down,
    latent_gain,
    rope_down,
    query_up,
    key_up,
    value_up,
    glu_value,
    glu_gate,
    conv_taps,
    group_gain,
    head_proj,
    channel_proj,
):
    tok_count = tokens.shape[0]
    reach_rows = conv_taps.shape[0] // 2
    head_count = key_up.shape[1] // NOPE
    normed = rms_scale(tokens.astype(jnp.float32), norm_gain).astype(jnp.bfloat16)
    offsets = lax.axis_index("sp") * tok_count + jnp.arange(tok_count, dtype=jnp.int32)
    query_latent = jnp.dot(
        normed,
        lax.all_gather(query_down, "sp", axis=0, tiled=True),
        preferred_element_type=jnp.float32,
    )
    value_in = jnp.dot(
        normed,
        lax.all_gather(glu_value, "sp", axis=0, tiled=True),
        preferred_element_type=jnp.float32,
    )
    gate_in = jnp.dot(
        normed,
        lax.all_gather(glu_gate, "sp", axis=0, tiled=True),
        preferred_element_type=jnp.float32,
    )
    latent_query = rms_scale(query_latent, query_gain).astype(jnp.bfloat16)
    query_all = jnp.dot(latent_query, query_up, preferred_element_type=jnp.float32).reshape(
        tok_count, head_count, NOPE + ROPE
    )
    query_plain = query_all[:, :, :NOPE].astype(jnp.bfloat16)
    query_rope = rotate(query_all[:, :, NOPE:], angles_for(offsets, ROPE)[:, None, :]).astype(
        jnp.bfloat16
    )
    absorbed = jnp.einsum(
        "thd,rhd->htr",
        query_plain,
        key_up.reshape(KVR, head_count, NOPE),
        preferred_element_type=jnp.float32,
    ).astype(jnp.bfloat16)
    queries = jnp.concatenate([absorbed, jnp.transpose(query_rope, (1, 0, 2))], axis=-1)
    score_scale = (NOPE + ROPE) ** (-0.5)
    half_rows = tok_count // lax.axis_size("tp")
    first_row = lax.axis_index("tp") * half_rows
    own_rows = lax.dynamic_slice_in_dim(normed, first_row, half_rows, 0)
    own_positions = lax.dynamic_slice_in_dim(offsets, first_row, half_rows, 0)
    own_keys = key_block(own_rows, latent_down, latent_gain, rope_down, own_positions)
    block_keys = lax.all_gather(own_keys, ("sp", "tp"), axis=0, tiled=True)
    row_max = jnp.full((head_count, tok_count), far_below, jnp.float32)
    scores = (
        jnp.einsum("hqc,kc->hqk", queries, block_keys, preferred_element_type=jnp.float32)
        * score_scale
    )
    new_max = jnp.maximum(row_max, jnp.max(scores, axis=2))
    weights = jnp.exp(scores - new_max[:, :, None])
    new_sum = jnp.sum(weights, axis=2)
    added = jnp.einsum(
        "hqk,kr->hqr",
        weights.astype(jnp.bfloat16),
        block_keys[:, :KVR],
        preferred_element_type=jnp.float32,
    )
    gated_rows = (value_in * jax.nn.sigmoid(gate_in)).astype(jnp.bfloat16)
    padded = padded_2(gated_rows, (("sp", 0),), reach_rows)
    filtered = padded[0:tok_count].astype(jnp.float32) * conv_taps[0].astype(jnp.float32)
    for tap_index in range(1, conv_taps.shape[0]):
        filtered = filtered + padded[tap_index : tap_index + tok_count].astype(
            jnp.float32
        ) * conv_taps[tap_index].astype(jnp.float32)
    grouped = filtered.reshape(tok_count, -1, CH // GROUPS)
    centred = grouped - jnp.mean(grouped, axis=-1, keepdims=True)
    spread = jnp.mean(centred * centred, axis=-1, keepdims=True)
    normal_groups = (centred * lax.rsqrt(spread + norm_eps)).reshape(tok_count, -1)
    conv_branch = jax.nn.silu(normal_groups * group_gain.astype(jnp.float32)).astype(jnp.bfloat16)
    attended = (added / new_sum[:, :, None]).astype(jnp.bfloat16)
    log_weight = new_max + jnp.log(new_sum)
    head_out = jnp.einsum(
        "htr,rhv->thv",
        attended,
        value_up.reshape(KVR, head_count, VDIM),
        preferred_element_type=jnp.float32,
    )
    head_out = head_out.reshape(tok_count, head_count * VDIM).astype(jnp.bfloat16)
    mixed_in = jnp.concatenate([head_out, conv_branch], axis=1)
    out_weight = jnp.concatenate([head_proj, channel_proj], axis=0)
    partial_terms = jnp.dot(
        mixed_in,
        lax.all_gather(out_weight, "sp", axis=1, tiled=True),
        preferred_element_type=jnp.float32,
    )
    mixed_out = lax.psum_scatter(
        partial_terms.astype(jnp.bfloat16), "tp", scatter_dimension=1, tiled=True
    )
    return (mixed_out, log_weight)


LANES = 128
MESH = pl.DeviceIdType.MESH
F32 = jnp.float32
BF16 = jnp.bfloat16
LOW, HIGH, FWD = range(3)
Q, K, V, W, H, C = range(6)


def rope_tables(length):
    quarter = ROPE // 4
    inverse = np.float32(rope_base) ** (-np.arange(quarter, dtype=np.float32) / np.float32(quarter))
    positions = np.arange(length)
    row = (positions // GRID_W).astype(np.float32)[:, None] * inverse
    col = (positions % GRID_W).astype(np.float32)[:, None] * inverse
    angles = np.concatenate([row, col], axis=1).astype(np.float32)
    cosine, sine = np.cos(angles), np.sin(angles)
    tables = np.zeros((3, length, LANES), np.float32)
    half = ROPE // 2
    tables[0, :, :half] = cosine
    tables[0, :, half:ROPE] = cosine
    tables[1, :, :half] = -sine
    tables[2, :, half:ROPE] = sine
    return tables


def dot(a, b):
    return jnp.dot(a, b, preferred_element_type=F32)


def row_of(ref):
    return ref[...].reshape(1, -1)


def dot_nt(a, b):
    return lax.dot_general(a, b, (((1,), (1,)), ((), ())), preferred_element_type=F32)


def fused_kernel(
    n_sp,
    tokens, norm_gain_in, query_down, query_gain_in, latent_down, latent_gain_in, rope_down, query_up,
    key_up, value_up, glu_value, glu_gate, taps_in, group_gain_in, head_proj, channel_proj, tables,
    out, log_out,
    norm_gain, query_gain, latent_gain, conv_taps, group_gain, log_v,
    w_q, w_g, w_o, tok_v, lat_v, rope_v, qup_v, kup_v, vup_v, tab_v,
    normed, keys, key_tmp, q_out, q_lat, q_scr, g_acc, gated, low_rows, high_rows, padded,
    mixed, parts, placed, out_v,
    load_sem, z_recv, z_send, pair_recv, pair_send, n_recv, n_send, np_recv, np_send, q_recv, q_send,
    head_recv, head_send, halo_recv, halo_send, conv_recv, conv_send, fin_recv, fin_send, out_sem,
    corner_sem,
):
    z = lax.axis_index("sp")
    c = lax.axis_index("fs")
    t = lax.axis_index("tp")
    peer = 1 - t
    c_x = c + 1 - 2 * (c % 2)
    c_y = (c + 2) % 4
    c_d = 3 - c
    others = (c_x, c_y, c_d)
    n_fs = normed.shape[0]
    n_tp = 2
    rows, width = tokens.shape
    depth, q_cols = w_q.shape[1:]
    cols = w_g.shape[2] // 2
    heads = key_up.shape[1] // NOPE
    head_rows = head_proj.shape[0]
    out_rows, out_cols = w_o.shape[1:]
    half_width = width // n_tp
    per_core = n_fs // n_tp
    half_sp = n_sp // n_tp

    def lanes_at(index, size):
        return pl.ds(pl.multiple_of(index * size, LANES), size)

    barrier = pltpu.get_barrier_semaphore()
    sides = [{"fs": c_x}, {"fs": c_y}, {"tp": peer}]
    for partner in sides:
        pl.semaphore_signal(barrier, inc=1, device_id=partner, device_id_type=MESH)

    @pl.when(z > 0)
    def _():
        pl.semaphore_signal(barrier, inc=1, device_id={"sp": z - 1}, device_id_type=MESH)

    @pl.when(z < n_sp - 1)
    def _():
        pl.semaphore_signal(barrier, inc=1, device_id={"sp": z + 1}, device_id_type=MESH)

    loads = {}

    def load(name, src, dst):
        copy = pltpu.make_async_copy(src, dst, load_sem.at[len(loads)])
        copy.start()
        loads[name] = copy

    load("tok", tokens, tok_v)
    load("ng", norm_gain_in, norm_gain)
    load("wq", query_down.at[:, lanes_at(c, q_cols)], w_q.at[z])
    load("wv", glu_value.at[:, lanes_at(c, cols)], w_g.at[z, :, pl.ds(0, cols)])
    load("wt", glu_gate.at[:, lanes_at(c, cols)], w_g.at[z, :, pl.ds(cols, cols)])
    load("lat", latent_down, lat_v)
    load("rope", rope_down, rope_v)
    load("tab", tables.at[:, pl.ds(pl.multiple_of(z * rows, LANES), rows), :], tab_v)
    load("hp", head_proj.at[:, lanes_at(c, out_cols)], w_o.at[z, pl.ds(0, head_rows), :])
    load("cp", channel_proj.at[:, lanes_at(c, out_cols)], w_o.at[z, pl.ds(head_rows, out_rows - head_rows), :])
    load("qup", query_up, qup_v)
    load("kup", key_up, kup_v)
    load("vup", value_up, vup_v)
    load("qg", query_gain_in, query_gain)
    load("lg", latent_gain_in, latent_gain)
    load("taps", taps_in.at[:, lanes_at(c, cols)], conv_taps)
    load("gg", group_gain_in, group_gain)

    loads["tok"].wait()
    loads["ng"].wait()
    values = tok_v[...].astype(F32)
    normed[c] = rms_scale(values, row_of(norm_gain)).astype(BF16)
    for name in ("wq", "wv", "wt"):
        loads[name].wait()

    ends = (z == 0).astype(jnp.int32) + (z == n_sp - 1).astype(jnp.int32)
    pl.semaphore_wait(barrier, len(sides) + 2 - ends)
    pl.semaphore_signal(corner_sem, inc=1, device_id={"fs": c_x}, device_id_type=MESH)

    def remote(src, dst, send_sem, recv_sem, device):
        return pltpu.make_async_remote_copy(
            src_ref=src, dst_ref=dst, send_sem=send_sem, recv_sem=recv_sem,
            device_id=device, device_id_type=MESH,
        )

    q_half = depth // n_tp
    g_half = depth // 2
    k_half = rows // n_tp

    def half(first, size):
        return pl.ds(pl.multiple_of(first * size, 16), size)

    def block(u, shard, side=t):
        if u == Q:
            return w_q.at[shard, half(side, q_half), :]
        if u == K:
            return keys.at[shard, half(side, k_half), :]
        if u == V:
            return w_g.at[shard, pl.ds(0, g_half), :]
        if u == W:
            return w_g.at[shard, pl.ds(g_half, depth - g_half), :]
        if u == H:
            return w_o.at[shard, pl.ds(0, head_rows), :]
        return w_o.at[shard, pl.ds(head_rows, out_rows - head_rows), :]

    def z_copy(u, shard, kind, target):
        ref = block(u, shard)
        return remote(ref, ref, z_send.at[u, shard, kind], z_recv.at[u, shard], {"sp": target})

    def own(u, action):
        @pl.when(z > 0)
        def _():
            action(z_copy(u, z, LOW, z - 1))

        @pl.when(z < n_sp - 1)
        def _():
            action(z_copy(u, z, HIGH, z + 1))

    def send_own(u):
        own(u, lambda copy: copy.start())

    nearest = jnp.minimum(z, n_sp - 1 - z)
    arrivals = []
    for k in range(n_sp - 1):
        both = k < 2 * nearest
        distance = jnp.where(both, k // 2 + 1, k - nearest + 1)
        from_low = jnp.where(both, 1 - k % 2, (2 * z > n_sp - 1).astype(jnp.int32))
        arrivals.append((z - distance * (2 * from_low - 1), z + 2 * from_low - 1))

    def forwards(k):
        target = arrivals[k][1]
        return (target >= 0) & (target < n_sp)

    def relay(u, k):
        shard, target = arrivals[k]

        @pl.when(forwards(k))
        def _():
            copy = z_copy(u, shard, FWD, target)
            copy.wait_recv()
            copy.start()

    def settle(u, k):
        @pl.when(jnp.logical_not(forwards(k)))
        def _():
            z_copy(u, arrivals[k][0], FWD, jnp.where(z > 0, z - 1, z + 1)).wait_recv()

    def pair(u, shard, side):
        ref = block(u, shard, side)
        return remote(ref, ref, pair_send.at[u, shard], pair_recv.at[u, shard], {"tp": peer})

    def share(u, k):
        settle(u, k)
        pair(u, arrivals[k][0], t).start()

    def n_copy(i):
        ref = normed.at[c, :, lanes_at(t, half_width)]
        return remote(ref, ref, n_send.at[i], n_recv.at[i], {"fs": others[i]})

    def n_pair(i, side):
        ref = normed.at[others[i], :, lanes_at(side, half_width)]
        return remote(ref, ref, np_send.at[i], np_recv.at[i], {"tp": peer})

    def share_normed(i):
        n_copy(i).wait_recv()
        n_pair(i, t).start()

    send_own(Q)
    send_own(V)
    n_copy(0).start()
    n_copy(1).start()

    def rotate_lanes(v):
        step = ROPE // 2
        return (
            v * tab_v[0] + pltpu.roll(v, LANES - step, 1) * tab_v[1] + pltpu.roll(v, step, 1) * tab_v[2]
        )

    loads["lat"].wait()
    loads["lg"].wait()
    own_normed = normed[c]
    latent = rms_scale(dot(own_normed, lat_v[...]), row_of(latent_gain))
    keys[z, :, 0:KVR] = latent.astype(BF16)
    loads["rope"].wait()
    loads["tab"].wait()
    key_tmp[...] = jnp.zeros_like(key_tmp)
    key_tmp[:, 0:ROPE] = dot_nt(own_normed, rope_v[...])
    keys[z, :, KVR : KVR + LANES] = rotate_lanes(key_tmp[...]).astype(BF16)
    send_own(K)

    pl.semaphore_wait(corner_sem, 1)
    n_copy(2).start()

    last = n_sp - 2
    for k in range(last):
        relay(Q, k)
    send_own(W)
    for k in range(last):
        relay(K, k)
    share(Q, 0)
    relay(Q, last)
    relay(K, last)
    for k in range(last):
        relay(V, k)
    share_normed(0)
    share_normed(1)
    share(K, 0)
    for k in range(1, last):
        share(Q, k)
        share(K, k)
    for k in range(last):
        relay(W, k)
    share(Q, last)
    share_normed(2)
    share(K, last)
    relay(V, last)

    for i in range(len(others)):
        n_pair(i, peer).wait_recv()
    for k in range(n_sp - 1):
        pair(Q, arrivals[k][0], peer).wait_recv()
    seqs = normed[pl.ds(per_core * t, per_core)].reshape(per_core * rows, width)
    q_out[...] = dot(seqs, w_q[...].reshape(n_sp * depth, q_cols)).reshape(per_core, rows, q_cols)

    def q_copies(i):
        seq = per_core * t + i
        return seq, [
            remote(q_out.at[i], q_lat.at[c], q_send.at[i, j], q_recv.at[c], {"fs": seq, "tp": core})
            for j, core in enumerate((t, peer))
        ]

    for i in range(per_core):
        seq, (same, other) = q_copies(i)
        other.start()

        @pl.when(seq != c)
        def _():
            same.start()

        @pl.when(seq == c)
        def _():
            q_lat[c] = q_out[i]

    def add_shard(shard, first=False):
        rows_in = normed[:, :, lanes_at(shard, depth)].reshape(n_fs * rows, depth)
        term = dot(rows_in, w_g[shard])
        g_acc[...] = term if first else g_acc[...] + term

    halo = low_rows.shape[1]
    up_copy = remote(
        gated.at[:, pl.ds(rows - halo, halo), :], low_rows, halo_send.at[0], halo_recv.at[0], {"sp": z + 1}
    )
    down_copy = remote(
        gated.at[:, pl.ds(0, halo), :], high_rows, halo_send.at[1], halo_recv.at[1], {"sp": z - 1}
    )

    def gate():
        for k in range(n_sp - 1):
            for u in (V, W):
                settle(u, k)
            add_shard(arrivals[k][0])
        acc = g_acc[...]
        gated[...] = (acc[:, 0:cols] * jax.nn.sigmoid(acc[:, cols : 2 * cols])).astype(BF16).reshape(n_fs, rows, cols)

        @pl.when(z < n_sp - 1)
        def _():
            up_copy.start()

        @pl.when(z > 0)
        def _():
            down_copy.start()

    inner = (z > 0) & (z < n_sp - 1)
    add_shard(z, True)
    relay(W, last)

    @pl.when(inner)
    def _():
        gate()

    for name in ("hp", "cp", "qup", "kup", "vup", "qg", "taps", "gg"):
        loads[name].wait()
    send_own(H)
    send_own(C)

    for source in range(n_fs):
        @pl.when((c != source) | (t != c // per_core))
        def _():
            remote(q_out.at[0], q_lat.at[source], q_send.at[0, 0], q_recv.at[source], {"tp": peer}).wait_recv()

    whole_q = jnp.concatenate([q_lat[i] for i in range(n_fs)], axis=1)
    latent_query = rms_scale(whole_q, row_of(query_gain)).astype(BF16)
    q_scr[...] = dot(latent_query, qup_v[...])
    for k in range(n_sp - 1):
        pair(K, arrivals[k][0], peer).wait_recv()

    def attend(h, shifted):
        start = h * (NOPE + ROPE)
        source = q_scr[...]
        if start % LANES:
            source, start = shifted, start - ROPE
        plain = source[:, start : start + NOPE].astype(BF16)
        rope_part = rotate_lanes(source[:, start + NOPE : start + NOPE + LANES]).astype(BF16)
        absorbed = dot_nt(plain, kup_v[:, h * NOPE : (h + 1) * NOPE]).astype(BF16)
        query = jnp.concatenate([absorbed, rope_part], axis=1)
        all_keys = keys[...].reshape(n_sp * rows, KVR + LANES)
        scores = dot_nt(query, all_keys) * (NOPE + ROPE) ** (-0.5)
        row_max = jnp.max(scores, axis=1, keepdims=True)
        weights = jnp.exp(scores - row_max)
        total = jnp.sum(weights, axis=1, keepdims=True)
        added = dot(weights.astype(BF16), all_keys[:, 0:KVR])
        attended = (added / total).astype(BF16)
        head_out = dot(attended, vup_v[:, h * VDIM : (h + 1) * VDIM])
        mixed[c, :, h * VDIM : (h + 1) * VDIM] = head_out.astype(BF16)
        return row_max + jnp.log(total)

    def head_copy(h, i):
        ref = mixed.at[c, :, pl.ds(h * VDIM, VDIM)]
        return remote(ref, ref, head_send.at[h, i], head_recv.at[h, i], {"fs": others[i]})

    whole = q_scr[...]
    shifted = pltpu.roll(whole, whole.shape[1] - ROPE, 1)
    lane = lax.broadcasted_iota(jnp.int32, (rows, LANES), 1)
    logs = jnp.zeros((rows, LANES), F32)
    relays = {heads - 1: [(u, k) for u in (H, C) for k in range(last)]}
    for h in range(heads):
        logs = jnp.where(lane == h, attend(h, shifted), logs)
        for i in range(len(others)):
            head_copy(h, i).start()
        for u, k in relays.get(h, []):
            relay(u, k)
    log_v[...] = jnp.transpose(logs)[0:heads, :]
    log_copy = pltpu.make_async_copy(log_v, log_out, out_sem.at[0])
    log_copy.start()

    @pl.when(jnp.logical_not(inner))
    def _():
        gate()

    reach = conv_taps.shape[0] // 2
    padded[:, halo : halo + rows, :] = gated[...].astype(F32)
    relay(H, last)

    @pl.when(z > 0)
    def _():
        up_copy.wait_recv()
        padded[:, 0:halo, :] = low_rows[...].astype(F32)

    @pl.when(z == 0)
    def _():
        padded[:, 0:halo, :] = jnp.zeros((n_fs, halo, cols), F32)

    @pl.when(z < n_sp - 1)
    def _():
        down_copy.wait_recv()
        padded[:, halo + rows : 2 * halo + rows, :] = high_rows[...].astype(F32)

    @pl.when(z == n_sp - 1)
    def _():
        padded[:, halo + rows : 2 * halo + rows, :] = jnp.zeros((n_fs, halo, cols), F32)

    def conv_copy(s, i):
        ref = mixed.at[s, :, pl.ds(pl.multiple_of(head_rows + c * cols, LANES), cols)]
        return remote(ref, ref, conv_send.at[s, i], conv_recv.at[s, i], {"fs": others[i]})

    taps = conv_taps[...].astype(F32)
    all_gains = row_of(group_gain).astype(F32)
    gains = all_gains[:, 0:cols]
    for i in range(1, n_fs):
        gains = jnp.where(c == i, all_gains[:, i * cols : (i + 1) * cols], gains)
    for s in range(n_fs):
        filtered = jnp.zeros((rows, cols), F32)
        for j in range(conv_taps.shape[0]):
            first = halo - reach + j
            filtered = filtered + padded[s, first : first + rows, :] * taps[j : j + 1, :]
        centred = filtered - jnp.mean(filtered, axis=1, keepdims=True)
        spread = jnp.mean(centred * centred, axis=1, keepdims=True)
        branch = centred * lax.rsqrt(spread + norm_eps) * gains
        branch = branch * jax.nn.sigmoid(branch)
        mixed[s, :, pl.ds(pl.multiple_of(head_rows + c * cols, LANES), cols)] = branch.astype(BF16)
        for i in range(len(others)):
            conv_copy(s, i).start()
    relay(C, last)

    for i in range(len(others)):
        for h in range(heads):
            head_copy(h, i).wait_recv()
    for s in range(n_fs):
        for i in range(len(others)):
            conv_copy(s, i).wait_recv()

    def place(core, shard):
        first = (shard % half_sp) * (n_fs * out_cols) + c * out_cols
        return placed.at[core, :, pl.ds(pl.multiple_of(first, LANES), out_cols)]

    def fin_copy(shard, j):
        seq = others[j] if j < len(others) else c
        return remote(
            parts.at[shard, pl.ds(pl.multiple_of(seq * rows, LANES), rows), :], place(t, shard),
            fin_send.at[shard, j], fin_recv.at[t, shard % half_sp, j], {"fs": seq, "tp": shard // half_sp},
        )

    def add_part(shard, between):
        part = dot(mixed[:, :, 0:head_rows].reshape(n_fs * rows, head_rows), w_o[shard, 0:head_rows, :])
        between()
        part = part + dot(
            mixed[:, :, head_rows:out_rows].reshape(n_fs * rows, out_rows - head_rows), w_o[shard, head_rows:out_rows, :]
        )
        parts[shard] = part.astype(BF16)
        for j in range(len(others)):
            fin_copy(shard, j).start()

        @pl.when(shard // half_sp != t)
        def _():
            fin_copy(shard, len(others)).start()

        @pl.when(shard // half_sp == t)
        def _():
            first = (shard % half_sp) * (n_fs * out_cols) + c * out_cols
            placed[t, :, pl.ds(pl.multiple_of(first, LANES), out_cols)] = parts[
                shard, pl.ds(pl.multiple_of(c * rows, LANES), rows), :
            ]

    add_part(z, lambda: None)
    for k in range(n_sp - 1):
        settle(H, k)
        add_part(arrivals[k][0], functools.partial(settle, C, k))

    for u in (Q, K, V, W, H, C):
        own(u, lambda copy: copy.wait_send())
        for k in range(n_sp - 1):
            shard, target = arrivals[k]

            @pl.when(forwards(k))
            def _():
                z_copy(u, shard, FWD, target).wait_send()

            if u in (Q, K):
                pair(u, shard, t).wait_send()
    for i in range(len(others)):
        n_copy(i).wait_send()
        n_pair(i, t).wait_send()
        for h in range(heads):
            head_copy(h, i).wait_send()
        for s in range(n_fs):
            conv_copy(s, i).wait_send()
    for i in range(per_core):
        seq, (same, other) = q_copies(i)
        other.wait_send()

        @pl.when(seq != c)
        def _():
            same.wait_send()

    @pl.when(z < n_sp - 1)
    def _():
        up_copy.wait_send()

    @pl.when(z > 0)
    def _():
        down_copy.wait_send()

    for shard in range(n_sp):
        for j in range(len(others)):
            fin_copy(shard, j).wait_send()

        @pl.when(shard // half_sp != t)
        def _():
            fin_copy(shard, len(others)).wait_send()

    out_copies = []
    for i in range(half_sp):
        for j in range(len(others)):
            for core in range(n_tp):
                remote(
                    parts.at[0, pl.ds(0, rows), :], place(0, i), fin_send.at[0, j], fin_recv.at[core, i, j], {"tp": peer}
                ).wait_recv()
        remote(
            parts.at[0, pl.ds(0, rows), :], place(0, i), fin_send.at[0, 0], fin_recv.at[peer, i, len(others)], {"tp": peer}
        ).wait_recv()
        span = pl.ds(i * n_fs * out_cols, n_fs * out_cols)
        total = placed[0, :, span].astype(F32) + placed[1, :, span].astype(F32)
        out_v[:, span] = total.astype(BF16)
        copy = pltpu.make_async_copy(out_v.at[:, span], out.at[:, span], out_sem.at[1 + i])
        copy.start()
        out_copies.append(copy)
    log_copy.wait()
    for copy in out_copies:
        copy.wait()


def fused_device(n_sp, n_fs, *args):
    (tokens, norm_gain, query_down, query_gain, latent_down, latent_gain, rope_down, query_up,
     key_up, value_up, glu_value, glu_gate, conv_taps, group_gain, head_proj, channel_proj) = args
    rows, width = tokens.shape
    depth, q_rank = query_down.shape
    cols = glu_value.shape[1] // n_fs
    heads = key_up.shape[1] // NOPE
    out_rows = head_proj.shape[0] + channel_proj.shape[0]
    out_cols = head_proj.shape[1] // n_fs
    q_cols = q_rank // n_fs
    halo = (conv_taps.shape[0] // 2 + 15) // 16 * 16
    tables = jnp.asarray(rope_tables(n_sp * rows))
    hbm = pl.BlockSpec(memory_space=pltpu.HBM)
    operands = [
        tokens, norm_gain, query_down, query_gain, latent_down, latent_gain, rope_down.T, query_up,
        key_up, value_up, glu_value, glu_gate, conv_taps, group_gain, head_proj, channel_proj, tables,
    ]
    like = lambda a: pltpu.VMEM(a.shape, a.dtype)
    dma = pltpu.SemaphoreType.DMA
    half_sp = n_sp // 2
    scratch = [
        like(norm_gain), like(query_gain), like(latent_gain), pltpu.VMEM((conv_taps.shape[0], cols), BF16), like(group_gain),
        pltpu.VMEM((heads, rows), F32),
        pltpu.VMEM((n_sp, depth, q_cols), BF16),
        pltpu.VMEM((n_sp, depth, 2 * cols), BF16),
        pltpu.VMEM((n_sp, out_rows, out_cols), BF16),
        like(tokens), like(latent_down), pltpu.VMEM(rope_down.shape[::-1], BF16), like(query_up), like(key_up), like(value_up),
        pltpu.VMEM((3, rows, LANES), F32),
        pltpu.VMEM((n_fs, rows, width), BF16),
        pltpu.VMEM((n_sp, rows, KVR + LANES), BF16),
        pltpu.VMEM((rows, LANES), F32),
        pltpu.VMEM((n_fs // 2, rows, q_cols), F32),
        pltpu.VMEM((n_fs, rows, q_cols), F32),
        pltpu.VMEM((rows, query_up.shape[1]), F32),
        pltpu.VMEM((n_fs * rows, 2 * cols), F32),
        pltpu.VMEM((n_fs, rows, cols), BF16),
        pltpu.VMEM((n_fs, halo, cols), BF16),
        pltpu.VMEM((n_fs, halo, cols), BF16),
        pltpu.VMEM((n_fs, rows + 2 * halo, cols), F32),
        pltpu.VMEM((n_fs, rows, out_rows), BF16),
        pltpu.VMEM((n_sp, n_fs * rows, out_cols), BF16),
        pltpu.VMEM((2, rows, half_sp * n_fs * out_cols), BF16),
        pltpu.VMEM((rows, half_sp * n_fs * out_cols), BF16),
        dma((17,)), dma((6, n_sp)), dma((6, n_sp, 3)), dma((2, n_sp)), dma((2, n_sp)),
        dma((3,)), dma((3,)), dma((3,)), dma((3,)), dma((n_fs,)), dma((n_fs // 2, 2)),
        dma((heads, 3)), dma((heads, 3)), dma((2,)), dma((2,)), dma((n_fs, 3)), dma((n_fs, 3)),
        dma((2, half_sp, 4)), dma((n_sp, 4)), dma((1 + half_sp,)),
        pltpu.SemaphoreType.REGULAR,
    ]
    return pl.pallas_call(
        functools.partial(fused_kernel, n_sp),
        out_shape=(
            jax.ShapeDtypeStruct((rows, half_sp * n_fs * out_cols), BF16),
            jax.ShapeDtypeStruct((heads, rows), F32),
        ),
        in_specs=[hbm] * len(operands),
        out_specs=(hbm, hbm),
        scratch_shapes=scratch,
        compiler_params=pltpu.CompilerParams(
            collective_id=0, has_side_effects=True, vmem_limit_bytes=63 * 1024 * 1024
        ),
        name="fused_layer",
    )(*operands)


def solution(mesh):
    in_specs = (
        P(("fs", "sp"), None),
        P(),
        P("sp", None),
        P(),
        P(),
        P(),
        P(),
        P(None, "tp"),
        P(None, "tp"),
        P(None, "tp"),
        P("sp", "tp"),
        P("sp", "tp"),
        P(None, "tp"),
        P("tp"),
        P("tp", "sp"),
        P("tp", "sp"),
    )
    out_specs = (P(("fs", "sp"), "tp"), P("tp", ("fs", "sp")))
    body = per_device
    if mesh.shape["fs"] == 4 and mesh.shape["tp"] == 2 and mesh.shape["sp"] == 4:
        body = functools.partial(fused_device, mesh.shape["sp"], mesh.shape["fs"])
    return jax.shard_map(
        body, mesh=mesh, in_specs=in_specs, out_specs=out_specs, check_vma=False
    )
```

```python
import functools

import jax
import jax.numpy as jnp
import numpy as np
from jax import lax
from jax.experimental import pallas as pl
from jax.experimental.pallas import tpu as pltpu
from jax.sharding import PartitionSpec as P

NOPE = 128
ROPE = 64
VDIM = 128
KVR = 256
CH = 1024
GROUPS = 8
GRID_W = 64


norm_eps = 1e-06
rope_base = 10000.0
far_below = -1e30


def padded_2(block, sides, width):
    for axis, dim in sides:
        count = lax.axis_size(axis)
        forward = [(i, i + 1) for i in range(count - 1)]
        backward = [(target, source) for source, target in forward]
        low = lax.ppermute(
            lax.slice_in_dim(block, block.shape[dim] - width, None, axis=dim), axis, forward
        )
        high = lax.ppermute(lax.slice_in_dim(block, 0, width, axis=dim), axis, backward)
        block = jnp.concatenate([low, block, high], axis=dim)
    return block


def rms_scale(values, scale_gain):
    inv_rms = lax.rsqrt(jnp.mean(values * values, axis=-1, keepdims=True) + norm_eps)
    return values * inv_rms * scale_gain.astype(jnp.float32)


def angles_for(positions, rope_size):
    quarter = rope_size // 4
    inverse = rope_base ** (-jnp.arange(quarter, dtype=jnp.float32) / quarter)
    grid_row = (positions // GRID_W).astype(jnp.float32)
    grid_col = (positions % GRID_W).astype(jnp.float32)
    return jnp.concatenate([grid_row[:, None] * inverse, grid_col[:, None] * inverse], axis=-1)


def rotate(values, angles):
    half_size = values.shape[-1] // 2
    front_half = values[..., :half_size]
    back_half = values[..., half_size:]
    cosine = jnp.cos(angles)
    sine_part = jnp.sin(angles)
    return jnp.concatenate(
        [front_half * cosine - back_half * sine_part, back_half * cosine + front_half * sine_part],
        axis=-1,
    )


def key_block(normed, latent_down, latent_gain, rope_down, positions):
    latent = jnp.dot(normed, latent_down, preferred_element_type=jnp.float32)
    latent = rms_scale(latent, latent_gain).astype(jnp.bfloat16)
    rope_key = jnp.dot(normed, rope_down, preferred_element_type=jnp.float32)
    rope_key = rotate(rope_key, angles_for(positions, rope_key.shape[-1])).astype(jnp.bfloat16)
    return jnp.concatenate([latent, rope_key], axis=1)


def per_device(
    tokens,
    norm_gain,
    query_down,
    query_gain,
    latent_down,
    latent_gain,
    rope_down,
    query_up,
    key_up,
    value_up,
    glu_value,
    glu_gate,
    conv_taps,
    group_gain,
    head_proj,
    channel_proj,
):
    tok_count = tokens.shape[0]
    reach_rows = conv_taps.shape[0] // 2
    head_count = key_up.shape[1] // NOPE
    normed = rms_scale(tokens.astype(jnp.float32), norm_gain).astype(jnp.bfloat16)
    offsets = lax.axis_index("sp") * tok_count + jnp.arange(tok_count, dtype=jnp.int32)
    query_latent = jnp.dot(
        normed,
        lax.all_gather(query_down, "sp", axis=0, tiled=True),
        preferred_element_type=jnp.float32,
    )
    value_in = jnp.dot(
        normed,
        lax.all_gather(glu_value, "sp", axis=0, tiled=True),
        preferred_element_type=jnp.float32,
    )
    gate_in = jnp.dot(
        normed,
        lax.all_gather(glu_gate, "sp", axis=0, tiled=True),
        preferred_element_type=jnp.float32,
    )
    latent_query = rms_scale(query_latent, query_gain).astype(jnp.bfloat16)
    query_all = jnp.dot(latent_query, query_up, preferred_element_type=jnp.float32).reshape(
        tok_count, head_count, NOPE + ROPE
    )
    query_plain = query_all[:, :, :NOPE].astype(jnp.bfloat16)
    query_rope = rotate(query_all[:, :, NOPE:], angles_for(offsets, ROPE)[:, None, :]).astype(
        jnp.bfloat16
    )
    absorbed = jnp.einsum(
        "thd,rhd->htr",
        query_plain,
        key_up.reshape(KVR, head_count, NOPE),
        preferred_element_type=jnp.float32,
    ).astype(jnp.bfloat16)
    queries = jnp.concatenate([absorbed, jnp.transpose(query_rope, (1, 0, 2))], axis=-1)
    score_scale = (NOPE + ROPE) ** (-0.5)
    half_rows = tok_count // lax.axis_size("tp")
    first_row = lax.axis_index("tp") * half_rows
    own_rows = lax.dynamic_slice_in_dim(normed, first_row, half_rows, 0)
    own_positions = lax.dynamic_slice_in_dim(offsets, first_row, half_rows, 0)
    own_keys = key_block(own_rows, latent_down, latent_gain, rope_down, own_positions)
    block_keys = lax.all_gather(own_keys, ("sp", "tp"), axis=0, tiled=True)
    row_max = jnp.full((head_count, tok_count), far_below, jnp.float32)
    scores = (
        jnp.einsum("hqc,kc->hqk", queries, block_keys, preferred_element_type=jnp.float32)
        * score_scale
    )
    new_max = jnp.maximum(row_max, jnp.max(scores, axis=2))
    weights = jnp.exp(scores - new_max[:, :, None])
    new_sum = jnp.sum(weights, axis=2)
    added = jnp.einsum(
        "hqk,kr->hqr",
        weights.astype(jnp.bfloat16),
        block_keys[:, :KVR],
        preferred_element_type=jnp.float32,
    )
    gated_rows = (value_in * jax.nn.sigmoid(gate_in)).astype(jnp.bfloat16)
    padded = padded_2(gated_rows, (("sp", 0),), reach_rows)
    filtered = padded[0:tok_count].astype(jnp.float32) * conv_taps[0].astype(jnp.float32)
    for tap_index in range(1, conv_taps.shape[0]):
        filtered = filtered + padded[tap_index : tap_index + tok_count].astype(
            jnp.float32
        ) * conv_taps[tap_index].astype(jnp.float32)
    grouped = filtered.reshape(tok_count, -1, CH // GROUPS)
    centred = grouped - jnp.mean(grouped, axis=-1, keepdims=True)
    spread = jnp.mean(centred * centred, axis=-1, keepdims=True)
    normal_groups = (centred * lax.rsqrt(spread + norm_eps)).reshape(tok_count, -1)
    conv_branch = jax.nn.silu(normal_groups * group_gain.astype(jnp.float32)).astype(jnp.bfloat16)
    attended = (added / new_sum[:, :, None]).astype(jnp.bfloat16)
    log_weight = new_max + jnp.log(new_sum)
    head_out = jnp.einsum(
        "htr,rhv->thv",
        attended,
        value_up.reshape(KVR, head_count, VDIM),
        preferred_element_type=jnp.float32,
    )
    head_out = head_out.reshape(tok_count, head_count * VDIM).astype(jnp.bfloat16)
    mixed_in = jnp.concatenate([head_out, conv_branch], axis=1)
    out_weight = jnp.concatenate([head_proj, channel_proj], axis=0)
    partial_terms = jnp.dot(
        mixed_in,
        lax.all_gather(out_weight, "sp", axis=1, tiled=True),
        preferred_element_type=jnp.float32,
    )
    mixed_out = lax.psum_scatter(
        partial_terms.astype(jnp.bfloat16), "tp", scatter_dimension=1, tiled=True
    )
    return (mixed_out, log_weight)


LANES = 128
MESH = pl.DeviceIdType.MESH
F32 = jnp.float32
BF16 = jnp.bfloat16
LOW, HIGH, FWD = range(3)
Q, K, V, W, H, C = range(6)


def rope_tables(length):
    quarter = ROPE // 4
    inverse = np.float32(rope_base) ** (-np.arange(quarter, dtype=np.float32) / np.float32(quarter))
    positions = np.arange(length)
    row = (positions // GRID_W).astype(np.float32)[:, None] * inverse
    col = (positions % GRID_W).astype(np.float32)[:, None] * inverse
    angles = np.concatenate([row, col], axis=1).astype(np.float32)
    cosine, sine = np.cos(angles), np.sin(angles)
    tables = np.zeros((3, length, LANES), np.float32)
    half = ROPE // 2
    tables[0, :, :half] = cosine
    tables[0, :, half:ROPE] = cosine
    tables[1, :, :half] = -sine
    tables[2, :, half:ROPE] = sine
    return tables


def dot(a, b):
    return jnp.dot(a, b, preferred_element_type=F32)


def row_of(ref):
    return ref[...].reshape(1, -1)


def dot_nt(a, b):
    return lax.dot_general(a, b, (((1,), (1,)), ((), ())), preferred_element_type=F32)


def fused_kernel(
    n_sp,
    tokens, norm_gain_in, query_down, query_gain_in, latent_down, latent_gain_in, rope_down, query_up,
    key_up, value_up, glu_value, glu_gate, taps_in, group_gain_in, head_proj, channel_proj, tables,
    placed, log_out,
    norm_gain, query_gain, latent_gain, conv_taps, group_gain, log_v,
    w_q, w_g, w_o, tok_v, lat_v, rope_v, qup_v, kup_v, vup_v, tab_v,
    normed, keys, key_tmp, q_out, q_lat, q_scr, g_acc, gated, low_rows, high_rows, padded,
    mixed, parts, w_full, mixed_o, part_o,
    load_sem, z_recv, z_send, pair_recv, pair_send, n_recv, n_send, np_recv, np_send, q_recv, q_send,
    head_recv, head_send, halo_recv, halo_send, conv_recv, conv_send, fin_recv, fin_send, out_sem,
    up_recv, up_send, back_recv, back_send,
    corner_sem,
):
    z = lax.axis_index("sp")
    c = lax.axis_index("fs")
    t = lax.axis_index("tp")
    peer = 1 - t
    c_x = c + 1 - 2 * (c % 2)
    c_y = (c + 2) % 4
    c_d = 3 - c
    others = (c_x, c_y, c_d)
    n_fs = normed.shape[0]
    n_tp = 2
    rows, width = tokens.shape
    depth, q_cols = w_q.shape[1:]
    cols = w_g.shape[2] // 2
    heads = key_up.shape[1] // NOPE
    head_rows = head_proj.shape[0]
    out_rows, out_cols = w_o.shape[1:]
    half_width = width // n_tp
    per_core = n_fs // n_tp
    half_sp = n_sp // n_tp

    def lanes_at(index, size):
        return pl.ds(pl.multiple_of(index * size, LANES), size)

    barrier = pltpu.get_barrier_semaphore()
    sides = [{"fs": c_x}, {"fs": c_y}, {"tp": peer}]
    for partner in sides:
        pl.semaphore_signal(barrier, inc=1, device_id=partner, device_id_type=MESH)

    @pl.when(z > 0)
    def _():
        pl.semaphore_signal(barrier, inc=1, device_id={"sp": z - 1}, device_id_type=MESH)

    @pl.when(z < n_sp - 1)
    def _():
        pl.semaphore_signal(barrier, inc=1, device_id={"sp": z + 1}, device_id_type=MESH)

    loads = {}

    def load(name, src, dst):
        copy = pltpu.make_async_copy(src, dst, load_sem.at[len(loads)])
        copy.start()
        loads[name] = copy

    load("tok", tokens, tok_v)
    load("ng", norm_gain_in, norm_gain)
    load("wq", query_down.at[:, lanes_at(c, q_cols)], w_q.at[z])
    load("wv", glu_value.at[:, lanes_at(c, cols)], w_g.at[z, :, pl.ds(0, cols)])
    load("wt", glu_gate.at[:, lanes_at(c, cols)], w_g.at[z, :, pl.ds(cols, cols)])
    load("lat", latent_down, lat_v)
    load("rope", rope_down, rope_v)
    load("tab", tables.at[:, pl.ds(pl.multiple_of(z * rows, LANES), rows), :], tab_v)
    load("hp", head_proj.at[:, lanes_at(c, out_cols)], w_o.at[z, pl.ds(0, head_rows), :])
    load("cp", channel_proj.at[:, lanes_at(c, out_cols)], w_o.at[z, pl.ds(head_rows, out_rows - head_rows), :])
    load("qup", query_up, qup_v)
    load("kup", key_up, kup_v)
    load("vup", value_up, vup_v)
    load("qg", query_gain_in, query_gain)
    load("lg", latent_gain_in, latent_gain)
    load("taps", taps_in.at[:, lanes_at(c, cols)], conv_taps)
    load("gg", group_gain_in, group_gain)
    load("hf", head_proj, w_full.at[pl.ds(0, head_rows), :])
    load("cf", channel_proj, w_full.at[pl.ds(head_rows, out_rows - head_rows), :])

    loads["tok"].wait()
    loads["ng"].wait()
    values = tok_v[...].astype(F32)
    normed[c] = rms_scale(values, row_of(norm_gain)).astype(BF16)
    for name in ("wq", "wv", "wt"):
        loads[name].wait()

    ends = (z == 0).astype(jnp.int32) + (z == n_sp - 1).astype(jnp.int32)
    pl.semaphore_wait(barrier, len(sides) + 2 - ends)
    pl.semaphore_signal(corner_sem, inc=1, device_id={"fs": c_x}, device_id_type=MESH)

    def remote(src, dst, send_sem, recv_sem, device):
        return pltpu.make_async_remote_copy(
            src_ref=src, dst_ref=dst, send_sem=send_sem, recv_sem=recv_sem,
            device_id=device, device_id_type=MESH,
        )

    q_half = depth // n_tp
    g_half = depth // 2
    k_half = rows // n_tp

    def half(first, size):
        return pl.ds(pl.multiple_of(first * size, 16), size)

    def block(u, shard, side=t):
        if u == Q:
            return w_q.at[shard, half(side, q_half), :]
        if u == K:
            return keys.at[shard, half(side, k_half), :]
        if u == V:
            return w_g.at[shard, pl.ds(0, g_half), :]
        if u == W:
            return w_g.at[shard, pl.ds(g_half, depth - g_half), :]
        if u == H:
            return w_o.at[shard, pl.ds(0, head_rows), :]
        return w_o.at[shard, pl.ds(head_rows, out_rows - head_rows), :]

    def z_copy(u, shard, kind, target):
        ref = block(u, shard)
        return remote(ref, ref, z_send.at[u, shard, kind], z_recv.at[u, shard], {"sp": target})

    def own(u, action):
        skip = 1 if u in (H, C) else 0

        @pl.when(z > skip)
        def _():
            action(z_copy(u, z, LOW, z - 1))

        @pl.when(z < n_sp - 1 - skip)
        def _():
            action(z_copy(u, z, HIGH, z + 1))

    def send_own(u):
        own(u, lambda copy: copy.start())

    nearest = jnp.minimum(z, n_sp - 1 - z)
    arrivals = []
    for k in range(n_sp - 1):
        both = k < 2 * nearest
        distance = jnp.where(both, k // 2 + 1, k - nearest + 1)
        from_low = jnp.where(both, 1 - k % 2, (2 * z > n_sp - 1).astype(jnp.int32))
        arrivals.append((z - distance * (2 * from_low - 1), z + 2 * from_low - 1))

    def forwards(k):
        target = arrivals[k][1]
        return (target >= 0) & (target < n_sp)

    def relay(u, k):
        shard, target = arrivals[k]

        @pl.when(forwards(k))
        def _():
            copy = z_copy(u, shard, FWD, target)
            copy.wait_recv()
            copy.start()

    inner = (z > 0) & (z < n_sp - 1)
    lower = 2 * z < n_sp
    outer = jnp.where(lower, 0, n_sp - 1)
    near = jnp.where(lower, 1, n_sp - 2)
    far = jnp.where(lower, n_sp - 2, 1)

    def pass_on(u, shard, target):
        @pl.when(inner)
        def _():
            copy = z_copy(u, shard, FWD, target)
            copy.wait_recv()
            copy.start()

    def settle(u, k):
        @pl.when(jnp.logical_not(forwards(k)))
        def _():
            z_copy(u, arrivals[k][0], FWD, jnp.where(z > 0, z - 1, z + 1)).wait_recv()

    def pair(u, shard, side):
        ref = block(u, shard, side)
        return remote(ref, ref, pair_send.at[u, shard], pair_recv.at[u, shard], {"tp": peer})

    def share(u, k):
        settle(u, k)
        pair(u, arrivals[k][0], t).start()

    def n_copy(i):
        ref = normed.at[c, :, lanes_at(t, half_width)]
        return remote(ref, ref, n_send.at[i], n_recv.at[i], {"fs": others[i]})

    def n_pair(i, side):
        ref = normed.at[others[i], :, lanes_at(side, half_width)]
        return remote(ref, ref, np_send.at[i], np_recv.at[i], {"tp": peer})

    def share_normed(i):
        n_copy(i).wait_recv()
        n_pair(i, t).start()

    send_own(Q)
    send_own(V)
    n_copy(0).start()
    n_copy(1).start()

    def rotate_lanes(v):
        step = ROPE // 2
        return (
            v * tab_v[0] + pltpu.roll(v, LANES - step, 1) * tab_v[1] + pltpu.roll(v, step, 1) * tab_v[2]
        )

    loads["lat"].wait()
    loads["lg"].wait()
    own_normed = normed[c]
    latent = rms_scale(dot(own_normed, lat_v[...]), row_of(latent_gain))
    keys[z, :, 0:KVR] = latent.astype(BF16)
    loads["rope"].wait()
    loads["tab"].wait()
    key_tmp[...] = jnp.zeros_like(key_tmp)
    key_tmp[:, 0:ROPE] = dot_nt(own_normed, rope_v[...])
    keys[z, :, KVR : KVR + LANES] = rotate_lanes(key_tmp[...]).astype(BF16)
    send_own(K)

    pl.semaphore_wait(corner_sem, 1)
    n_copy(2).start()

    last = n_sp - 2
    for k in range(last):
        relay(Q, k)
    send_own(W)
    for k in range(last):
        relay(K, k)
    share(Q, 0)
    relay(Q, last)
    relay(K, last)
    for k in range(last):
        relay(V, k)
    share_normed(0)
    share_normed(1)
    share(K, 0)
    for k in range(1, last):
        share(Q, k)
        share(K, k)
    for k in range(last):
        relay(W, k)
    share(Q, last)
    share_normed(2)
    share(K, last)
    relay(V, last)

    for i in range(len(others)):
        n_pair(i, peer).wait_recv()
    for k in range(n_sp - 1):
        pair(Q, arrivals[k][0], peer).wait_recv()
    seqs = normed[pl.ds(per_core * t, per_core)].reshape(per_core * rows, width)
    q_out[...] = dot(seqs, w_q[...].reshape(n_sp * depth, q_cols)).reshape(per_core, rows, q_cols)

    def q_copies(i):
        seq = per_core * t + i
        return seq, [
            remote(q_out.at[i], q_lat.at[c], q_send.at[i, j], q_recv.at[c], {"fs": seq, "tp": core})
            for j, core in enumerate((t, peer))
        ]

    for i in range(per_core):
        seq, (same, other) = q_copies(i)
        other.start()

        @pl.when(seq != c)
        def _():
            same.start()

        @pl.when(seq == c)
        def _():
            q_lat[c] = q_out[i]

    def add_shard(shard, first=False):
        rows_in = normed[:, :, lanes_at(shard, depth)].reshape(n_fs * rows, depth)
        term = dot(rows_in, w_g[shard])
        g_acc[...] = term if first else g_acc[...] + term

    halo = low_rows.shape[1]
    up_copy = remote(
        gated.at[:, pl.ds(rows - halo, halo), :], low_rows, halo_send.at[0], halo_recv.at[0], {"sp": z + 1}
    )
    down_copy = remote(
        gated.at[:, pl.ds(0, halo), :], high_rows, halo_send.at[1], halo_recv.at[1], {"sp": z - 1}
    )

    def gate():
        for k in range(n_sp - 1):
            for u in (V, W):
                settle(u, k)
            add_shard(arrivals[k][0])
        acc = g_acc[...]
        gated[...] = (acc[:, 0:cols] * jax.nn.sigmoid(acc[:, cols : 2 * cols])).astype(BF16).reshape(n_fs, rows, cols)

        @pl.when(z < n_sp - 1)
        def _():
            up_copy.start()

        @pl.when(z > 0)
        def _():
            down_copy.start()

    add_shard(z, True)
    relay(W, last)

    @pl.when(inner)
    def _():
        gate()

    for name in ("hp", "cp", "qup", "kup", "vup", "qg", "taps", "gg"):
        loads[name].wait()
    send_own(H)
    send_own(C)

    for source in range(n_fs):
        @pl.when((c != source) | (t != c // per_core))
        def _():
            remote(q_out.at[0], q_lat.at[source], q_send.at[0, 0], q_recv.at[source], {"tp": peer}).wait_recv()

    for u in (H, C):
        pass_on(u, outer, far)
    whole_q = jnp.concatenate([q_lat[i] for i in range(n_fs)], axis=1)
    latent_query = rms_scale(whole_q, row_of(query_gain)).astype(BF16)
    q_scr[...] = dot(latent_query, qup_v[...])
    for k in range(n_sp - 1):
        pair(K, arrivals[k][0], peer).wait_recv()

    def attend(h, shifted):
        start = h * (NOPE + ROPE)
        source = q_scr[...]
        if start % LANES:
            source, start = shifted, start - ROPE
        plain = source[:, start : start + NOPE].astype(BF16)
        rope_part = rotate_lanes(source[:, start + NOPE : start + NOPE + LANES]).astype(BF16)
        absorbed = dot_nt(plain, kup_v[:, h * NOPE : (h + 1) * NOPE]).astype(BF16)
        query = jnp.concatenate([absorbed, rope_part], axis=1)
        all_keys = keys[...].reshape(n_sp * rows, KVR + LANES)
        scores = dot_nt(query, all_keys) * (NOPE + ROPE) ** (-0.5)
        row_max = jnp.max(scores, axis=1, keepdims=True)
        weights = jnp.exp(scores - row_max)
        total = jnp.sum(weights, axis=1, keepdims=True)
        added = dot(weights.astype(BF16), all_keys[:, 0:KVR])
        attended = (added / total).astype(BF16)
        head_out = dot(attended, vup_v[:, h * VDIM : (h + 1) * VDIM])
        mixed[c, :, h * VDIM : (h + 1) * VDIM] = head_out.astype(BF16)
        return row_max + jnp.log(total)

    def head_copy(h, i):
        ref = mixed.at[c, :, pl.ds(h * VDIM, VDIM)]
        return remote(ref, ref, head_send.at[h, i], head_recv.at[h, i], {"fs": others[i]})

    whole = q_scr[...]
    shifted = pltpu.roll(whole, whole.shape[1] - ROPE, 1)
    lane = lax.broadcasted_iota(jnp.int32, (rows, LANES), 1)
    logs = jnp.zeros((rows, LANES), F32)

    def up_copy_of(index, group):
        ref = mixed.at[c, :, lanes_at(group, cols)]
        return remote(ref, mixed_o.at[:, lanes_at(group, cols)], up_send.at[index], up_recv.at[index], {"sp": near})

    def send_up(index, group):
        @pl.when(jnp.logical_not(inner))
        def _():
            up_copy_of(index, group).start()

    for h in range(heads):
        logs = jnp.where(lane == h, attend(h, shifted), logs)
        for i in range(len(others)):
            head_copy(h, i).start()
        send_up(h, h)
        if h == 0:
            pass_on(H, far, outer)
    pass_on(C, far, outer)
    log_v[...] = jnp.transpose(logs)[0:heads, :]
    log_copy = pltpu.make_async_copy(log_v, log_out, out_sem.at[0])
    log_copy.start()

    @pl.when(jnp.logical_not(inner))
    def _():
        gate()

    reach = conv_taps.shape[0] // 2
    padded[:, halo : halo + rows, :] = gated[...].astype(F32)

    @pl.when(z > 0)
    def _():
        up_copy.wait_recv()
        padded[:, 0:halo, :] = low_rows[...].astype(F32)

    @pl.when(z == 0)
    def _():
        padded[:, 0:halo, :] = jnp.zeros((n_fs, halo, cols), F32)

    @pl.when(z < n_sp - 1)
    def _():
        down_copy.wait_recv()
        padded[:, halo + rows : 2 * halo + rows, :] = high_rows[...].astype(F32)

    @pl.when(z == n_sp - 1)
    def _():
        padded[:, halo + rows : 2 * halo + rows, :] = jnp.zeros((n_fs, halo, cols), F32)

    def conv_copy(s, i):
        ref = mixed.at[s, :, pl.ds(pl.multiple_of(head_rows + c * cols, LANES), cols)]
        return remote(ref, ref, conv_send.at[s, i], conv_recv.at[s, i], {"fs": others[i]})

    taps = conv_taps[...].astype(F32)
    all_gains = row_of(group_gain).astype(F32)
    gains = all_gains[:, 0:cols]
    for i in range(1, n_fs):
        gains = jnp.where(c == i, all_gains[:, i * cols : (i + 1) * cols], gains)
    relay(H, last)

    def conv_seq(s):
        filtered = jnp.zeros((rows, cols), F32)
        for j in range(conv_taps.shape[0]):
            first = halo - reach + j
            filtered = filtered + padded[s, first : first + rows, :] * taps[j : j + 1, :]
        centred = filtered - jnp.mean(filtered, axis=1, keepdims=True)
        spread = jnp.mean(centred * centred, axis=1, keepdims=True)
        branch = centred * lax.rsqrt(spread + norm_eps) * gains
        branch = branch * jax.nn.sigmoid(branch)
        mixed[s, :, pl.ds(pl.multiple_of(head_rows + c * cols, LANES), cols)] = branch.astype(BF16)

    for i in (2, 0, 1):
        conv_seq(others[i])
        conv_copy(others[i], i).start()
    conv_seq(c)
    send_up(heads + c, heads + c)
    for s in others + (c,):
        for i in range(len(others)):
            if s is not others[i]:
                conv_copy(s, i).start()
    relay(C, last)
    for i in range(len(others)):
        conv_copy(c, i).wait_recv()
        send_up(heads + others[i], heads + others[i])

    back_lanes = lanes_at(z % half_sp, n_fs * out_cols)
    back_copy = remote(
        part_o, placed.at[t, :, back_lanes], back_send.at[0], back_recv.at[t], {"sp": outer, "tp": z // half_sp}
    )
    for name in ("hf", "cf"):
        loads[name].wait()

    def neighbour_part():
        for i in range(heads + n_fs):
            up_copy_of(i, i).wait_recv()
        part_o[...] = dot(mixed_o[...], w_full[...]).astype(BF16)
        back_copy.start()

    @pl.when(inner)
    def _():
        neighbour_part()

    for i in range(len(others)):
        for h in range(heads):
            head_copy(h, i).wait_recv()
    for s in others:
        for i in range(len(others)):
            conv_copy(s, i).wait_recv()

    def place(core, shard):
        first = (shard % half_sp) * (n_fs * out_cols) + c * out_cols
        return placed.at[core, :, pl.ds(pl.multiple_of(first, LANES), out_cols)]

    def fin_copy(shard, j):
        seq = others[j] if j < len(others) else c
        return remote(
            parts.at[shard, pl.ds(pl.multiple_of(seq * rows, LANES), rows), :], place(t, shard),
            fin_send.at[shard, j], fin_recv.at[t, shard % half_sp, j], {"fs": seq, "tp": shard // half_sp},
        )

    def keep_copy(shard):
        ref = parts.at[shard, pl.ds(pl.multiple_of(c * rows, LANES), rows), :]
        return pltpu.make_async_copy(ref, place(t, shard), out_sem.at[1 + shard % half_sp])

    def add_part(shard, between):
        part = dot(mixed[:, :, 0:head_rows].reshape(n_fs * rows, head_rows), w_o[shard, 0:head_rows, :])
        between()
        part = part + dot(
            mixed[:, :, head_rows:out_rows].reshape(n_fs * rows, out_rows - head_rows), w_o[shard, head_rows:out_rows, :]
        )
        parts[shard] = part.astype(BF16)
        for j in range(len(others)):
            fin_copy(shard, j).start()

        @pl.when(shard // half_sp != t)
        def _():
            fin_copy(shard, len(others)).start()

        @pl.when(shard // half_sp == t)
        def _():
            keep_copy(shard).start()

    add_part(z, lambda: None)

    @pl.when(inner)
    def _():
        add_part(arrivals[0][0], lambda: None)

    for k in range(1, n_sp - 1):
        settle(H, k)
        add_part(arrivals[k][0], functools.partial(settle, C, k))

    for u in (Q, K, V, W, H, C):
        own(u, lambda copy: copy.wait_send())
        for k in range(n_sp - 1):
            shard, target = arrivals[k]

            @pl.when(forwards(k))
            def _():
                z_copy(u, shard, FWD, target).wait_send()

            if u in (Q, K):
                pair(u, shard, t).wait_send()
    for i in range(len(others)):
        n_copy(i).wait_send()
        n_pair(i, t).wait_send()
        for h in range(heads):
            head_copy(h, i).wait_send()
        for s in range(n_fs):
            conv_copy(s, i).wait_send()
    for i in range(per_core):
        seq, (same, other) = q_copies(i)
        other.wait_send()

        @pl.when(seq != c)
        def _():
            same.wait_send()

    @pl.when(z < n_sp - 1)
    def _():
        up_copy.wait_send()

    @pl.when(z > 0)
    def _():
        down_copy.wait_send()

    for index in range(heads + n_fs):
        @pl.when(jnp.logical_not(inner))
        def _():
            up_copy_of(index, index).wait_send()

    @pl.when(inner)
    def _():
        back_copy.wait_send()

    for shard in range(n_sp):
        computed = inner | (shard != near)

        @pl.when(computed)
        def _():
            for j in range(len(others)):
                fin_copy(shard, j).wait_send()

        @pl.when(computed & (shard // half_sp != t))
        def _():
            fin_copy(shard, len(others)).wait_send()

    for i in range(half_sp):
        shard = t * half_sp + i
        computed = inner | (shard != near)

        def arrived(core, j):
            remote(
                parts.at[0, pl.ds(0, rows), :], place(0, i), fin_send.at[0, j], fin_recv.at[core, i, j], {"tp": peer}
            ).wait_recv()

        @pl.when(computed)
        def _():
            for core in range(n_tp):
                for j in range(len(others)):
                    arrived(core, j)
            arrived(peer, len(others))
            keep_copy(shard).wait()

        @pl.when(jnp.logical_not(computed))
        def _():
            for core in range(n_tp):
                remote(
                    part_o, placed.at[0, :, lanes_at(i, n_fs * out_cols)], back_send.at[0], back_recv.at[core], {"tp": peer}
                ).wait_recv()
    log_copy.wait()


def finish_kernel(placed, log_in, out, log_out):
    out[...] = (placed[0].astype(F32) + placed[1].astype(F32)).astype(BF16)
    log_out[...] = log_in[...]


def fused_device(n_sp, n_fs, *args):
    (tokens, norm_gain, query_down, query_gain, latent_down, latent_gain, rope_down, query_up,
     key_up, value_up, glu_value, glu_gate, conv_taps, group_gain, head_proj, channel_proj) = args
    rows, width = tokens.shape
    depth, q_rank = query_down.shape
    cols = glu_value.shape[1] // n_fs
    heads = key_up.shape[1] // NOPE
    out_rows = head_proj.shape[0] + channel_proj.shape[0]
    out_cols = head_proj.shape[1] // n_fs
    q_cols = q_rank // n_fs
    halo = (conv_taps.shape[0] // 2 + 15) // 16 * 16
    tables = jnp.asarray(rope_tables(n_sp * rows))
    hbm = pl.BlockSpec(memory_space=pltpu.HBM)
    operands = [
        tokens, norm_gain, query_down, query_gain, latent_down, latent_gain, rope_down.T, query_up,
        key_up, value_up, glu_value, glu_gate, conv_taps, group_gain, head_proj, channel_proj, tables,
    ]
    like = lambda a: pltpu.VMEM(a.shape, a.dtype)
    dma = pltpu.SemaphoreType.DMA
    half_sp = n_sp // 2
    scratch = [
        like(norm_gain), like(query_gain), like(latent_gain), pltpu.VMEM((conv_taps.shape[0], cols), BF16), like(group_gain),
        pltpu.VMEM((heads, rows), F32),
        pltpu.VMEM((n_sp, depth, q_cols), BF16),
        pltpu.VMEM((n_sp, depth, 2 * cols), BF16),
        pltpu.VMEM((n_sp, out_rows, out_cols), BF16),
        like(tokens), like(latent_down), pltpu.VMEM(rope_down.shape[::-1], BF16), like(query_up), like(key_up), like(value_up),
        pltpu.VMEM((3, rows, LANES), F32),
        pltpu.VMEM((n_fs, rows, width), BF16),
        pltpu.VMEM((n_sp, rows, KVR + LANES), BF16),
        pltpu.VMEM((rows, LANES), F32),
        pltpu.VMEM((n_fs // 2, rows, q_cols), F32),
        pltpu.VMEM((n_fs, rows, q_cols), F32),
        pltpu.VMEM((rows, query_up.shape[1]), F32),
        pltpu.VMEM((n_fs * rows, 2 * cols), F32),
        pltpu.VMEM((n_fs, rows, cols), BF16),
        pltpu.VMEM((n_fs, halo, cols), BF16),
        pltpu.VMEM((n_fs, halo, cols), BF16),
        pltpu.VMEM((n_fs, rows + 2 * halo, cols), F32),
        pltpu.VMEM((n_fs, rows, out_rows), BF16),
        pltpu.VMEM((n_sp, n_fs * rows, out_cols), BF16),
        pltpu.VMEM((out_rows, n_fs * out_cols), BF16),
        pltpu.VMEM((rows, out_rows), BF16),
        pltpu.VMEM((rows, n_fs * out_cols), BF16),
        dma((19,)), dma((6, n_sp)), dma((6, n_sp, 3)), dma((2, n_sp)), dma((2, n_sp)),
        dma((3,)), dma((3,)), dma((3,)), dma((3,)), dma((n_fs,)), dma((n_fs // 2, 2)),
        dma((heads, 3)), dma((heads, 3)), dma((2,)), dma((2,)), dma((n_fs, 3)), dma((n_fs, 3)),
        dma((2, half_sp, 4)), dma((n_sp, 4)), dma((1 + half_sp,)),
        dma((heads + n_fs,)), dma((heads + n_fs,)), dma((2,)), dma((1,)),
        pltpu.SemaphoreType.REGULAR,
    ]
    shapes = (
        jax.ShapeDtypeStruct((rows, half_sp * n_fs * out_cols), BF16),
        jax.ShapeDtypeStruct((heads, rows), F32),
    )
    placed, logs = pl.pallas_call(
        functools.partial(fused_kernel, n_sp),
        out_shape=(jax.ShapeDtypeStruct((2,) + shapes[0].shape, BF16), shapes[1]),
        in_specs=[hbm] * len(operands),
        out_specs=(hbm, hbm),
        scratch_shapes=scratch,
        compiler_params=pltpu.CompilerParams(
            collective_id=0, has_side_effects=True, vmem_limit_bytes=63 * 1024 * 1024
        ),
        name="fused_layer",
    )(*operands)
    return pl.pallas_call(finish_kernel, out_shape=shapes, name="finish")(placed, logs)


def solution(mesh):
    in_specs = (
        P(("fs", "sp"), None),
        P(),
        P("sp", None),
        P(),
        P(),
        P(),
        P(),
        P(None, "tp"),
        P(None, "tp"),
        P(None, "tp"),
        P("sp", "tp"),
        P("sp", "tp"),
        P(None, "tp"),
        P("tp"),
        P("tp", "sp"),
        P("tp", "sp"),
    )
    out_specs = (P(("fs", "sp"), "tp"), P("tp", ("fs", "sp")))
    body = per_device
    if mesh.shape["fs"] == 4 and mesh.shape["tp"] == 2 and mesh.shape["sp"] == 4:
        body = functools.partial(fused_device, mesh.shape["sp"], mesh.shape["fs"])
    return jax.shard_map(
        body, mesh=mesh, in_specs=in_specs, out_specs=out_specs, check_vma=False
    )
```

```python
import functools

import jax
import jax.numpy as jnp
import numpy as np
from jax import lax
from jax.experimental import pallas as pl
from jax.experimental.pallas import tpu as pltpu
from jax.sharding import PartitionSpec as P

NOPE = 128
ROPE = 64
VDIM = 128
KVR = 256
CH = 1024
GROUPS = 8
GRID_W = 64


norm_eps = 1e-06
rope_base = 10000.0
far_below = -1e30


def padded_2(block, sides, width):
    for axis, dim in sides:
        count = lax.axis_size(axis)
        forward = [(i, i + 1) for i in range(count - 1)]
        backward = [(target, source) for source, target in forward]
        low = lax.ppermute(
            lax.slice_in_dim(block, block.shape[dim] - width, None, axis=dim), axis, forward
        )
        high = lax.ppermute(lax.slice_in_dim(block, 0, width, axis=dim), axis, backward)
        block = jnp.concatenate([low, block, high], axis=dim)
    return block


def rms_scale(values, scale_gain):
    inv_rms = lax.rsqrt(jnp.mean(values * values, axis=-1, keepdims=True) + norm_eps)
    return values * inv_rms * scale_gain.astype(jnp.float32)


def angles_for(positions, rope_size):
    quarter = rope_size // 4
    inverse = rope_base ** (-jnp.arange(quarter, dtype=jnp.float32) / quarter)
    grid_row = (positions // GRID_W).astype(jnp.float32)
    grid_col = (positions % GRID_W).astype(jnp.float32)
    return jnp.concatenate([grid_row[:, None] * inverse, grid_col[:, None] * inverse], axis=-1)


def rotate(values, angles):
    half_size = values.shape[-1] // 2
    front_half = values[..., :half_size]
    back_half = values[..., half_size:]
    cosine = jnp.cos(angles)
    sine_part = jnp.sin(angles)
    return jnp.concatenate(
        [front_half * cosine - back_half * sine_part, back_half * cosine + front_half * sine_part],
        axis=-1,
    )


def key_block(normed, latent_down, latent_gain, rope_down, positions):
    latent = jnp.dot(normed, latent_down, preferred_element_type=jnp.float32)
    latent = rms_scale(latent, latent_gain).astype(jnp.bfloat16)
    rope_key = jnp.dot(normed, rope_down, preferred_element_type=jnp.float32)
    rope_key = rotate(rope_key, angles_for(positions, rope_key.shape[-1])).astype(jnp.bfloat16)
    return jnp.concatenate([latent, rope_key], axis=1)


def per_device(
    tokens,
    norm_gain,
    query_down,
    query_gain,
    latent_down,
    latent_gain,
    rope_down,
    query_up,
    key_up,
    value_up,
    glu_value,
    glu_gate,
    conv_taps,
    group_gain,
    head_proj,
    channel_proj,
):
    tok_count = tokens.shape[0]
    reach_rows = conv_taps.shape[0] // 2
    head_count = key_up.shape[1] // NOPE
    normed = rms_scale(tokens.astype(jnp.float32), norm_gain).astype(jnp.bfloat16)
    offsets = lax.axis_index("sp") * tok_count + jnp.arange(tok_count, dtype=jnp.int32)
    query_latent = jnp.dot(
        normed,
        lax.all_gather(query_down, "sp", axis=0, tiled=True),
        preferred_element_type=jnp.float32,
    )
    value_in = jnp.dot(
        normed,
        lax.all_gather(glu_value, "sp", axis=0, tiled=True),
        preferred_element_type=jnp.float32,
    )
    gate_in = jnp.dot(
        normed,
        lax.all_gather(glu_gate, "sp", axis=0, tiled=True),
        preferred_element_type=jnp.float32,
    )
    latent_query = rms_scale(query_latent, query_gain).astype(jnp.bfloat16)
    query_all = jnp.dot(latent_query, query_up, preferred_element_type=jnp.float32).reshape(
        tok_count, head_count, NOPE + ROPE
    )
    query_plain = query_all[:, :, :NOPE].astype(jnp.bfloat16)
    query_rope = rotate(query_all[:, :, NOPE:], angles_for(offsets, ROPE)[:, None, :]).astype(
        jnp.bfloat16
    )
    absorbed = jnp.einsum(
        "thd,rhd->htr",
        query_plain,
        key_up.reshape(KVR, head_count, NOPE),
        preferred_element_type=jnp.float32,
    ).astype(jnp.bfloat16)
    queries = jnp.concatenate([absorbed, jnp.transpose(query_rope, (1, 0, 2))], axis=-1)
    score_scale = (NOPE + ROPE) ** (-0.5)
    half_rows = tok_count // lax.axis_size("tp")
    first_row = lax.axis_index("tp") * half_rows
    own_rows = lax.dynamic_slice_in_dim(normed, first_row, half_rows, 0)
    own_positions = lax.dynamic_slice_in_dim(offsets, first_row, half_rows, 0)
    own_keys = key_block(own_rows, latent_down, latent_gain, rope_down, own_positions)
    block_keys = lax.all_gather(own_keys, ("sp", "tp"), axis=0, tiled=True)
    row_max = jnp.full((head_count, tok_count), far_below, jnp.float32)
    scores = (
        jnp.einsum("hqc,kc->hqk", queries, block_keys, preferred_element_type=jnp.float32)
        * score_scale
    )
    new_max = jnp.maximum(row_max, jnp.max(scores, axis=2))
    weights = jnp.exp(scores - new_max[:, :, None])
    new_sum = jnp.sum(weights, axis=2)
    added = jnp.einsum(
        "hqk,kr->hqr",
        weights.astype(jnp.bfloat16),
        block_keys[:, :KVR],
        preferred_element_type=jnp.float32,
    )
    gated_rows = (value_in * jax.nn.sigmoid(gate_in)).astype(jnp.bfloat16)
    padded = padded_2(gated_rows, (("sp", 0),), reach_rows)
    filtered = padded[0:tok_count].astype(jnp.float32) * conv_taps[0].astype(jnp.float32)
    for tap_index in range(1, conv_taps.shape[0]):
        filtered = filtered + padded[tap_index : tap_index + tok_count].astype(
            jnp.float32
        ) * conv_taps[tap_index].astype(jnp.float32)
    grouped = filtered.reshape(tok_count, -1, CH // GROUPS)
    centred = grouped - jnp.mean(grouped, axis=-1, keepdims=True)
    spread = jnp.mean(centred * centred, axis=-1, keepdims=True)
    normal_groups = (centred * lax.rsqrt(spread + norm_eps)).reshape(tok_count, -1)
    conv_branch = jax.nn.silu(normal_groups * group_gain.astype(jnp.float32)).astype(jnp.bfloat16)
    attended = (added / new_sum[:, :, None]).astype(jnp.bfloat16)
    log_weight = new_max + jnp.log(new_sum)
    head_out = jnp.einsum(
        "htr,rhv->thv",
        attended,
        value_up.reshape(KVR, head_count, VDIM),
        preferred_element_type=jnp.float32,
    )
    head_out = head_out.reshape(tok_count, head_count * VDIM).astype(jnp.bfloat16)
    mixed_in = jnp.concatenate([head_out, conv_branch], axis=1)
    out_weight = jnp.concatenate([head_proj, channel_proj], axis=0)
    partial_terms = jnp.dot(
        mixed_in,
        lax.all_gather(out_weight, "sp", axis=1, tiled=True),
        preferred_element_type=jnp.float32,
    )
    mixed_out = lax.psum_scatter(
        partial_terms.astype(jnp.bfloat16), "tp", scatter_dimension=1, tiled=True
    )
    return (mixed_out, log_weight)


LANES = 128
MESH = pl.DeviceIdType.MESH
F32 = jnp.float32
BF16 = jnp.bfloat16
Q, K, H, C, G = range(5)
PIECES = 4
RING = 32


def rope_tables(length):
    quarter = ROPE // 4
    inverse = np.float32(rope_base) ** (-np.arange(quarter, dtype=np.float32) / np.float32(quarter))
    positions = np.arange(length)
    row = (positions // GRID_W).astype(np.float32)[:, None] * inverse
    col = (positions % GRID_W).astype(np.float32)[:, None] * inverse
    angles = np.concatenate([row, col], axis=1).astype(np.float32)
    cosine, sine = np.cos(angles), np.sin(angles)
    tables = np.zeros((3, length, LANES), np.float32)
    half = ROPE // 2
    tables[0, :, :half] = cosine
    tables[0, :, half:ROPE] = cosine
    tables[1, :, :half] = -sine
    tables[2, :, half:ROPE] = sine
    return tables


def dot(a, b):
    return jnp.dot(a, b, preferred_element_type=F32)


def row_of(ref):
    return ref[...].reshape(1, -1)


def dot_nt(a, b):
    return lax.dot_general(a, b, (((1,), (1,)), ((), ())), preferred_element_type=F32)


def fused_kernel(
    n_sp,
    tokens, norm_gain_in, query_down, query_gain_in, latent_down, latent_gain_in, rope_down, query_up,
    key_up, value_up, glu_value, glu_gate, taps_in, group_gain_in, head_proj, channel_proj, tables,
    placed, log_out,
    norm_gain, query_gain, latent_gain, conv_taps, group_gain, log_v,
    w_q, w_g, w_o, tok_v, lat_v, rope_v, qup_v, kup_v, vup_v, tab_v,
    normed, keys, key_tmp, q_out, q_lat, q_scr, g_acc, gated, low_rows, high_rows, padded,
    mixed, parts, w_full, mixed_o, part_o,
    load_sem, ring_sem, z_recv, pair_recv, n_recv, np_recv, q_recv, head_recv, halo_recv, halo_send,
    conv_recv, fin_recv, out_sem, up_recv, back_recv, back_send, nr_recv, hr_recv, cr_recv, corner_recv,
):
    z = lax.axis_index("sp")
    c = lax.axis_index("fs")
    t = lax.axis_index("tp")
    peer = 1 - t
    c_x = c + 1 - 2 * (c % 2)
    c_y = (c + 2) % 4
    c_d = 3 - c
    others = (c_x, c_y, c_d)
    n_fs = normed.shape[0]
    n_tp = 2
    rows, width = tokens.shape
    depth, q_cols = w_q.shape[1:]
    cols = w_g.shape[2] // 2
    heads = key_up.shape[1] // NOPE
    head_rows = head_proj.shape[0]
    out_rows, out_cols = w_o.shape[1:]
    half_width = width // n_tp
    per_core = n_fs // n_tp
    half_sp = n_sp // n_tp

    def lanes_at(index, size):
        return pl.ds(pl.multiple_of(index * size, LANES), size)

    barrier = pltpu.get_barrier_semaphore()
    sides = [{"fs": c_x}, {"fs": c_y}, {"tp": peer}]
    for partner in sides:
        pl.semaphore_signal(barrier, inc=1, device_id=partner, device_id_type=MESH)

    @pl.when(z > 0)
    def _():
        pl.semaphore_signal(barrier, inc=1, device_id={"sp": z - 1}, device_id_type=MESH)

    @pl.when(z < n_sp - 1)
    def _():
        pl.semaphore_signal(barrier, inc=1, device_id={"sp": z + 1}, device_id_type=MESH)

    loads = {}

    def load(name, slot, src, dst):
        copy = pltpu.make_async_copy(src, dst, load_sem.at[slot])
        copy.start()
        loads[name] = copy

    load("tok", 0, tokens, tok_v)
    load("ng", 1, norm_gain_in, norm_gain)
    load("wq", 2, query_down.at[:, lanes_at(c, q_cols)], w_q.at[z])
    load("wv", 3, glu_value.at[:, lanes_at(c, cols)], w_g.at[z, :, pl.ds(0, cols)])
    load("wt", 4, glu_gate.at[:, lanes_at(c, cols)], w_g.at[z, :, pl.ds(cols, cols)])
    load("lat", 5, latent_down, lat_v)
    load("rope", 6, rope_down, rope_v)
    load("tab", 7, tables.at[:, pl.ds(pl.multiple_of(z * rows, LANES), rows), :], tab_v)
    load("lg", 8, latent_gain_in, latent_gain)

    def load_rest():
        load("hp", 0, head_proj.at[:, lanes_at(c, out_cols)], w_o.at[z, pl.ds(0, head_rows), :])
        load("cp", 1, channel_proj.at[:, lanes_at(c, out_cols)], w_o.at[z, pl.ds(head_rows, out_rows - head_rows), :])
        load("qup", 2, query_up, qup_v)
        load("kup", 3, key_up, kup_v)
        load("vup", 4, value_up, vup_v)
        load("qg", 5, query_gain_in, query_gain)
        load("taps", 6, taps_in.at[:, lanes_at(c, cols)], conv_taps)
        load("gg", 7, group_gain_in, group_gain)
        load("hf", 8, head_proj, w_full.at[pl.ds(0, head_rows), :])
        load("cf", 9, channel_proj, w_full.at[pl.ds(head_rows, out_rows - head_rows), :])

    loads["tok"].wait()
    loads["ng"].wait()
    values = tok_v[...].astype(F32)
    normed[c] = rms_scale(values, row_of(norm_gain)).astype(BF16)
    for name in ("wq", "wv", "wt"):
        loads[name].wait()

    ends = (z == 0).astype(jnp.int32) + (z == n_sp - 1).astype(jnp.int32)
    pl.semaphore_wait(barrier, len(sides) + 2 - ends)

    sent = []

    def when(cond, action):
        if cond is None:
            action()
        else:
            pl.when(cond)(action)

    def both(first, second):
        return second if first is None else first & second

    def remote(src, dst, recv_sem, device):
        def make(send_sem):
            return pltpu.make_async_remote_copy(
                src_ref=src, dst_ref=dst, send_sem=send_sem, recv_sem=recv_sem,
                device_id=device, device_id_type=MESH,
            )

        return make

    def drain(entry):
        copy, cond = entry
        when(cond, copy.wait_send)

    def send(make, cond=None):
        slot = len(sent) % RING
        if len(sent) >= RING:
            drain(sent[-RING])
        copy = make(ring_sem.at[slot])
        when(cond, copy.start)
        sent.append((copy, cond))

    def arrive(make):
        make(ring_sem.at[0]).wait_recv()

    q_half = depth // n_tp
    piece = depth // PIECES
    k_half = rows // n_tp
    inner = (z > 0) & (z < n_sp - 1)
    at_end = jnp.logical_not(inner)
    lower = 2 * z < n_sp
    outer = jnp.where(lower, 0, n_sp - 1)
    near = jnp.where(lower, 1, n_sp - 2)
    far = jnp.where(lower, n_sp - 2, 1)
    neighbour = jnp.where(lower, z + 1, z - 1)

    def half(first, size):
        return pl.ds(pl.multiple_of(first * size, 16), size)

    def block(u, shard, side=t):
        if u == Q:
            return w_q.at[shard, half(side, q_half), :]
        if u == K:
            return keys.at[shard, half(side, k_half), :]
        if u == H:
            return w_o.at[shard, pl.ds(0, head_rows), :]
        if u == C:
            return w_o.at[shard, pl.ds(head_rows, out_rows - head_rows), :]
        return w_g.at[shard, pl.ds((u - G) * piece, piece), :]

    def slot_of(shard, at):
        return shard - (shard > at).astype(jnp.int32)

    def z_copy(u, shard, target):
        ref = block(u, shard)
        return remote(ref, ref, z_recv.at[u, slot_of(shard, target)], {"sp": target})

    def z_arrive(u, shard):
        ref = block(u, shard)
        arrive(remote(ref, ref, z_recv.at[u, slot_of(shard, z)], {"sp": neighbour}))

    def send_own(u, cond=None):
        skip = 1 if u in (H, C) else 0
        send(z_copy(u, z, z - 1), both(cond, z > skip))
        send(z_copy(u, z, z + 1), both(cond, z < n_sp - 1 - skip))

    nearest = jnp.minimum(z, n_sp - 1 - z)
    arrivals = []
    for k in range(n_sp - 1):
        two_sided = k < 2 * nearest
        distance = jnp.where(two_sided, k // 2 + 1, k - nearest + 1)
        from_low = jnp.where(two_sided, 1 - k % 2, (2 * z > n_sp - 1).astype(jnp.int32))
        arrivals.append((z - distance * (2 * from_low - 1), z + 2 * from_low - 1))

    def pass_on(u, shard, target):
        when(inner, lambda: z_arrive(u, shard))
        send(z_copy(u, shard, target), inner)

    def relay(u, k):
        pass_on(u, *arrivals[k])

    def settle(u, k):
        when(at_end, lambda: z_arrive(u, arrivals[k][0]))

    def pair(u, shard, side):
        ref = block(u, shard, side)
        return remote(ref, ref, pair_recv.at[u, slot_of(shard, z)], {"tp": peer})

    def share(u, k):
        settle(u, k)
        send(pair(u, arrivals[k][0], t))

    quarter_width = half_width // 2

    def n_block(owner, part):
        return normed.at[owner, :, lanes_at(2 * t + part, quarter_width)]

    def n_copy(i, part):
        ref = n_block(c, part)
        return remote(ref, ref, n_recv.at[i, part], {"fs": others[i]})

    def n_relay(i):
        ref = n_block(others[i], i)
        return remote(ref, ref, nr_recv.at[i], {"fs": others[1 - i]})

    def n_pair(i, side):
        ref = normed.at[others[i], :, lanes_at(side, half_width)]
        return remote(ref, ref, np_recv.at[i], {"tp": peer})

    def pass_normed(i):
        arrive(n_copy(i, i))
        send(n_relay(i))

    def share_normed(i):
        if i < 2:
            arrive(n_copy(i, 1 - i))
        else:
            for j in range(2):
                arrive(n_relay(j))
        send(n_pair(i, t))

    send_own(Q)
    for part in range(2):
        send(n_copy(0, part))
        send(n_copy(1, 1 - part))

    def rotate_lanes(v):
        step = ROPE // 2
        return (
            v * tab_v[0] + pltpu.roll(v, LANES - step, 1) * tab_v[1] + pltpu.roll(v, step, 1) * tab_v[2]
        )

    loads["lat"].wait()
    loads["lg"].wait()
    own_normed = normed[c]
    latent = rms_scale(dot(own_normed, lat_v[...]), row_of(latent_gain))
    keys[z, :, 0:KVR] = latent.astype(BF16)
    loads["rope"].wait()
    loads["tab"].wait()
    key_tmp[...] = jnp.zeros_like(key_tmp)
    key_tmp[:, 0:ROPE] = dot_nt(own_normed, rope_v[...])
    keys[z, :, KVR : KVR + LANES] = rotate_lanes(key_tmp[...]).astype(BF16)
    send_own(K)
    send_own(G)
    load_rest()

    last = n_sp - 2
    for k in range(last):
        relay(Q, k)
    send_own(G + 1)
    pass_normed(0)
    pass_normed(1)
    for k in range(last):
        relay(K, k)
    share(Q, 0)
    relay(Q, last)
    for p in range(2, PIECES):
        send_own(G + p)
    for k in range(last):
        relay(G, k)
    share_normed(0)
    share_normed(1)
    relay(K, last)
    for k in range(last):
        relay(G + 1, k)
    for k in range(1, last):
        share(Q, k)
    share_normed(2)
    share(Q, last)
    for p in range(2, PIECES):
        for k in range(last):
            relay(G + p, k)

    for i in range(len(others)):
        arrive(n_pair(i, peer))
    for k in range(n_sp - 1):
        arrive(pair(Q, arrivals[k][0], peer))
    seqs = normed[pl.ds(per_core * t, per_core)].reshape(per_core * rows, width)
    q_out[...] = dot(seqs, w_q[...].reshape(n_sp * depth, q_cols)).reshape(per_core, rows, q_cols)

    for i in range(per_core):
        seq = per_core * t + i
        for core in (peer, t):
            copy = remote(q_out.at[i], q_lat.at[c], q_recv.at[c], {"fs": seq, "tp": core})
            send(copy, None if core is peer else seq != c)

        @pl.when(seq == c)
        def _():
            q_lat[c] = q_out[i]

    for name in ("hp", "cp"):
        loads[name].wait()
    for u in (H, C):
        send_own(u, at_end)

    def add_shard(shard, first=False):
        rows_in = normed[:, :, lanes_at(shard, depth)].reshape(n_fs * rows, depth)
        term = dot(rows_in, w_g[shard])
        g_acc[...] = term if first else g_acc[...] + term

    halo = low_rows.shape[1]
    up_copy = remote(
        gated.at[:, pl.ds(rows - halo, halo), :], low_rows, halo_recv.at[0], {"sp": z + 1}
    )(halo_send.at[0])
    down_copy = remote(
        gated.at[:, pl.ds(0, halo), :], high_rows, halo_recv.at[1], {"sp": z - 1}
    )(halo_send.at[1])

    def gate():
        for k in range(n_sp - 1):
            for p in range(PIECES):
                settle(G + p, k)
            add_shard(arrivals[k][0])
        acc = g_acc[...]
        gated[...] = (acc[:, 0:cols] * jax.nn.sigmoid(acc[:, cols : 2 * cols])).astype(BF16).reshape(n_fs, rows, cols)

        @pl.when(z < n_sp - 1)
        def _():
            up_copy.start()

        @pl.when(z > 0)
        def _():
            down_copy.start()

    for p in range(2):
        relay(G + p, last)
    for k in range(last):
        share(K, k)
    add_shard(z, True)
    for p in range(2, PIECES):
        relay(G + p, last)
    share(K, last)

    @pl.when(inner)
    def _():
        gate()

    for u in (H, C):
        send_own(u, inner)
    for name in ("qup", "kup", "vup", "qg", "taps", "gg"):
        loads[name].wait()

    for source in range(n_fs):
        @pl.when((c != source) | (t != c // per_core))
        def _():
            arrive(remote(q_out.at[0], q_lat.at[source], q_recv.at[source], {"tp": peer}))

    pass_on(H, outer, far)
    whole_q = jnp.concatenate([q_lat[i] for i in range(n_fs)], axis=1)
    latent_query = rms_scale(whole_q, row_of(query_gain)).astype(BF16)
    q_scr[...] = dot(latent_query, qup_v[...])
    for k in range(n_sp - 1):
        arrive(pair(K, arrivals[k][0], peer))

    def attend(h, shifted):
        start = h * (NOPE + ROPE)
        source = q_scr[...]
        if start % LANES:
            source, start = shifted, start - ROPE
        plain = source[:, start : start + NOPE].astype(BF16)
        rope_part = rotate_lanes(source[:, start + NOPE : start + NOPE + LANES]).astype(BF16)
        absorbed = dot_nt(plain, kup_v[:, h * NOPE : (h + 1) * NOPE]).astype(BF16)
        query = jnp.concatenate([absorbed, rope_part], axis=1)
        all_keys = keys[...].reshape(n_sp * rows, KVR + LANES)
        scores = dot_nt(query, all_keys) * (NOPE + ROPE) ** (-0.5)
        row_max = jnp.max(scores, axis=1, keepdims=True)
        weights = jnp.exp(scores - row_max)
        total = jnp.sum(weights, axis=1, keepdims=True)
        added = dot(weights.astype(BF16), all_keys[:, 0:KVR])
        attended = (added / total).astype(BF16)
        head_out = dot(attended, vup_v[:, h * VDIM : (h + 1) * VDIM])
        mixed[c, :, h * VDIM : (h + 1) * VDIM] = head_out.astype(BF16)
        return row_max + jnp.log(total)

    def head_copy(h, i):
        ref = mixed.at[c, :, pl.ds(h * VDIM, VDIM)]
        return remote(ref, ref, head_recv.at[h, i], {"fs": others[i]})

    def head_relay(h):
        i = h * 2 // heads
        ref = mixed.at[others[i], :, pl.ds(h * VDIM, VDIM)]
        return i, remote(ref, ref, hr_recv.at[h], {"fs": others[1 - i]})

    def pass_head(h):
        i, copy = head_relay(h)
        arrive(head_copy(h, i))
        send(copy)

    whole = q_scr[...]
    shifted = pltpu.roll(whole, whole.shape[1] - ROPE, 1)
    lane = lax.broadcasted_iota(jnp.int32, (rows, LANES), 1)
    logs = jnp.zeros((rows, LANES), F32)

    def to_near(group):
        ref = mixed.at[c, :, lanes_at(group, cols)]
        return remote(ref, mixed_o.at[:, lanes_at(group, cols)], up_recv.at[group], {"sp": near})

    for h in range(heads):
        logs = jnp.where(lane == h, attend(h, shifted), logs)
        for i in range(2):
            send(head_copy(h, i))
        send(to_near(h), at_end)
        if h == 0:
            pass_on(C, outer, far)
    log_v[...] = jnp.transpose(logs)[0:heads, :]
    log_copy = pltpu.make_async_copy(log_v, log_out, out_sem.at[0])
    log_copy.start()
    pass_on(H, far, outer)
    for h in range(heads):
        pass_head(h)
    pass_on(C, far, outer)

    @pl.when(at_end)
    def _():
        gate()

    reach = conv_taps.shape[0] // 2
    padded[:, halo : halo + rows, :] = gated[...].astype(F32)

    @pl.when(z > 0)
    def _():
        up_copy.wait_recv()
        padded[:, 0:halo, :] = low_rows[...].astype(F32)

    @pl.when(z == 0)
    def _():
        padded[:, 0:halo, :] = jnp.zeros((n_fs, halo, cols), F32)

    @pl.when(z < n_sp - 1)
    def _():
        down_copy.wait_recv()
        padded[:, halo + rows : 2 * halo + rows, :] = high_rows[...].astype(F32)

    @pl.when(z == n_sp - 1)
    def _():
        padded[:, halo + rows : 2 * halo + rows, :] = jnp.zeros((n_fs, halo, cols), F32)

    def conv_ref(s, group):
        return mixed.at[s, :, pl.ds(pl.multiple_of(head_rows + group * cols, LANES), cols)]

    def conv_copy(s, i):
        ref = conv_ref(s, c)
        return remote(ref, ref, conv_recv.at[s, i], {"fs": others[i]})

    def conv_corner():
        ref = conv_ref(c_d, c)
        return remote(ref, ref, corner_recv.at[0], {"fs": c_d})

    def conv_corner_in():
        ref = conv_ref(c, c_d)
        return remote(ref, ref, corner_recv.at[0], {"fs": c_d})

    def conv_relay(s, i):
        ref = conv_ref(s, others[i])
        return remote(ref, ref, cr_recv.at[s], {"fs": others[1 - i]})

    taps = conv_taps[...].astype(F32)
    all_gains = row_of(group_gain).astype(F32)
    gains = all_gains[:, 0:cols]
    for i in range(1, n_fs):
        gains = jnp.where(c == i, all_gains[:, i * cols : (i + 1) * cols], gains)
    relay(H, last)

    def conv_seq(s):
        filtered = jnp.zeros((rows, cols), F32)
        for j in range(conv_taps.shape[0]):
            first = halo - reach + j
            filtered = filtered + padded[s, first : first + rows, :] * taps[j : j + 1, :]
        centred = filtered - jnp.mean(filtered, axis=1, keepdims=True)
        spread = jnp.mean(centred * centred, axis=1, keepdims=True)
        branch = centred * lax.rsqrt(spread + norm_eps) * gains
        branch = branch * jax.nn.sigmoid(branch)
        mixed[s, :, pl.ds(pl.multiple_of(head_rows + c * cols, LANES), cols)] = branch.astype(BF16)

    conv_seq(c_d)
    send(conv_corner())
    conv_seq(c_x)
    send(conv_copy(c_x, 0))
    conv_seq(c_y)
    send(conv_copy(c_y, 1))
    conv_seq(c)
    send(to_near(heads + c), at_end)
    for s, i in ((c, 0), (c_d, 1), (c_y, 0), (c, 1), (c_d, 0), (c_x, 1)):
        send(conv_copy(s, i))
    arrive(conv_copy(c, 0))
    send(to_near(heads + c_x), at_end)
    arrive(conv_copy(c, 1))
    send(to_near(heads + c_y), at_end)
    send(conv_relay(c, 1))
    arrive(conv_corner_in())
    send(to_near(heads + c_d), at_end)
    relay(C, last)
    for s, i in ((c_x, 0), (c_d, 1)):
        arrive(conv_copy(s, i))
        send(conv_relay(s, i))

    back_lanes = lanes_at(z % half_sp, n_fs * out_cols)
    back_copy = remote(
        part_o, placed.at[t, :, back_lanes], back_recv.at[t], {"sp": outer, "tp": z // half_sp}
    )(back_send.at[0])
    for name in ("hf", "cf"):
        loads[name].wait()

    def neighbour_part():
        for i in range(heads + n_fs):
            arrive(to_near(i))
        part_o[...] = dot(mixed_o[...], w_full[...]).astype(BF16)
        back_copy.start()

    @pl.when(inner)
    def _():
        neighbour_part()

    for h in range(heads):
        arrive(head_copy(h, 1 - head_relay(h)[0]))
        arrive(head_relay(h)[1])
    for s, i in ((c_y, 1), (c_d, 0), (c_x, 1), (c_y, 0)):
        arrive(conv_copy(s, i))
    for s in others:
        arrive(conv_relay(s, 0))

    def place(core, shard):
        first = (shard % half_sp) * (n_fs * out_cols) + c * out_cols
        return placed.at[core, :, pl.ds(pl.multiple_of(first, LANES), out_cols)]

    def fin_copy(shard, j):
        seq = others[j] if j < len(others) else c
        return remote(
            parts.at[shard, pl.ds(pl.multiple_of(seq * rows, LANES), rows), :], place(t, shard),
            fin_recv.at[t, shard % half_sp, j], {"fs": seq, "tp": shard // half_sp},
        )

    def keep_copy(shard):
        ref = parts.at[shard, pl.ds(pl.multiple_of(c * rows, LANES), rows), :]
        return pltpu.make_async_copy(ref, place(t, shard), out_sem.at[1 + shard % half_sp])

    def add_part(shard, between, cond=None):
        def compute():
            part = dot(mixed[:, :, 0:head_rows].reshape(n_fs * rows, head_rows), w_o[shard, 0:head_rows, :])
            between()
            part = part + dot(
                mixed[:, :, head_rows:out_rows].reshape(n_fs * rows, out_rows - head_rows), w_o[shard, head_rows:out_rows, :]
            )
            parts[shard] = part.astype(BF16)

        when(cond, compute)
        for j in (2, 0, 1):
            send(fin_copy(shard, j), cond)
        mine = shard // half_sp == t
        send(fin_copy(shard, len(others)), both(cond, jnp.logical_not(mine)))
        when(both(cond, mine), lambda: keep_copy(shard).start())

    add_part(z, lambda: None)
    add_part(arrivals[0][0], lambda: None, inner)
    for k in range(1, n_sp - 1):
        settle(H, k)
        add_part(arrivals[k][0], functools.partial(settle, C, k))

    for entry in sent[-RING:]:
        drain(entry)

    @pl.when(z < n_sp - 1)
    def _():
        up_copy.wait_send()

    @pl.when(z > 0)
    def _():
        down_copy.wait_send()

    @pl.when(inner)
    def _():
        back_copy.wait_send()

    for i in range(half_sp):
        shard = t * half_sp + i
        computed = inner | (shard != near)

        def arrived(core, j):
            arrive(remote(parts.at[0, pl.ds(0, rows), :], place(0, i), fin_recv.at[core, i, j], {"tp": peer}))

        @pl.when(computed)
        def _():
            for core in range(n_tp):
                for j in range(len(others)):
                    arrived(core, j)
            arrived(peer, len(others))
            keep_copy(shard).wait()

        @pl.when(jnp.logical_not(computed))
        def _():
            for core in range(n_tp):
                arrive(remote(part_o, placed.at[0, :, lanes_at(i, n_fs * out_cols)], back_recv.at[core], {"tp": peer}))
    log_copy.wait()


def finish_kernel(placed, log_in, out, log_out):
    out[...] = (placed[0].astype(F32) + placed[1].astype(F32)).astype(BF16)
    log_out[...] = log_in[...]


def fused_device(n_sp, n_fs, *args):
    (tokens, norm_gain, query_down, query_gain, latent_down, latent_gain, rope_down, query_up,
     key_up, value_up, glu_value, glu_gate, conv_taps, group_gain, head_proj, channel_proj) = args
    rows, width = tokens.shape
    depth, q_rank = query_down.shape
    cols = glu_value.shape[1] // n_fs
    heads = key_up.shape[1] // NOPE
    out_rows = head_proj.shape[0] + channel_proj.shape[0]
    out_cols = head_proj.shape[1] // n_fs
    q_cols = q_rank // n_fs
    halo = (conv_taps.shape[0] // 2 + 15) // 16 * 16
    tables = jnp.asarray(rope_tables(n_sp * rows))
    hbm = pl.BlockSpec(memory_space=pltpu.HBM)
    operands = [
        tokens, norm_gain, query_down, query_gain, latent_down, latent_gain, rope_down.T, query_up,
        key_up, value_up, glu_value, glu_gate, conv_taps, group_gain, head_proj, channel_proj, tables,
    ]
    like = lambda a: pltpu.VMEM(a.shape, a.dtype)
    dma = pltpu.SemaphoreType.DMA
    half_sp = n_sp // 2
    scratch = [
        like(norm_gain), like(query_gain), like(latent_gain), pltpu.VMEM((conv_taps.shape[0], cols), BF16), like(group_gain),
        pltpu.VMEM((heads, rows), F32),
        pltpu.VMEM((n_sp, depth, q_cols), BF16),
        pltpu.VMEM((n_sp, depth, 2 * cols), BF16),
        pltpu.VMEM((n_sp, out_rows, out_cols), BF16),
        like(tokens), like(latent_down), pltpu.VMEM(rope_down.shape[::-1], BF16), like(query_up), like(key_up), like(value_up),
        pltpu.VMEM((3, rows, LANES), F32),
        pltpu.VMEM((n_fs, rows, width), BF16),
        pltpu.VMEM((n_sp, rows, KVR + LANES), BF16),
        pltpu.VMEM((rows, LANES), F32),
        pltpu.VMEM((n_fs // 2, rows, q_cols), F32),
        pltpu.VMEM((n_fs, rows, q_cols), F32),
        pltpu.VMEM((rows, query_up.shape[1]), F32),
        pltpu.VMEM((n_fs * rows, 2 * cols), F32),
        pltpu.VMEM((n_fs, rows, cols), BF16),
        pltpu.VMEM((n_fs, halo, cols), BF16),
        pltpu.VMEM((n_fs, halo, cols), BF16),
        pltpu.VMEM((n_fs, rows + 2 * halo, cols), F32),
        pltpu.VMEM((n_fs, rows, out_rows), BF16),
        pltpu.VMEM((n_sp, n_fs * rows, out_cols), BF16),
        pltpu.VMEM((out_rows, n_fs * out_cols), BF16),
        pltpu.VMEM((rows, out_rows), BF16),
        pltpu.VMEM((rows, n_fs * out_cols), BF16),
        dma((10,)), dma((RING,)), dma((G + PIECES, n_sp - 1)), dma((2, n_sp - 1)), dma((2, 2)), dma((3,)), dma((n_fs,)),
        dma((heads, 2)), dma((2,)), dma((2,)), dma((n_fs, 2)), dma((2, half_sp, 4)), dma((1 + half_sp,)),
        dma((heads + n_fs,)), dma((2,)), dma((1,)), dma((2,)), dma((heads,)), dma((n_fs,)), dma((1,)),
    ]
    shapes = (
        jax.ShapeDtypeStruct((rows, half_sp * n_fs * out_cols), BF16),
        jax.ShapeDtypeStruct((heads, rows), F32),
    )
    placed, logs = pl.pallas_call(
        functools.partial(fused_kernel, n_sp),
        out_shape=(jax.ShapeDtypeStruct((2,) + shapes[0].shape, BF16), shapes[1]),
        in_specs=[hbm] * len(operands),
        out_specs=(hbm, hbm),
        scratch_shapes=scratch,
        compiler_params=pltpu.CompilerParams(
            collective_id=0, has_side_effects=True, vmem_limit_bytes=63 * 1024 * 1024
        ),
        name="fused_layer",
    )(*operands)
    return pl.pallas_call(finish_kernel, out_shape=shapes, name="finish")(placed, logs)


def solution(mesh):
    in_specs = (
        P(("fs", "sp"), None),
        P(),
        P("sp", None),
        P(),
        P(),
        P(),
        P(),
        P(None, "tp"),
        P(None, "tp"),
        P(None, "tp"),
        P("sp", "tp"),
        P("sp", "tp"),
        P(None, "tp"),
        P("tp"),
        P("tp", "sp"),
        P("tp", "sp"),
    )
    out_specs = (P(("fs", "sp"), "tp"), P("tp", ("fs", "sp")))
    body = per_device
    if mesh.shape["fs"] == 4 and mesh.shape["tp"] == 2 and mesh.shape["sp"] == 4:
        body = functools.partial(fused_device, mesh.shape["sp"], mesh.shape["fs"])
    return jax.shard_map(
        body, mesh=mesh, in_specs=in_specs, out_specs=out_specs, check_vma=False
    )
```

```python
import functools

import jax
import jax.numpy as jnp
import numpy as np
from jax import lax
from jax.experimental import pallas as pl
from jax.experimental.pallas import tpu as pltpu
from jax.sharding import PartitionSpec as P

NOPE = 128
ROPE = 64
VDIM = 128
KVR = 256
CH = 1024
GROUPS = 8
GRID_W = 64


norm_eps = 1e-06
rope_base = 10000.0
far_below = -1e30


def padded_2(block, sides, width):
    for axis, dim in sides:
        count = lax.axis_size(axis)
        forward = [(i, i + 1) for i in range(count - 1)]
        backward = [(target, source) for source, target in forward]
        low = lax.ppermute(
            lax.slice_in_dim(block, block.shape[dim] - width, None, axis=dim), axis, forward
        )
        high = lax.ppermute(lax.slice_in_dim(block, 0, width, axis=dim), axis, backward)
        block = jnp.concatenate([low, block, high], axis=dim)
    return block


def rms_scale(values, scale_gain):
    inv_rms = lax.rsqrt(jnp.mean(values * values, axis=-1, keepdims=True) + norm_eps)
    return values * inv_rms * scale_gain.astype(jnp.float32)


def angles_for(positions, rope_size):
    quarter = rope_size // 4
    inverse = rope_base ** (-jnp.arange(quarter, dtype=jnp.float32) / quarter)
    grid_row = (positions // GRID_W).astype(jnp.float32)
    grid_col = (positions % GRID_W).astype(jnp.float32)
    return jnp.concatenate([grid_row[:, None] * inverse, grid_col[:, None] * inverse], axis=-1)


def rotate(values, angles):
    half_size = values.shape[-1] // 2
    front_half = values[..., :half_size]
    back_half = values[..., half_size:]
    cosine = jnp.cos(angles)
    sine_part = jnp.sin(angles)
    return jnp.concatenate(
        [front_half * cosine - back_half * sine_part, back_half * cosine + front_half * sine_part],
        axis=-1,
    )


def key_block(normed, latent_down, latent_gain, rope_down, positions):
    latent = jnp.dot(normed, latent_down, preferred_element_type=jnp.float32)
    latent = rms_scale(latent, latent_gain).astype(jnp.bfloat16)
    rope_key = jnp.dot(normed, rope_down, preferred_element_type=jnp.float32)
    rope_key = rotate(rope_key, angles_for(positions, rope_key.shape[-1])).astype(jnp.bfloat16)
    return jnp.concatenate([latent, rope_key], axis=1)


def per_device(
    tokens,
    norm_gain,
    query_down,
    query_gain,
    latent_down,
    latent_gain,
    rope_down,
    query_up,
    key_up,
    value_up,
    glu_value,
    glu_gate,
    conv_taps,
    group_gain,
    head_proj,
    channel_proj,
):
    tok_count = tokens.shape[0]
    reach_rows = conv_taps.shape[0] // 2
    head_count = key_up.shape[1] // NOPE
    normed = rms_scale(tokens.astype(jnp.float32), norm_gain).astype(jnp.bfloat16)
    offsets = lax.axis_index("sp") * tok_count + jnp.arange(tok_count, dtype=jnp.int32)
    query_latent = jnp.dot(
        normed,
        lax.all_gather(query_down, "sp", axis=0, tiled=True),
        preferred_element_type=jnp.float32,
    )
    value_in = jnp.dot(
        normed,
        lax.all_gather(glu_value, "sp", axis=0, tiled=True),
        preferred_element_type=jnp.float32,
    )
    gate_in = jnp.dot(
        normed,
        lax.all_gather(glu_gate, "sp", axis=0, tiled=True),
        preferred_element_type=jnp.float32,
    )
    latent_query = rms_scale(query_latent, query_gain).astype(jnp.bfloat16)
    query_all = jnp.dot(latent_query, query_up, preferred_element_type=jnp.float32).reshape(
        tok_count, head_count, NOPE + ROPE
    )
    query_plain = query_all[:, :, :NOPE].astype(jnp.bfloat16)
    query_rope = rotate(query_all[:, :, NOPE:], angles_for(offsets, ROPE)[:, None, :]).astype(
        jnp.bfloat16
    )
    absorbed = jnp.einsum(
        "thd,rhd->htr",
        query_plain,
        key_up.reshape(KVR, head_count, NOPE),
        preferred_element_type=jnp.float32,
    ).astype(jnp.bfloat16)
    queries = jnp.concatenate([absorbed, jnp.transpose(query_rope, (1, 0, 2))], axis=-1)
    score_scale = (NOPE + ROPE) ** (-0.5)
    half_rows = tok_count // lax.axis_size("tp")
    first_row = lax.axis_index("tp") * half_rows
    own_rows = lax.dynamic_slice_in_dim(normed, first_row, half_rows, 0)
    own_positions = lax.dynamic_slice_in_dim(offsets, first_row, half_rows, 0)
    own_keys = key_block(own_rows, latent_down, latent_gain, rope_down, own_positions)
    block_keys = lax.all_gather(own_keys, ("sp", "tp"), axis=0, tiled=True)
    row_max = jnp.full((head_count, tok_count), far_below, jnp.float32)
    scores = (
        jnp.einsum("hqc,kc->hqk", queries, block_keys, preferred_element_type=jnp.float32)
        * score_scale
    )
    new_max = jnp.maximum(row_max, jnp.max(scores, axis=2))
    weights = jnp.exp(scores - new_max[:, :, None])
    new_sum = jnp.sum(weights, axis=2)
    added = jnp.einsum(
        "hqk,kr->hqr",
        weights.astype(jnp.bfloat16),
        block_keys[:, :KVR],
        preferred_element_type=jnp.float32,
    )
    gated_rows = (value_in * jax.nn.sigmoid(gate_in)).astype(jnp.bfloat16)
    padded = padded_2(gated_rows, (("sp", 0),), reach_rows)
    filtered = padded[0:tok_count].astype(jnp.float32) * conv_taps[0].astype(jnp.float32)
    for tap_index in range(1, conv_taps.shape[0]):
        filtered = filtered + padded[tap_index : tap_index + tok_count].astype(
            jnp.float32
        ) * conv_taps[tap_index].astype(jnp.float32)
    grouped = filtered.reshape(tok_count, -1, CH // GROUPS)
    centred = grouped - jnp.mean(grouped, axis=-1, keepdims=True)
    spread = jnp.mean(centred * centred, axis=-1, keepdims=True)
    normal_groups = (centred * lax.rsqrt(spread + norm_eps)).reshape(tok_count, -1)
    conv_branch = jax.nn.silu(normal_groups * group_gain.astype(jnp.float32)).astype(jnp.bfloat16)
    attended = (added / new_sum[:, :, None]).astype(jnp.bfloat16)
    log_weight = new_max + jnp.log(new_sum)
    head_out = jnp.einsum(
        "htr,rhv->thv",
        attended,
        value_up.reshape(KVR, head_count, VDIM),
        preferred_element_type=jnp.float32,
    )
    head_out = head_out.reshape(tok_count, head_count * VDIM).astype(jnp.bfloat16)
    mixed_in = jnp.concatenate([head_out, conv_branch], axis=1)
    out_weight = jnp.concatenate([head_proj, channel_proj], axis=0)
    partial_terms = jnp.dot(
        mixed_in,
        lax.all_gather(out_weight, "sp", axis=1, tiled=True),
        preferred_element_type=jnp.float32,
    )
    mixed_out = lax.psum_scatter(
        partial_terms.astype(jnp.bfloat16), "tp", scatter_dimension=1, tiled=True
    )
    return (mixed_out, log_weight)


LANES = 128
MESH = pl.DeviceIdType.MESH
F32 = jnp.float32
BF16 = jnp.bfloat16
Q, K, H, C, G = range(5)
PIECES = 4
RING = 32


def rope_tables(length):
    quarter = ROPE // 4
    inverse = np.float32(rope_base) ** (-np.arange(quarter, dtype=np.float32) / np.float32(quarter))
    positions = np.arange(length)
    row = (positions // GRID_W).astype(np.float32)[:, None] * inverse
    col = (positions % GRID_W).astype(np.float32)[:, None] * inverse
    angles = np.concatenate([row, col], axis=1).astype(np.float32)
    cosine, sine = np.cos(angles), np.sin(angles)
    tables = np.zeros((3, length, LANES), np.float32)
    half = ROPE // 2
    tables[0, :, :half] = cosine
    tables[0, :, half:ROPE] = cosine
    tables[1, :, :half] = -sine
    tables[2, :, half:ROPE] = sine
    return tables


def dot(a, b):
    return jnp.dot(a, b, preferred_element_type=F32)


def row_of(ref):
    return ref[...].reshape(1, -1)


def dot_nt(a, b):
    return lax.dot_general(a, b, (((1,), (1,)), ((), ())), preferred_element_type=F32)


def fused_kernel(
    n_sp,
    tokens, norm_gain_in, query_down, query_gain_in, latent_down, latent_gain_in, rope_down, query_up,
    key_up, value_up, glu_value, glu_gate, taps_in, group_gain_in, head_proj, channel_proj, tables,
    placed, log_out,
    norm_gain, query_gain, latent_gain, conv_taps, group_gain, log_v,
    w_q, w_g, w_o, tok_v, lat_v, rope_v, qup_v, kup_v, vup_v, tab_v,
    normed, keys, key_tmp, q_out, q_lat, q_scr, g_acc, gated, low_rows, high_rows, padded,
    mixed, parts, w_full, mixed_o, part_o, edge_in, head_acc,
    load_sem, ring_sem, z_recv, pair_recv, n_recv, np_recv, q_recv, head_recv, halo_recv, halo_send,
    conv_recv, fin_recv, out_sem, up_recv, back_recv, back_send, nr_recv, hr_recv, cr_recv, corner_recv, edge_recv,
):
    z = lax.axis_index("sp")
    c = lax.axis_index("fs")
    t = lax.axis_index("tp")
    peer = 1 - t
    c_x = c + 1 - 2 * (c % 2)
    c_y = (c + 2) % 4
    c_d = 3 - c
    others = (c_x, c_y, c_d)
    n_fs = normed.shape[0]
    n_tp = 2
    rows, width = tokens.shape
    depth, q_cols = w_q.shape[1:]
    cols = w_g.shape[2] // 2
    heads = key_up.shape[1] // NOPE
    head_rows = head_proj.shape[0]
    out_rows, out_cols = w_o.shape[1:]
    half_width = width // n_tp
    per_core = n_fs // n_tp
    half_sp = n_sp // n_tp

    def lanes_at(index, size):
        return pl.ds(pl.multiple_of(index * size, LANES), size)

    barrier = pltpu.get_barrier_semaphore()
    sides = [{"fs": c_x}, {"fs": c_y}, {"tp": peer}]
    for partner in sides:
        pl.semaphore_signal(barrier, inc=1, device_id=partner, device_id_type=MESH)

    @pl.when(z > 0)
    def _():
        pl.semaphore_signal(barrier, inc=1, device_id={"sp": z - 1}, device_id_type=MESH)

    @pl.when(z < n_sp - 1)
    def _():
        pl.semaphore_signal(barrier, inc=1, device_id={"sp": z + 1}, device_id_type=MESH)

    loads = {}

    def load(name, slot, src, dst):
        copy = pltpu.make_async_copy(src, dst, load_sem.at[slot])
        copy.start()
        loads[name] = copy

    load("tok", 0, tokens, tok_v)
    load("ng", 1, norm_gain_in, norm_gain)
    load("wq", 2, query_down.at[:, lanes_at(c, q_cols)], w_q.at[z])
    load("wv", 3, glu_value.at[:, lanes_at(c, cols)], w_g.at[z, :, pl.ds(0, cols)])
    load("wt", 4, glu_gate.at[:, lanes_at(c, cols)], w_g.at[z, :, pl.ds(cols, cols)])
    load("lat", 5, latent_down, lat_v)
    load("rope", 6, rope_down, rope_v)
    load("tab", 7, tables.at[:, pl.ds(pl.multiple_of(z * rows, LANES), rows), :], tab_v)
    load("lg", 8, latent_gain_in, latent_gain)

    def load_rest():
        load("hp", 0, head_proj.at[:, lanes_at(c, out_cols)], w_o.at[z, pl.ds(0, head_rows), :])
        load("cp", 1, channel_proj.at[:, lanes_at(c, out_cols)], w_o.at[z, pl.ds(head_rows, out_rows - head_rows), :])
        load("qup", 2, query_up, qup_v)
        load("kup", 3, key_up, kup_v)
        load("vup", 4, value_up, vup_v)
        load("qg", 5, query_gain_in, query_gain)
        load("taps", 6, taps_in.at[:, lanes_at(c, cols)], conv_taps)
        load("gg", 7, group_gain_in, group_gain)
        load("hf", 8, head_proj, w_full.at[pl.ds(0, head_rows), :])
        load("cf", 9, channel_proj, w_full.at[pl.ds(head_rows, out_rows - head_rows), :])

    loads["tok"].wait()
    loads["ng"].wait()
    values = tok_v[...].astype(F32)
    normed[c] = rms_scale(values, row_of(norm_gain)).astype(BF16)
    for name in ("wq", "wv", "wt"):
        loads[name].wait()

    ends = (z == 0).astype(jnp.int32) + (z == n_sp - 1).astype(jnp.int32)
    pl.semaphore_wait(barrier, len(sides) + 2 - ends)

    sent = []

    def when(cond, action):
        if cond is None:
            action()
        else:
            pl.when(cond)(action)

    def both(first, second):
        return second if first is None else first & second

    def remote(src, dst, recv_sem, device):
        def make(send_sem):
            return pltpu.make_async_remote_copy(
                src_ref=src, dst_ref=dst, send_sem=send_sem, recv_sem=recv_sem,
                device_id=device, device_id_type=MESH,
            )

        return make

    def drain(entry):
        copy, cond = entry
        when(cond, copy.wait_send)

    def send(make, cond=None):
        slot = len(sent) % RING
        if len(sent) >= RING:
            drain(sent[-RING])
        copy = make(ring_sem.at[slot])
        when(cond, copy.start)
        sent.append((copy, cond))

    def arrive(make):
        make(ring_sem.at[0]).wait_recv()

    q_half = depth // n_tp
    piece = depth // PIECES
    k_half = rows // n_tp
    inner = (z > 0) & (z < n_sp - 1)
    at_end = jnp.logical_not(inner)
    lower = 2 * z < n_sp
    outer = jnp.where(lower, 0, n_sp - 1)
    near = jnp.where(lower, 1, n_sp - 2)
    far = jnp.where(lower, n_sp - 2, 1)
    neighbour = jnp.where(lower, z + 1, z - 1)

    def half(first, size):
        return pl.ds(pl.multiple_of(first * size, 16), size)

    def block(u, shard, side=t):
        if u == Q:
            return w_q.at[shard, half(side, q_half), :]
        if u == K:
            return keys.at[shard, half(side, k_half), :]
        if u == H:
            return w_o.at[shard, pl.ds(0, head_rows), :]
        if u == C:
            return w_o.at[shard, pl.ds(head_rows, out_rows - head_rows), :]
        return w_g.at[shard, pl.ds((u - G) * piece, piece), :]

    def slot_of(shard, at):
        return shard - (shard > at).astype(jnp.int32)

    def z_copy(u, shard, target):
        ref = block(u, shard)
        return remote(ref, ref, z_recv.at[u, slot_of(shard, target)], {"sp": target})

    def z_arrive(u, shard):
        ref = block(u, shard)
        arrive(remote(ref, ref, z_recv.at[u, slot_of(shard, z)], {"sp": neighbour}))

    def send_own(u, cond=None):
        skip = 1 if u in (H, C) else 0
        send(z_copy(u, z, z - 1), both(cond, z > skip))
        send(z_copy(u, z, z + 1), both(cond, z < n_sp - 1 - skip))

    nearest = jnp.minimum(z, n_sp - 1 - z)
    arrivals = []
    for k in range(n_sp - 1):
        two_sided = k < 2 * nearest
        distance = jnp.where(two_sided, k // 2 + 1, k - nearest + 1)
        from_low = jnp.where(two_sided, 1 - k % 2, (2 * z > n_sp - 1).astype(jnp.int32))
        arrivals.append((z - distance * (2 * from_low - 1), z + 2 * from_low - 1))

    def pass_on(u, shard, target):
        when(inner, lambda: z_arrive(u, shard))
        send(z_copy(u, shard, target), inner)

    def relay(u, k):
        pass_on(u, *arrivals[k])

    def settle(u, k):
        when(at_end, lambda: z_arrive(u, arrivals[k][0]))

    def pair(u, shard, side):
        ref = block(u, shard, side)
        return remote(ref, ref, pair_recv.at[u, slot_of(shard, z)], {"tp": peer})

    def share(u, k):
        settle(u, k)
        send(pair(u, arrivals[k][0], t))

    quarter_width = half_width // 2

    def n_block(owner, part):
        return normed.at[owner, :, lanes_at(2 * t + part, quarter_width)]

    def n_copy(i, part):
        ref = n_block(c, part)
        return remote(ref, ref, n_recv.at[i, part], {"fs": others[i]})

    def n_relay(i):
        ref = n_block(others[i], i)
        return remote(ref, ref, nr_recv.at[i], {"fs": others[1 - i]})

    def n_pair(i, side):
        ref = normed.at[others[i], :, lanes_at(side, half_width)]
        return remote(ref, ref, np_recv.at[i], {"tp": peer})

    def pass_normed(i):
        arrive(n_copy(i, i))
        send(n_relay(i))

    def share_normed(i):
        if i < 2:
            arrive(n_copy(i, 1 - i))
        else:
            for j in range(2):
                arrive(n_relay(j))
        send(n_pair(i, t))

    send_own(Q)
    for part in range(2):
        send(n_copy(0, part))
        send(n_copy(1, 1 - part))

    def rotate_lanes(v):
        step = ROPE // 2
        return (
            v * tab_v[0] + pltpu.roll(v, LANES - step, 1) * tab_v[1] + pltpu.roll(v, step, 1) * tab_v[2]
        )

    loads["lat"].wait()
    loads["lg"].wait()
    own_normed = normed[c]
    latent = rms_scale(dot(own_normed, lat_v[...]), row_of(latent_gain))
    keys[z, :, 0:KVR] = latent.astype(BF16)
    loads["rope"].wait()
    loads["tab"].wait()
    key_tmp[...] = jnp.zeros_like(key_tmp)
    key_tmp[:, 0:ROPE] = dot_nt(own_normed, rope_v[...])
    keys[z, :, KVR : KVR + LANES] = rotate_lanes(key_tmp[...]).astype(BF16)
    send_own(K)
    send_own(G)
    load_rest()

    last = n_sp - 2
    for k in range(last):
        relay(Q, k)
    send_own(G + 1)
    pass_normed(0)
    pass_normed(1)
    for k in range(last):
        relay(K, k)
    share(Q, 0)
    send_own(G + 2)
    relay(Q, last)
    send_own(G + 3)
    for k in range(last):
        relay(G, k)
    share_normed(0)
    share_normed(1)
    relay(K, last)
    for k in range(last):
        relay(G + 1, k)
    for k in range(1, last):
        share(Q, k)
    share_normed(2)
    share(Q, last)
    for p in range(2, PIECES):
        for k in range(last):
            relay(G + p, k)

    for i in range(len(others)):
        arrive(n_pair(i, peer))
    halo = low_rows.shape[1]
    edge_rows = pl.ds(pl.multiple_of(jnp.where(lower, rows - halo, 0), 16), halo)
    edge_half = edge_in.at[:, :, lanes_at(t, half_width)]
    edge_copy = remote(normed.at[:, edge_rows, lanes_at(t, half_width)], edge_half, edge_recv.at[0], {"sp": near})
    edge_pair = remote(edge_half, edge_half, edge_recv.at[1], {"tp": peer})
    for k in range(n_sp - 1):
        arrive(pair(Q, arrivals[k][0], peer))
    seqs = normed[pl.ds(per_core * t, per_core)].reshape(per_core * rows, width)
    q_out[...] = dot(seqs, w_q[...].reshape(n_sp * depth, q_cols)).reshape(per_core, rows, q_cols)

    for i in range(per_core):
        seq = per_core * t + i
        for core in (peer, t):
            copy = remote(q_out.at[i], q_lat.at[c], q_recv.at[c], {"fs": seq, "tp": core})
            send(copy, None if core is peer else seq != c)

        @pl.when(seq == c)
        def _():
            q_lat[c] = q_out[i]

    for name in ("hp", "cp"):
        loads[name].wait()
    send_own(H, at_end)
    send(edge_copy, at_end)
    send_own(C, at_end)

    def add_shard(shard, first=False):
        rows_in = normed[:, :, lanes_at(shard, depth)].reshape(n_fs * rows, depth)
        term = dot(rows_in, w_g[shard])
        g_acc[...] = term if first else g_acc[...] + term

    up_copy = remote(
        gated.at[:, pl.ds(rows - halo, halo), :], low_rows, halo_recv.at[0], {"sp": z + 1}
    )(halo_send.at[0])
    down_copy = remote(
        gated.at[:, pl.ds(0, halo), :], high_rows, halo_recv.at[1], {"sp": z - 1}
    )(halo_send.at[1])

    def add_arrival(k):
        for p in range(PIECES):
            settle(G + p, k)
        add_shard(arrivals[k][0])

    def gate():
        gated[...] = gate_of(g_acc[...]).reshape(n_fs, rows, cols)

        @pl.when(inner)
        def _():
            up_copy.start()
            down_copy.start()

    def gate_of(acc):
        return (acc[:, 0:cols] * jax.nn.sigmoid(acc[:, cols : 2 * cols])).astype(BF16)

    def edge():
        arrive(edge_pair)
        acc = dot(edge_in[...].reshape(n_fs * halo, width), w_g[...].reshape(n_sp * depth, 2 * cols))
        values = gate_of(acc).astype(F32).reshape(n_fs, halo, cols)

        @pl.when(lower)
        def _():
            padded[:, 0:halo, :] = values

        @pl.when(jnp.logical_not(lower))
        def _():
            padded[:, halo + rows : 2 * halo + rows, :] = values

    for p in range(2):
        relay(G + p, last)
    for k in range(last):
        share(K, k)
    add_shard(z, True)
    for p in range(2, PIECES):
        relay(G + p, last)
    share(K, last)

    add_arrival(0)

    @pl.when(inner)
    def _():
        for k in range(1, n_sp - 1):
            add_arrival(k)
        gate()

    for u in (H, C):
        send_own(u, inner)
    for name in ("qup", "kup", "vup", "qg", "taps", "gg"):
        loads[name].wait()

    for source in range(n_fs):
        @pl.when((c != source) | (t != c // per_core))
        def _():
            arrive(remote(q_out.at[0], q_lat.at[source], q_recv.at[source], {"tp": peer}))

    pass_on(H, outer, far)
    whole_q = jnp.concatenate([q_lat[i] for i in range(n_fs)], axis=1)
    latent_query = rms_scale(whole_q, row_of(query_gain)).astype(BF16)
    q_scr[...] = dot(latent_query, qup_v[...])
    for k in range(n_sp - 1):
        arrive(pair(K, arrivals[k][0], peer))

    def attend(h, shifted):
        start = h * (NOPE + ROPE)
        source = q_scr[...]
        if start % LANES:
            source, start = shifted, start - ROPE
        plain = source[:, start : start + NOPE].astype(BF16)
        rope_part = rotate_lanes(source[:, start + NOPE : start + NOPE + LANES]).astype(BF16)
        absorbed = dot_nt(plain, kup_v[:, h * NOPE : (h + 1) * NOPE]).astype(BF16)
        query = jnp.concatenate([absorbed, rope_part], axis=1)
        all_keys = keys[...].reshape(n_sp * rows, KVR + LANES)
        scores = dot_nt(query, all_keys) * (NOPE + ROPE) ** (-0.5)
        row_max = jnp.max(scores, axis=1, keepdims=True)
        weights = jnp.exp(scores - row_max)
        total = jnp.sum(weights, axis=1, keepdims=True)
        added = dot(weights.astype(BF16), all_keys[:, 0:KVR])
        attended = (added / total).astype(BF16)
        head_out = dot(attended, vup_v[:, h * VDIM : (h + 1) * VDIM])
        mixed[c, :, h * VDIM : (h + 1) * VDIM] = head_out.astype(BF16)
        return row_max + jnp.log(total)

    def head_copy(h, i):
        ref = mixed.at[c, :, pl.ds(h * VDIM, VDIM)]
        return remote(ref, ref, head_recv.at[h, i], {"fs": others[i]})

    def head_relay(h):
        i = h * 2 // heads
        ref = mixed.at[others[i], :, pl.ds(h * VDIM, VDIM)]
        return i, remote(ref, ref, hr_recv.at[h], {"fs": others[1 - i]})

    def pass_head(h, cond):
        i, copy = head_relay(h)
        when(cond, lambda: arrive(head_copy(h, i)))
        send(copy, cond)

    whole = q_scr[...]
    shifted = pltpu.roll(whole, whole.shape[1] - ROPE, 1)
    lane = lax.broadcasted_iota(jnp.int32, (rows, LANES), 1)
    logs = jnp.zeros((rows, LANES), F32)

    def to_near(group):
        ref = mixed.at[c, :, lanes_at(group, cols)]
        return remote(ref, mixed_o.at[:, lanes_at(group, cols)], up_recv.at[group], {"sp": near})

    for h in range(heads):
        logs = jnp.where(lane == h, attend(h, shifted), logs)
        for i in range(2):
            send(head_copy(h, i))
        send(to_near(h), at_end)
        if h == 1:
            when(inner, lambda: arrive(edge_copy))
            send(edge_pair, inner)
    log_v[...] = jnp.transpose(logs)[0:heads, :]
    log_copy = pltpu.make_async_copy(log_v, log_out, out_sem.at[0])
    log_copy.start()
    pass_on(H, far, outer)

    @pl.when(at_end)
    def _():
        for k in range(1, last):
            add_arrival(k)

    for h in range(heads):
        pass_head(h, at_end)

    @pl.when(at_end)
    def _():
        add_arrival(last)
        gate()

    @pl.when(inner)
    def _():
        edge()

    reach = conv_taps.shape[0] // 2
    padded[:, halo : halo + rows, :] = gated[...].astype(F32)

    @pl.when(z > 1)
    def _():
        up_copy.wait_recv()
        padded[:, 0:halo, :] = low_rows[...].astype(F32)

    @pl.when(z == 0)
    def _():
        padded[:, 0:halo, :] = jnp.zeros((n_fs, halo, cols), F32)

    @pl.when(z < n_sp - 2)
    def _():
        down_copy.wait_recv()
        padded[:, halo + rows : 2 * halo + rows, :] = high_rows[...].astype(F32)

    @pl.when(z == n_sp - 1)
    def _():
        padded[:, halo + rows : 2 * halo + rows, :] = jnp.zeros((n_fs, halo, cols), F32)

    def conv_ref(s, group):
        return mixed.at[s, :, pl.ds(pl.multiple_of(head_rows + group * cols, LANES), cols)]

    def conv_copy(s, i):
        ref = conv_ref(s, c)
        return remote(ref, ref, conv_recv.at[s, i], {"fs": others[i]})

    def conv_corner():
        ref = conv_ref(c_d, c)
        return remote(ref, ref, corner_recv.at[0], {"fs": c_d})

    def conv_corner_in():
        ref = conv_ref(c, c_d)
        return remote(ref, ref, corner_recv.at[0], {"fs": c_d})

    def conv_relay(s, i):
        ref = conv_ref(s, others[i])
        return remote(ref, ref, cr_recv.at[s], {"fs": others[1 - i]})

    taps = conv_taps[...].astype(F32)
    all_gains = row_of(group_gain).astype(F32)
    gains = all_gains[:, 0:cols]
    for i in range(1, n_fs):
        gains = jnp.where(c == i, all_gains[:, i * cols : (i + 1) * cols], gains)
    def conv_seq(s):
        filtered = jnp.zeros((rows, cols), F32)
        for j in range(conv_taps.shape[0]):
            first = halo - reach + j
            filtered = filtered + padded[s, first : first + rows, :] * taps[j : j + 1, :]
        centred = filtered - jnp.mean(filtered, axis=1, keepdims=True)
        spread = jnp.mean(centred * centred, axis=1, keepdims=True)
        branch = centred * lax.rsqrt(spread + norm_eps) * gains
        branch = branch * jax.nn.sigmoid(branch)
        mixed[s, :, pl.ds(pl.multiple_of(head_rows + c * cols, LANES), cols)] = branch.astype(BF16)

    conv_seq(c_d)
    send(conv_corner())
    conv_seq(c_x)
    send(conv_copy(c_x, 0))
    conv_seq(c_y)
    send(conv_copy(c_y, 1))
    conv_seq(c)
    send(to_near(heads + c), at_end)
    for s, i in ((c, 0), (c_d, 1), (c_y, 0), (c, 1), (c_d, 0), (c_x, 1)):
        send(conv_copy(s, i))
    pass_on(C, outer, far)
    pass_on(C, far, outer)
    for h in range(heads):
        pass_head(h, inner)
    relay(H, last)
    arrive(conv_copy(c, 0))
    send(to_near(heads + c_x), at_end)
    arrive(conv_copy(c, 1))
    send(to_near(heads + c_y), at_end)
    send(conv_relay(c, 1))
    arrive(conv_corner_in())
    send(to_near(heads + c_d), at_end)
    for s, i in ((c_x, 0), (c_d, 1)):
        arrive(conv_copy(s, i))
        send(conv_relay(s, i))
    relay(C, last)
    for h in range(heads):
        arrive(head_copy(h, 1 - head_relay(h)[0]))
        arrive(head_relay(h)[1])

    def head_part(shard):
        head_acc[shard] = dot(mixed[:, :, 0:head_rows].reshape(n_fs * rows, head_rows), w_o[shard, 0:head_rows, :])

    head_part(z)
    settle(H, 1)
    head_part(arrivals[1][0])

    @pl.when(inner)
    def _():
        head_part(arrivals[0][0])
        for k in range(2, n_sp - 1):
            head_part(arrivals[k][0])

    for s, i in ((c_y, 1), (c_d, 0), (c_x, 1), (c_y, 0)):
        arrive(conv_copy(s, i))
    for s in others:
        arrive(conv_relay(s, 0))

    def place(core, shard):
        first = (shard % half_sp) * (n_fs * out_cols) + c * out_cols
        return placed.at[core, :, pl.ds(pl.multiple_of(first, LANES), out_cols)]

    def fin_copy(shard, j):
        seq = others[j] if j < len(others) else c
        return remote(
            parts.at[shard, pl.ds(pl.multiple_of(seq * rows, LANES), rows), :], place(t, shard),
            fin_recv.at[t, shard % half_sp, j], {"fs": seq, "tp": shard // half_sp},
        )

    def keep_copy(shard):
        ref = parts.at[shard, pl.ds(pl.multiple_of(c * rows, LANES), rows), :]
        return pltpu.make_async_copy(ref, place(t, shard), out_sem.at[1 + shard % half_sp])

    def add_part(shard, cond=None):
        def compute():
            part = head_acc[shard] + dot(
                mixed[:, :, head_rows:out_rows].reshape(n_fs * rows, out_rows - head_rows), w_o[shard, head_rows:out_rows, :]
            )
            parts[shard] = part.astype(BF16)

        when(cond, compute)
        for j in (2, 0, 1):
            send(fin_copy(shard, j), cond)
        mine = shard // half_sp == t
        send(fin_copy(shard, len(others)), both(cond, jnp.logical_not(mine)))
        when(both(cond, mine), lambda: keep_copy(shard).start())

    add_part(z)
    add_part(arrivals[0][0], inner)
    settle(C, 1)
    add_part(arrivals[1][0])
    for k in range(2, n_sp - 1):
        settle(H, k)

        @pl.when(at_end)
        def _():
            head_part(arrivals[k][0])

        settle(C, k)
        add_part(arrivals[k][0])

    back_lanes = lanes_at(z % half_sp, n_fs * out_cols)
    back_copy = remote(
        part_o, placed.at[t, :, back_lanes], back_recv.at[t], {"sp": outer, "tp": z // half_sp}
    )(back_send.at[0])
    for name in ("hf", "cf"):
        loads[name].wait()

    def neighbour_part():
        for i in range(heads + n_fs):
            arrive(to_near(i))
        part_o[...] = dot(mixed_o[...], w_full[...]).astype(BF16)
        back_copy.start()

    @pl.when(inner)
    def _():
        neighbour_part()

    for entry in sent[-RING:]:
        drain(entry)

    @pl.when(inner)
    def _():
        up_copy.wait_send()
        down_copy.wait_send()
        back_copy.wait_send()

    for i in range(half_sp):
        shard = t * half_sp + i
        computed = inner | (shard != near)

        def arrived(core, j):
            arrive(remote(parts.at[0, pl.ds(0, rows), :], place(0, i), fin_recv.at[core, i, j], {"tp": peer}))

        @pl.when(computed)
        def _():
            for core in range(n_tp):
                for j in range(len(others)):
                    arrived(core, j)
            arrived(peer, len(others))
            keep_copy(shard).wait()

        @pl.when(jnp.logical_not(computed))
        def _():
            for core in range(n_tp):
                arrive(remote(part_o, placed.at[0, :, lanes_at(i, n_fs * out_cols)], back_recv.at[core], {"tp": peer}))
    log_copy.wait()


def finish_kernel(placed, log_in, out, log_out):
    out[...] = (placed[0].astype(F32) + placed[1].astype(F32)).astype(BF16)
    log_out[...] = log_in[...]


def fused_device(n_sp, n_fs, *args):
    (tokens, norm_gain, query_down, query_gain, latent_down, latent_gain, rope_down, query_up,
     key_up, value_up, glu_value, glu_gate, conv_taps, group_gain, head_proj, channel_proj) = args
    rows, width = tokens.shape
    depth, q_rank = query_down.shape
    cols = glu_value.shape[1] // n_fs
    heads = key_up.shape[1] // NOPE
    out_rows = head_proj.shape[0] + channel_proj.shape[0]
    out_cols = head_proj.shape[1] // n_fs
    q_cols = q_rank // n_fs
    halo = (conv_taps.shape[0] // 2 + 15) // 16 * 16
    tables = jnp.asarray(rope_tables(n_sp * rows))
    hbm = pl.BlockSpec(memory_space=pltpu.HBM)
    operands = [
        tokens, norm_gain, query_down, query_gain, latent_down, latent_gain, rope_down.T, query_up,
        key_up, value_up, glu_value, glu_gate, conv_taps, group_gain, head_proj, channel_proj, tables,
    ]
    like = lambda a: pltpu.VMEM(a.shape, a.dtype)
    dma = pltpu.SemaphoreType.DMA
    half_sp = n_sp // 2
    scratch = [
        like(norm_gain), like(query_gain), like(latent_gain), pltpu.VMEM((conv_taps.shape[0], cols), BF16), like(group_gain),
        pltpu.VMEM((heads, rows), F32),
        pltpu.VMEM((n_sp, depth, q_cols), BF16),
        pltpu.VMEM((n_sp, depth, 2 * cols), BF16),
        pltpu.VMEM((n_sp, out_rows, out_cols), BF16),
        like(tokens), like(latent_down), pltpu.VMEM(rope_down.shape[::-1], BF16), like(query_up), like(key_up), like(value_up),
        pltpu.VMEM((3, rows, LANES), F32),
        pltpu.VMEM((n_fs, rows, width), BF16),
        pltpu.VMEM((n_sp, rows, KVR + LANES), BF16),
        pltpu.VMEM((rows, LANES), F32),
        pltpu.VMEM((n_fs // 2, rows, q_cols), F32),
        pltpu.VMEM((n_fs, rows, q_cols), F32),
        pltpu.VMEM((rows, query_up.shape[1]), F32),
        pltpu.VMEM((n_fs * rows, 2 * cols), F32),
        pltpu.VMEM((n_fs, rows, cols), BF16),
        pltpu.VMEM((n_fs, halo, cols), BF16),
        pltpu.VMEM((n_fs, halo, cols), BF16),
        pltpu.VMEM((n_fs, rows + 2 * halo, cols), F32),
        pltpu.VMEM((n_fs, rows, out_rows), BF16),
        pltpu.VMEM((n_sp, n_fs * rows, out_cols), BF16),
        pltpu.VMEM((out_rows, n_fs * out_cols), BF16),
        pltpu.VMEM((rows, out_rows), BF16),
        pltpu.VMEM((rows, n_fs * out_cols), BF16),
        pltpu.VMEM((n_fs, halo, width), BF16),
        pltpu.VMEM((n_sp, n_fs * rows, out_cols), F32),
        dma((10,)), dma((RING,)), dma((G + PIECES, n_sp - 1)), dma((2, n_sp - 1)), dma((2, 2)), dma((3,)), dma((n_fs,)),
        dma((heads, 2)), dma((2,)), dma((2,)), dma((n_fs, 2)), dma((2, half_sp, 4)), dma((1 + half_sp,)),
        dma((heads + n_fs,)), dma((2,)), dma((1,)), dma((2,)), dma((heads,)), dma((n_fs,)), dma((1,)), dma((2,)),
    ]
    shapes = (
        jax.ShapeDtypeStruct((rows, half_sp * n_fs * out_cols), BF16),
        jax.ShapeDtypeStruct((heads, rows), F32),
    )
    placed, logs = pl.pallas_call(
        functools.partial(fused_kernel, n_sp),
        out_shape=(jax.ShapeDtypeStruct((2,) + shapes[0].shape, BF16), shapes[1]),
        in_specs=[hbm] * len(operands),
        out_specs=(hbm, hbm),
        scratch_shapes=scratch,
        compiler_params=pltpu.CompilerParams(
            collective_id=0, has_side_effects=True, vmem_limit_bytes=63 * 1024 * 1024
        ),
        name="fused_layer",
    )(*operands)
    return pl.pallas_call(finish_kernel, out_shape=shapes, name="finish")(placed, logs)


def solution(mesh):
    in_specs = (
        P(("fs", "sp"), None),
        P(),
        P("sp", None),
        P(),
        P(),
        P(),
        P(),
        P(None, "tp"),
        P(None, "tp"),
        P(None, "tp"),
        P("sp", "tp"),
        P("sp", "tp"),
        P(None, "tp"),
        P("tp"),
        P("tp", "sp"),
        P("tp", "sp"),
    )
    out_specs = (P(("fs", "sp"), "tp"), P("tp", ("fs", "sp")))
    body = per_device
    if mesh.shape["fs"] == 4 and mesh.shape["tp"] == 2 and mesh.shape["sp"] == 4:
        body = functools.partial(fused_device, mesh.shape["sp"], mesh.shape["fs"])
    return jax.shard_map(
        body, mesh=mesh, in_specs=in_specs, out_specs=out_specs, check_vma=False
    )
```

```python
import functools

import jax
import jax.numpy as jnp
import numpy as np
from jax import lax
from jax.experimental import pallas as pl
from jax.experimental.pallas import tpu as pltpu
from jax.sharding import PartitionSpec as P

NOPE = 128
ROPE = 64
VDIM = 128
KVR = 256
CH = 1024
GROUPS = 8
GRID_W = 64


norm_eps = 1e-06
rope_base = 10000.0
far_below = -1e30


def padded_2(block, sides, width):
    for axis, dim in sides:
        count = lax.axis_size(axis)
        forward = [(i, i + 1) for i in range(count - 1)]
        backward = [(target, source) for source, target in forward]
        low = lax.ppermute(
            lax.slice_in_dim(block, block.shape[dim] - width, None, axis=dim), axis, forward
        )
        high = lax.ppermute(lax.slice_in_dim(block, 0, width, axis=dim), axis, backward)
        block = jnp.concatenate([low, block, high], axis=dim)
    return block


def rms_scale(values, scale_gain):
    inv_rms = lax.rsqrt(jnp.mean(values * values, axis=-1, keepdims=True) + norm_eps)
    return values * inv_rms * scale_gain.astype(jnp.float32)


def angles_for(positions, rope_size):
    quarter = rope_size // 4
    inverse = rope_base ** (-jnp.arange(quarter, dtype=jnp.float32) / quarter)
    grid_row = (positions // GRID_W).astype(jnp.float32)
    grid_col = (positions % GRID_W).astype(jnp.float32)
    return jnp.concatenate([grid_row[:, None] * inverse, grid_col[:, None] * inverse], axis=-1)


def rotate(values, angles):
    half_size = values.shape[-1] // 2
    front_half = values[..., :half_size]
    back_half = values[..., half_size:]
    cosine = jnp.cos(angles)
    sine_part = jnp.sin(angles)
    return jnp.concatenate(
        [front_half * cosine - back_half * sine_part, back_half * cosine + front_half * sine_part],
        axis=-1,
    )


def key_block(normed, latent_down, latent_gain, rope_down, positions):
    latent = jnp.dot(normed, latent_down, preferred_element_type=jnp.float32)
    latent = rms_scale(latent, latent_gain).astype(jnp.bfloat16)
    rope_key = jnp.dot(normed, rope_down, preferred_element_type=jnp.float32)
    rope_key = rotate(rope_key, angles_for(positions, rope_key.shape[-1])).astype(jnp.bfloat16)
    return jnp.concatenate([latent, rope_key], axis=1)


def per_device(
    tokens,
    norm_gain,
    query_down,
    query_gain,
    latent_down,
    latent_gain,
    rope_down,
    query_up,
    key_up,
    value_up,
    glu_value,
    glu_gate,
    conv_taps,
    group_gain,
    head_proj,
    channel_proj,
):
    tok_count = tokens.shape[0]
    reach_rows = conv_taps.shape[0] // 2
    head_count = key_up.shape[1] // NOPE
    normed = rms_scale(tokens.astype(jnp.float32), norm_gain).astype(jnp.bfloat16)
    offsets = lax.axis_index("sp") * tok_count + jnp.arange(tok_count, dtype=jnp.int32)
    query_latent = jnp.dot(
        normed,
        lax.all_gather(query_down, "sp", axis=0, tiled=True),
        preferred_element_type=jnp.float32,
    )
    value_in = jnp.dot(
        normed,
        lax.all_gather(glu_value, "sp", axis=0, tiled=True),
        preferred_element_type=jnp.float32,
    )
    gate_in = jnp.dot(
        normed,
        lax.all_gather(glu_gate, "sp", axis=0, tiled=True),
        preferred_element_type=jnp.float32,
    )
    latent_query = rms_scale(query_latent, query_gain).astype(jnp.bfloat16)
    query_all = jnp.dot(latent_query, query_up, preferred_element_type=jnp.float32).reshape(
        tok_count, head_count, NOPE + ROPE
    )
    query_plain = query_all[:, :, :NOPE].astype(jnp.bfloat16)
    query_rope = rotate(query_all[:, :, NOPE:], angles_for(offsets, ROPE)[:, None, :]).astype(
        jnp.bfloat16
    )
    absorbed = jnp.einsum(
        "thd,rhd->htr",
        query_plain,
        key_up.reshape(KVR, head_count, NOPE),
        preferred_element_type=jnp.float32,
    ).astype(jnp.bfloat16)
    queries = jnp.concatenate([absorbed, jnp.transpose(query_rope, (1, 0, 2))], axis=-1)
    score_scale = (NOPE + ROPE) ** (-0.5)
    half_rows = tok_count // lax.axis_size("tp")
    first_row = lax.axis_index("tp") * half_rows
    own_rows = lax.dynamic_slice_in_dim(normed, first_row, half_rows, 0)
    own_positions = lax.dynamic_slice_in_dim(offsets, first_row, half_rows, 0)
    own_keys = key_block(own_rows, latent_down, latent_gain, rope_down, own_positions)
    block_keys = lax.all_gather(own_keys, ("sp", "tp"), axis=0, tiled=True)
    row_max = jnp.full((head_count, tok_count), far_below, jnp.float32)
    scores = (
        jnp.einsum("hqc,kc->hqk", queries, block_keys, preferred_element_type=jnp.float32)
        * score_scale
    )
    new_max = jnp.maximum(row_max, jnp.max(scores, axis=2))
    weights = jnp.exp(scores - new_max[:, :, None])
    new_sum = jnp.sum(weights, axis=2)
    added = jnp.einsum(
        "hqk,kr->hqr",
        weights.astype(jnp.bfloat16),
        block_keys[:, :KVR],
        preferred_element_type=jnp.float32,
    )
    gated_rows = (value_in * jax.nn.sigmoid(gate_in)).astype(jnp.bfloat16)
    padded = padded_2(gated_rows, (("sp", 0),), reach_rows)
    filtered = padded[0:tok_count].astype(jnp.float32) * conv_taps[0].astype(jnp.float32)
    for tap_index in range(1, conv_taps.shape[0]):
        filtered = filtered + padded[tap_index : tap_index + tok_count].astype(
            jnp.float32
        ) * conv_taps[tap_index].astype(jnp.float32)
    grouped = filtered.reshape(tok_count, -1, CH // GROUPS)
    centred = grouped - jnp.mean(grouped, axis=-1, keepdims=True)
    spread = jnp.mean(centred * centred, axis=-1, keepdims=True)
    normal_groups = (centred * lax.rsqrt(spread + norm_eps)).reshape(tok_count, -1)
    conv_branch = jax.nn.silu(normal_groups * group_gain.astype(jnp.float32)).astype(jnp.bfloat16)
    attended = (added / new_sum[:, :, None]).astype(jnp.bfloat16)
    log_weight = new_max + jnp.log(new_sum)
    head_out = jnp.einsum(
        "htr,rhv->thv",
        attended,
        value_up.reshape(KVR, head_count, VDIM),
        preferred_element_type=jnp.float32,
    )
    head_out = head_out.reshape(tok_count, head_count * VDIM).astype(jnp.bfloat16)
    mixed_in = jnp.concatenate([head_out, conv_branch], axis=1)
    out_weight = jnp.concatenate([head_proj, channel_proj], axis=0)
    partial_terms = jnp.dot(
        mixed_in,
        lax.all_gather(out_weight, "sp", axis=1, tiled=True),
        preferred_element_type=jnp.float32,
    )
    mixed_out = lax.psum_scatter(
        partial_terms.astype(jnp.bfloat16), "tp", scatter_dimension=1, tiled=True
    )
    return (mixed_out, log_weight)


LANES = 128
MESH = pl.DeviceIdType.MESH
F32 = jnp.float32
BF16 = jnp.bfloat16
Q, K, H, C, G = range(5)
PIECES = 4
RING = 24


def rope_tables(length):
    quarter = ROPE // 4
    inverse = np.float32(rope_base) ** (-np.arange(quarter, dtype=np.float32) / np.float32(quarter))
    positions = np.arange(length)
    row = (positions // GRID_W).astype(np.float32)[:, None] * inverse
    col = (positions % GRID_W).astype(np.float32)[:, None] * inverse
    angles = np.concatenate([row, col], axis=1).astype(np.float32)
    cosine, sine = np.cos(angles), np.sin(angles)
    tables = np.zeros((3, length, LANES), np.float32)
    half = ROPE // 2
    tables[0, :, :half] = cosine
    tables[0, :, half:ROPE] = cosine
    tables[1, :, :half] = -sine
    tables[2, :, half:ROPE] = sine
    return tables


def dot(a, b):
    return jnp.dot(a, b, preferred_element_type=F32)


def row_of(ref):
    return ref[...].reshape(1, -1)


def dot_nt(a, b):
    return lax.dot_general(a, b, (((1,), (1,)), ((), ())), preferred_element_type=F32)


def fused_kernel(
    n_sp,
    tokens, norm_gain_in, query_down, query_gain_in, latent_down, latent_gain_in, rope_down, query_up,
    key_up, value_up, glu_value, glu_gate, taps_in, group_gain_in, head_proj, channel_proj, tables,
    placed, log_out,
    norm_gain, query_gain, latent_gain, conv_taps, group_gain, log_v,
    w_q, w_g, w_o, tok_v, lat_v, rope_v, qup_v, kup_v, vup_v, tab_v,
    normed, keys, rope_keys, key_tmp, q_out, q_lat, q_scr, g_acc, gated, low_rows, high_rows, padded,
    mixed, parts, w_full, mixed_o, part_o, edge_in, head_acc,
    load_sem, ring_sem, z_recv, pair_recv, n_recv, np_recv, q_recv, head_recv, halo_recv, halo_send,
    conv_recv, fin_recv, out_sem, up_recv, back_recv, back_send, nr_recv, hr_recv, cr_recv, corner_recv, edge_recv,
):
    z = lax.axis_index("sp")
    c = lax.axis_index("fs")
    t = lax.axis_index("tp")
    peer = 1 - t
    c_x = c + 1 - 2 * (c % 2)
    c_y = (c + 2) % 4
    c_d = 3 - c
    others = (c_x, c_y, c_d)
    n_fs = normed.shape[0]
    n_tp = 2
    rows, width = tokens.shape
    depth, q_cols = w_q.shape[1:]
    cols = w_g.shape[2] // 2
    heads = key_up.shape[1] // NOPE
    head_rows = head_proj.shape[0]
    out_rows, out_cols = w_o.shape[1:]
    half_width = width // n_tp
    per_core = n_fs // n_tp
    half_sp = n_sp // n_tp

    def lanes_at(index, size):
        return pl.ds(pl.multiple_of(index * size, LANES), size)

    barrier = pltpu.get_barrier_semaphore()
    sides = [{"fs": c_x}, {"fs": c_y}, {"tp": peer}]
    for partner in sides:
        pl.semaphore_signal(barrier, inc=1, device_id=partner, device_id_type=MESH)

    @pl.when(z > 0)
    def _():
        pl.semaphore_signal(barrier, inc=1, device_id={"sp": z - 1}, device_id_type=MESH)

    @pl.when(z < n_sp - 1)
    def _():
        pl.semaphore_signal(barrier, inc=1, device_id={"sp": z + 1}, device_id_type=MESH)

    loads = {}

    def load(name, slot, src, dst):
        copy = pltpu.make_async_copy(src, dst, load_sem.at[slot])
        copy.start()
        loads[name] = copy

    load("tok", 0, tokens, tok_v)
    load("ng", 1, norm_gain_in, norm_gain)
    load("wq", 2, query_down.at[:, lanes_at(c, q_cols)], w_q.at[z])
    load("wv", 3, glu_value.at[:, lanes_at(c, cols)], w_g.at[z, :, pl.ds(0, cols)])
    load("wt", 4, glu_gate.at[:, lanes_at(c, cols)], w_g.at[z, :, pl.ds(cols, cols)])
    load("lat", 5, latent_down, lat_v)
    load("rope", 6, rope_down, rope_v)
    load("tab", 7, tables.at[:, pl.ds(pl.multiple_of(z * rows, LANES), rows), :], tab_v)
    load("lg", 8, latent_gain_in, latent_gain)

    def load_rest():
        load("hp", 0, head_proj.at[:, lanes_at(c, out_cols)], w_o.at[z, pl.ds(0, head_rows), :])
        load("cp", 1, channel_proj.at[:, lanes_at(c, out_cols)], w_o.at[z, pl.ds(head_rows, out_rows - head_rows), :])
        load("qup", 2, query_up, qup_v)
        load("kup", 3, key_up, kup_v)
        load("vup", 4, value_up, vup_v)
        load("qg", 5, query_gain_in, query_gain)
        load("taps", 6, taps_in.at[:, lanes_at(c, cols)], conv_taps)
        load("gg", 7, group_gain_in, group_gain)
        load("hf", 8, head_proj, w_full.at[pl.ds(0, head_rows), :])
        load("cf", 9, channel_proj, w_full.at[pl.ds(head_rows, out_rows - head_rows), :])

    loads["tok"].wait()
    loads["ng"].wait()
    values = tok_v[...].astype(F32)
    normed[c] = rms_scale(values, row_of(norm_gain)).astype(BF16)
    for name in ("wq", "wv", "wt"):
        loads[name].wait()

    ends = (z == 0).astype(jnp.int32) + (z == n_sp - 1).astype(jnp.int32)
    pl.semaphore_wait(barrier, len(sides) + 2 - ends)

    sent = []

    def when(cond, action):
        if cond is None:
            action()
        else:
            pl.when(cond)(action)

    def both(first, second):
        return second if first is None else first & second

    def remote(src, dst, recv_sem, device):
        def make(send_sem):
            return pltpu.make_async_remote_copy(
                src_ref=src, dst_ref=dst, send_sem=send_sem, recv_sem=recv_sem,
                device_id=device, device_id_type=MESH,
            )

        return make

    def drain(entry):
        copy, cond = entry
        when(cond, copy.wait_send)

    def send(make, cond=None):
        slot = len(sent) % RING
        if len(sent) >= RING:
            drain(sent[-RING])
        copy = make(ring_sem.at[slot])
        when(cond, copy.start)
        sent.append((copy, cond))

    def arrive(make):
        make(ring_sem.at[0]).wait_recv()

    q_half = depth // n_tp
    piece = depth // PIECES
    k_half = rows // n_tp
    inner = (z > 0) & (z < n_sp - 1)
    at_end = jnp.logical_not(inner)
    lower = 2 * z < n_sp
    outer = jnp.where(lower, 0, n_sp - 1)
    near = jnp.where(lower, 1, n_sp - 2)
    far = jnp.where(lower, n_sp - 2, 1)
    neighbour = jnp.where(lower, z + 1, z - 1)

    def half(first, size):
        return pl.ds(pl.multiple_of(first * size, 16), size)

    def block(u, shard, side=t):
        if u == Q:
            return w_q.at[shard, half(side, q_half), :]
        if u == K:
            return keys.at[shard, side]
        if u == H:
            return w_o.at[shard, pl.ds(0, head_rows), :]
        if u == C:
            return w_o.at[shard, pl.ds(head_rows, out_rows - head_rows), :]
        return w_g.at[shard, pl.ds((u - G) * piece, piece), :]

    def slot_of(shard, at):
        return shard - (shard > at).astype(jnp.int32)

    def z_copy(u, shard, target):
        ref = block(u, shard)
        return remote(ref, ref, z_recv.at[u, slot_of(shard, target)], {"sp": target})

    def z_arrive(u, shard):
        ref = block(u, shard)
        arrive(remote(ref, ref, z_recv.at[u, slot_of(shard, z)], {"sp": neighbour}))

    def send_own(u, cond=None):
        skip = 1 if u in (H, C) else 0
        send(z_copy(u, z, z - 1), both(cond, z > skip))
        send(z_copy(u, z, z + 1), both(cond, z < n_sp - 1 - skip))

    nearest = jnp.minimum(z, n_sp - 1 - z)
    arrivals = []
    for k in range(n_sp - 1):
        two_sided = k < 2 * nearest
        distance = jnp.where(two_sided, k // 2 + 1, k - nearest + 1)
        from_low = jnp.where(two_sided, 1 - k % 2, (2 * z > n_sp - 1).astype(jnp.int32))
        arrivals.append((z - distance * (2 * from_low - 1), z + 2 * from_low - 1))

    def pass_on(u, shard, target):
        when(inner, lambda: z_arrive(u, shard))
        send(z_copy(u, shard, target), inner)

    def relay(u, k):
        pass_on(u, *arrivals[k])

    def both_ways(u):
        pass_on(u, outer, far)
        pass_on(u, far, outer)

    def settle(u, k):
        when(at_end, lambda: z_arrive(u, arrivals[k][0]))

    def pair(u, shard, side):
        ref = block(u, shard, side)
        return remote(ref, ref, pair_recv.at[u, slot_of(shard, z)], {"tp": peer})

    def share(u, k):
        settle(u, k)
        send(pair(u, arrivals[k][0], t))

    quarter_width = half_width // 2

    def n_block(owner, part):
        return normed.at[owner, :, lanes_at(2 * t + part, quarter_width)]

    def n_copy(i, part):
        ref = n_block(c, part)
        return remote(ref, ref, n_recv.at[i, part], {"fs": others[i]})

    def n_relay(i):
        ref = n_block(others[i], i)
        return remote(ref, ref, nr_recv.at[i], {"fs": others[1 - i]})

    def n_pair(i, side):
        ref = normed.at[others[i], :, lanes_at(side, half_width)]
        return remote(ref, ref, np_recv.at[i], {"tp": peer})

    def pass_normed(i):
        arrive(n_copy(i, i))
        send(n_relay(i))

    def share_normed(i):
        if i < 2:
            arrive(n_copy(i, 1 - i))
        else:
            for j in range(2):
                arrive(n_relay(j))
        send(n_pair(i, t))

    send_own(Q)
    for part in range(2):
        send(n_copy(0, part))
        send(n_copy(1, 1 - part))

    def rotate_lanes(v):
        step = ROPE // 2
        return (
            v * tab_v[0] + pltpu.roll(v, LANES - step, 1) * tab_v[1] + pltpu.roll(v, step, 1) * tab_v[2]
        )

    loads["lat"].wait()
    loads["lg"].wait()
    own_normed = normed[c]
    latent = rms_scale(dot(own_normed, lat_v[...]), row_of(latent_gain))
    keys[z, :, 0:k_half, :] = latent.astype(BF16).reshape(n_tp, k_half, KVR)
    loads["rope"].wait()
    loads["tab"].wait()
    key_tmp[...] = jnp.zeros_like(key_tmp)
    key_tmp[:, 0:ROPE] = dot_nt(own_normed, rope_v[...])
    rotated = rotate_lanes(key_tmp[...])
    fold = KVR // ROPE
    strip = k_half // fold
    for side in range(n_tp):
        for pair_of in range(fold // 2):
            first = side * k_half + 2 * pair_of * strip
            packed = rotated[first : first + strip, :] + pltpu.roll(
                rotated[first + strip : first + 2 * strip, :], ROPE, 1
            )
            keys[z, side, k_half : k_half + strip, pair_of * LANES : (pair_of + 1) * LANES] = packed.astype(BF16)
    send_own(K)
    send_own(G)
    send_own(G + 1)
    load_rest()

    last = n_sp - 2
    both_ways(Q)
    pass_normed(0)
    pass_normed(1)
    both_ways(K)
    share(Q, 0)
    send_own(G + 2)
    relay(Q, last)
    send_own(G + 3)
    both_ways(G)
    share_normed(0)
    share_normed(1)
    relay(K, last)
    both_ways(G + 1)
    for k in range(1, last):
        share(Q, k)
    share_normed(2)
    share(Q, last)
    for p in range(2, PIECES):
        both_ways(G + p)

    for i in range(len(others)):
        arrive(n_pair(i, peer))
    halo = low_rows.shape[1]
    edge_rows = pl.ds(pl.multiple_of(jnp.where(lower, rows - halo, 0), 16), halo)
    edge_half = edge_in.at[:, :, lanes_at(t, half_width)]
    edge_copy = remote(normed.at[:, edge_rows, lanes_at(t, half_width)], edge_half, edge_recv.at[0], {"sp": near})
    edge_pair = remote(edge_half, edge_half, edge_recv.at[1], {"tp": peer})
    for k in range(n_sp - 1):
        arrive(pair(Q, arrivals[k][0], peer))
    seqs = normed[pl.ds(per_core * t, per_core)].reshape(per_core * rows, width)
    q_out[...] = dot(seqs, w_q[...].reshape(n_sp * depth, q_cols)).reshape(per_core, rows, q_cols)

    for i in range(per_core):
        seq = per_core * t + i
        for core in (peer, t):
            copy = remote(q_out.at[i], q_lat.at[c], q_recv.at[c], {"fs": seq, "tp": core})
            send(copy, None if core is peer else seq != c)

        @pl.when(seq == c)
        def _():
            q_lat[c] = q_out[i]

    for name in ("hp", "cp"):
        loads[name].wait()
    send_own(H, at_end)
    send(edge_copy, at_end)
    send_own(C, at_end)

    def add_shard(shard, first=False):
        rows_in = normed[:, :, lanes_at(shard, depth)].reshape(n_fs * rows, depth)
        term = dot(rows_in, w_g[shard])
        g_acc[...] = term if first else g_acc[...] + term

    up_copy = remote(
        gated.at[:, pl.ds(rows - halo, halo), :], low_rows, halo_recv.at[0], {"sp": z + 1}
    )(halo_send.at[0])
    down_copy = remote(
        gated.at[:, pl.ds(0, halo), :], high_rows, halo_recv.at[1], {"sp": z - 1}
    )(halo_send.at[1])

    def add_arrival(k):
        for p in range(PIECES):
            settle(G + p, k)
        add_shard(arrivals[k][0])

    def gate():
        gated[...] = gate_of(g_acc[...]).reshape(n_fs, rows, cols)

        @pl.when(inner)
        def _():
            up_copy.start()
            down_copy.start()

    def gate_of(acc):
        return (acc[:, 0:cols] * jax.nn.sigmoid(acc[:, cols : 2 * cols])).astype(BF16)

    def edge():
        arrive(edge_pair)
        acc = dot(edge_in[...].reshape(n_fs * halo, width), w_g[...].reshape(n_sp * depth, 2 * cols))
        values = gate_of(acc).astype(F32).reshape(n_fs, halo, cols)

        @pl.when(lower)
        def _():
            padded[:, 0:halo, :] = values

        @pl.when(jnp.logical_not(lower))
        def _():
            padded[:, halo + rows : 2 * halo + rows, :] = values

    for p in range(2):
        relay(G + p, last)
    for k in range(last):
        share(K, k)
    add_shard(z, True)
    for p in range(2, PIECES):
        relay(G + p, last)
    share(K, last)

    add_arrival(0)

    send_own(H, inner)

    @pl.when(inner)
    def _():
        for k in range(1, n_sp - 1):
            add_arrival(k)
        gate()

    send_own(C, inner)
    for name in ("qup", "kup", "vup", "qg", "taps", "gg"):
        loads[name].wait()

    for source in range(n_fs):
        @pl.when((c != source) | (t != c // per_core))
        def _():
            arrive(remote(q_out.at[0], q_lat.at[source], q_recv.at[source], {"tp": peer}))

    pass_on(H, outer, far)
    whole_q = jnp.concatenate([q_lat[i] for i in range(n_fs)], axis=1)
    latent_query = rms_scale(whole_q, row_of(query_gain)).astype(BF16)
    q_scr[...] = dot(latent_query, qup_v[...])
    for k in range(n_sp - 1):
        arrive(pair(K, arrivals[k][0], peer))

    key_lane = lax.broadcasted_iota(jnp.int32, (strip, LANES), 1)
    for shard in range(n_sp):
        for side in range(n_tp):
            for pair_of in range(fold // 2):
                packed = keys[
                    shard, side, k_half : k_half + strip, pair_of * LANES : (pair_of + 1) * LANES
                ].astype(F32)
                for part, values in enumerate((packed, pltpu.roll(packed, ROPE, 1))):
                    first = (shard * n_tp + side) * k_half + (2 * pair_of + part) * strip
                    rope_keys[first : first + strip, :] = jnp.where(key_lane < ROPE, values, 0.0).astype(BF16)

    def attend(h, shifted):
        start = h * (NOPE + ROPE)
        source = q_scr[...]
        if start % LANES:
            source, start = shifted, start - ROPE
        plain = source[:, start : start + NOPE].astype(BF16)
        rope_part = rotate_lanes(source[:, start + NOPE : start + NOPE + LANES]).astype(BF16)
        absorbed = dot_nt(plain, kup_v[:, h * NOPE : (h + 1) * NOPE]).astype(BF16)
        latents = keys[:, :, 0:k_half, :].reshape(n_sp * rows, KVR)
        scores = (dot_nt(absorbed, latents) + dot_nt(rope_part, rope_keys[...])) * (NOPE + ROPE) ** (-0.5)
        row_max = jnp.max(scores, axis=1, keepdims=True)
        weights = jnp.exp(scores - row_max)
        total = jnp.sum(weights, axis=1, keepdims=True)
        added = dot(weights.astype(BF16), latents)
        attended = (added / total).astype(BF16)
        head_out = dot(attended, vup_v[:, h * VDIM : (h + 1) * VDIM])
        mixed[c, :, h * VDIM : (h + 1) * VDIM] = head_out.astype(BF16)
        return row_max + jnp.log(total)

    def head_ref(owner, h):
        return mixed.at[owner, :, pl.ds(2 * h * VDIM, 2 * VDIM)]

    def head_copy(h, i):
        ref = head_ref(c, h)
        return remote(ref, ref, head_recv.at[h, i], {"fs": others[i]})

    def head_relay(h):
        ref = head_ref(others[h], h)
        return remote(ref, ref, hr_recv.at[h], {"fs": others[1 - h]})

    def pass_head(h, cond):
        when(cond, lambda: arrive(head_copy(h, h)))
        send(head_relay(h), cond)

    whole = q_scr[...]
    shifted = pltpu.roll(whole, whole.shape[1] - ROPE, 1)
    lane = lax.broadcasted_iota(jnp.int32, (rows, LANES), 1)
    logs = jnp.zeros((rows, LANES), F32)

    def to_near(group):
        lanes = lanes_at(group, cols) if isinstance(group, jax.Array) or group >= heads else pl.ds(2 * group * cols, 2 * cols)
        index = group - heads + 2 if isinstance(group, jax.Array) or group >= heads else group
        return remote(mixed.at[c, :, lanes], mixed_o.at[:, lanes], up_recv.at[index], {"sp": near})

    for h in range(heads):
        logs = jnp.where(lane == h, attend(h, shifted), logs)
        if h % 2:
            for i in range(2):
                send(head_copy(h // 2, i))
            send(to_near(h // 2), at_end)
        if h == 1:
            when(inner, lambda: arrive(edge_copy))
            send(edge_pair, inner)
    log_v[...] = jnp.transpose(logs)[0:heads, :]
    log_copy = pltpu.make_async_copy(log_v, log_out, out_sem.at[0])
    log_copy.start()
    pass_on(H, far, outer)

    @pl.when(at_end)
    def _():
        for k in range(1, last):
            add_arrival(k)

    for h in range(2):
        pass_head(h, at_end)

    @pl.when(at_end)
    def _():
        add_arrival(last)
        gate()

    @pl.when(inner)
    def _():
        edge()

    reach = conv_taps.shape[0] // 2
    padded[:, halo : halo + rows, :] = gated[...].astype(F32)

    @pl.when(z > 1)
    def _():
        up_copy.wait_recv()
        padded[:, 0:halo, :] = low_rows[...].astype(F32)

    @pl.when(z == 0)
    def _():
        padded[:, 0:halo, :] = jnp.zeros((n_fs, halo, cols), F32)

    @pl.when(z < n_sp - 2)
    def _():
        down_copy.wait_recv()
        padded[:, halo + rows : 2 * halo + rows, :] = high_rows[...].astype(F32)

    @pl.when(z == n_sp - 1)
    def _():
        padded[:, halo + rows : 2 * halo + rows, :] = jnp.zeros((n_fs, halo, cols), F32)

    def conv_ref(s, group):
        return mixed.at[s, :, pl.ds(pl.multiple_of(head_rows + group * cols, LANES), cols)]

    def conv_copy(s, i):
        ref = conv_ref(s, c)
        return remote(ref, ref, conv_recv.at[s, i], {"fs": others[i]})

    def conv_corner():
        ref = conv_ref(c_d, c)
        return remote(ref, ref, corner_recv.at[0], {"fs": c_d})

    def conv_corner_in():
        ref = conv_ref(c, c_d)
        return remote(ref, ref, corner_recv.at[0], {"fs": c_d})

    def conv_relay(s, i):
        ref = conv_ref(s, others[i])
        return remote(ref, ref, cr_recv.at[s], {"fs": others[1 - i]})

    taps = conv_taps[...].astype(F32)
    all_gains = row_of(group_gain).astype(F32)
    gains = all_gains[:, 0:cols]
    for i in range(1, n_fs):
        gains = jnp.where(c == i, all_gains[:, i * cols : (i + 1) * cols], gains)
    def conv_seq(s):
        filtered = jnp.zeros((rows, cols), F32)
        for j in range(conv_taps.shape[0]):
            first = halo - reach + j
            filtered = filtered + padded[s, first : first + rows, :] * taps[j : j + 1, :]
        centred = filtered - jnp.mean(filtered, axis=1, keepdims=True)
        spread = jnp.mean(centred * centred, axis=1, keepdims=True)
        branch = centred * lax.rsqrt(spread + norm_eps) * gains
        branch = branch * jax.nn.sigmoid(branch)
        mixed[s, :, pl.ds(pl.multiple_of(head_rows + c * cols, LANES), cols)] = branch.astype(BF16)

    conv_seq(c_d)
    send(conv_corner())
    conv_seq(c_x)
    send(conv_copy(c_x, 0))
    conv_seq(c_y)
    send(conv_copy(c_y, 1))
    conv_seq(c)
    send(to_near(heads + c), at_end)
    for s, i in ((c, 0), (c_d, 1), (c_y, 0), (c, 1), (c_d, 0), (c_x, 1)):
        send(conv_copy(s, i))
    pass_on(C, outer, far)
    pass_on(C, far, outer)
    for h in range(2):
        pass_head(h, inner)
    relay(H, last)
    arrive(conv_copy(c, 0))
    send(to_near(heads + c_x), at_end)
    arrive(conv_copy(c, 1))
    send(to_near(heads + c_y), at_end)
    send(conv_relay(c, 1))
    arrive(conv_corner_in())
    send(to_near(heads + c_d), at_end)
    for s, i in ((c_x, 0), (c_d, 1)):
        arrive(conv_copy(s, i))
        send(conv_relay(s, i))
    relay(C, last)
    for h in range(2):
        arrive(head_copy(h, 1 - h))
        arrive(head_relay(h))

    def head_part(shard):
        head_acc[shard] = dot(mixed[:, :, 0:head_rows].reshape(n_fs * rows, head_rows), w_o[shard, 0:head_rows, :])

    head_part(z)
    settle(H, 1)
    head_part(arrivals[1][0])

    @pl.when(inner)
    def _():
        head_part(arrivals[0][0])
        for k in range(2, n_sp - 1):
            head_part(arrivals[k][0])

    for s, i in ((c_y, 1), (c_d, 0), (c_x, 1), (c_y, 0)):
        arrive(conv_copy(s, i))
    for s in others:
        arrive(conv_relay(s, 0))

    def place(core, shard):
        first = (shard % half_sp) * (n_fs * out_cols) + c * out_cols
        return placed.at[core, :, pl.ds(pl.multiple_of(first, LANES), out_cols)]

    def fin_copy(shard, j):
        seq = others[j] if j < len(others) else c
        return remote(
            parts.at[shard, pl.ds(pl.multiple_of(seq * rows, LANES), rows), :], place(t, shard),
            fin_recv.at[t, shard % half_sp, j], {"fs": seq, "tp": shard // half_sp},
        )

    def keep_copy(shard):
        ref = parts.at[shard, pl.ds(pl.multiple_of(c * rows, LANES), rows), :]
        return pltpu.make_async_copy(ref, place(t, shard), out_sem.at[1 + shard % half_sp])

    def add_part(shard, cond=None):
        def compute():
            part = head_acc[shard] + dot(
                mixed[:, :, head_rows:out_rows].reshape(n_fs * rows, out_rows - head_rows), w_o[shard, head_rows:out_rows, :]
            )
            parts[shard] = part.astype(BF16)

        when(cond, compute)
        for j in (2, 0, 1):
            send(fin_copy(shard, j), cond)
        mine = shard // half_sp == t
        send(fin_copy(shard, len(others)), both(cond, jnp.logical_not(mine)))
        when(both(cond, mine), lambda: keep_copy(shard).start())

    back_lanes = lanes_at(z % half_sp, n_fs * out_cols)
    back_copy = remote(
        part_o, placed.at[t, :, back_lanes], back_recv.at[t], {"sp": outer, "tp": z // half_sp}
    )(back_send.at[0])
    for name in ("hf", "cf"):
        loads[name].wait()

    def neighbour_part():
        for i in (0, 1, *range(heads, heads + n_fs)):
            arrive(to_near(i))
        part_o[...] = dot(mixed_o[...], w_full[...]).astype(BF16)
        back_copy.start()

    @pl.when(inner)
    def _():
        neighbour_part()

    add_part(z)
    add_part(arrivals[0][0], inner)
    settle(C, 1)
    add_part(arrivals[1][0])
    for k in range(2, n_sp - 1):
        settle(H, k)

        @pl.when(at_end)
        def _():
            head_part(arrivals[k][0])

        settle(C, k)
        add_part(arrivals[k][0])

    for entry in sent[-RING:]:
        drain(entry)

    @pl.when(inner)
    def _():
        up_copy.wait_send()
        down_copy.wait_send()
        back_copy.wait_send()

    for i in range(half_sp):
        shard = t * half_sp + i
        computed = inner | (shard != near)

        def arrived(core, j):
            arrive(remote(parts.at[0, pl.ds(0, rows), :], place(0, i), fin_recv.at[core, i, j], {"tp": peer}))

        @pl.when(computed)
        def _():
            for core in range(n_tp):
                for j in range(len(others)):
                    arrived(core, j)
            arrived(peer, len(others))
            keep_copy(shard).wait()

        @pl.when(jnp.logical_not(computed))
        def _():
            for core in range(n_tp):
                arrive(remote(part_o, placed.at[0, :, lanes_at(i, n_fs * out_cols)], back_recv.at[core], {"tp": peer}))
    log_copy.wait()


def finish_kernel(placed, log_in, out, log_out):
    out[...] = (placed[0].astype(F32) + placed[1].astype(F32)).astype(BF16)
    log_out[...] = log_in[...]


def fused_device(n_sp, n_fs, *args):
    (tokens, norm_gain, query_down, query_gain, latent_down, latent_gain, rope_down, query_up,
     key_up, value_up, glu_value, glu_gate, conv_taps, group_gain, head_proj, channel_proj) = args
    rows, width = tokens.shape
    depth, q_rank = query_down.shape
    cols = glu_value.shape[1] // n_fs
    heads = key_up.shape[1] // NOPE
    out_rows = head_proj.shape[0] + channel_proj.shape[0]
    out_cols = head_proj.shape[1] // n_fs
    q_cols = q_rank // n_fs
    halo = (conv_taps.shape[0] // 2 + 15) // 16 * 16
    tables = jnp.asarray(rope_tables(n_sp * rows))
    hbm = pl.BlockSpec(memory_space=pltpu.HBM)
    operands = [
        tokens, norm_gain, query_down, query_gain, latent_down, latent_gain, rope_down.T, query_up,
        key_up, value_up, glu_value, glu_gate, conv_taps, group_gain, head_proj, channel_proj, tables,
    ]
    like = lambda a: pltpu.VMEM(a.shape, a.dtype)
    dma = pltpu.SemaphoreType.DMA
    half_sp = n_sp // 2
    scratch = [
        like(norm_gain), like(query_gain), like(latent_gain), pltpu.VMEM((conv_taps.shape[0], cols), BF16), like(group_gain),
        pltpu.VMEM((heads, rows), F32),
        pltpu.VMEM((n_sp, depth, q_cols), BF16),
        pltpu.VMEM((n_sp, depth, 2 * cols), BF16),
        pltpu.VMEM((n_sp, out_rows, out_cols), BF16),
        like(tokens), like(latent_down), pltpu.VMEM(rope_down.shape[::-1], BF16), like(query_up), like(key_up), like(value_up),
        pltpu.VMEM((3, rows, LANES), F32),
        pltpu.VMEM((n_fs, rows, width), BF16),
        pltpu.VMEM((n_sp, 2, rows // 2 + rows // 2 * ROPE // KVR, KVR), BF16),
        pltpu.VMEM((n_sp * rows, LANES), BF16),
        pltpu.VMEM((rows, LANES), F32),
        pltpu.VMEM((n_fs // 2, rows, q_cols), F32),
        pltpu.VMEM((n_fs, rows, q_cols), F32),
        pltpu.VMEM((rows, query_up.shape[1]), F32),
        pltpu.VMEM((n_fs * rows, 2 * cols), F32),
        pltpu.VMEM((n_fs, rows, cols), BF16),
        pltpu.VMEM((n_fs, halo, cols), BF16),
        pltpu.VMEM((n_fs, halo, cols), BF16),
        pltpu.VMEM((n_fs, rows + 2 * halo, cols), F32),
        pltpu.VMEM((n_fs, rows, out_rows), BF16),
        pltpu.VMEM((n_sp, n_fs * rows, out_cols), BF16),
        pltpu.VMEM((out_rows, n_fs * out_cols), BF16),
        pltpu.VMEM((rows, out_rows), BF16),
        pltpu.VMEM((rows, n_fs * out_cols), BF16),
        pltpu.VMEM((n_fs, halo, width), BF16),
        pltpu.VMEM((n_sp, n_fs * rows, out_cols), F32),
        dma((10,)), dma((RING,)), dma((G + PIECES, n_sp - 1)), dma((2, n_sp - 1)), dma((2, 2)), dma((3,)), dma((n_fs,)),
        dma((2, 2)), dma((2,)), dma((2,)), dma((n_fs, 2)), dma((2, half_sp, 4)), dma((1 + half_sp,)),
        dma((2 + n_fs,)), dma((2,)), dma((1,)), dma((2,)), dma((2,)), dma((n_fs,)), dma((1,)), dma((2,)),
    ]
    shapes = (
        jax.ShapeDtypeStruct((rows, half_sp * n_fs * out_cols), BF16),
        jax.ShapeDtypeStruct((heads, rows), F32),
    )
    placed, logs = pl.pallas_call(
        functools.partial(fused_kernel, n_sp),
        out_shape=(jax.ShapeDtypeStruct((2,) + shapes[0].shape, BF16), shapes[1]),
        in_specs=[hbm] * len(operands),
        out_specs=(hbm, hbm),
        scratch_shapes=scratch,
        compiler_params=pltpu.CompilerParams(
            collective_id=0, has_side_effects=True, vmem_limit_bytes=63 * 1024 * 1024
        ),
        name="fused_layer",
    )(*operands)
    return pl.pallas_call(finish_kernel, out_shape=shapes, name="finish")(placed, logs)


def solution(mesh):
    in_specs = (
        P(("fs", "sp"), None),
        P(),
        P("sp", None),
        P(),
        P(),
        P(),
        P(),
        P(None, "tp"),
        P(None, "tp"),
        P(None, "tp"),
        P("sp", "tp"),
        P("sp", "tp"),
        P(None, "tp"),
        P("tp"),
        P("tp", "sp"),
        P("tp", "sp"),
    )
    out_specs = (P(("fs", "sp"), "tp"), P("tp", ("fs", "sp")))
    body = per_device
    if mesh.shape["fs"] == 4 and mesh.shape["tp"] == 2 and mesh.shape["sp"] == 4:
        body = functools.partial(fused_device, mesh.shape["sp"], mesh.shape["fs"])
    return jax.shard_map(
        body, mesh=mesh, in_specs=in_specs, out_specs=out_specs, check_vma=False
    )
```

```python
import functools

import jax
import jax.numpy as jnp
import numpy as np
from jax import lax
from jax.experimental import pallas as pl
from jax.experimental.pallas import tpu as pltpu
from jax.sharding import PartitionSpec as P

NOPE = 128
ROPE = 64
VDIM = 128
KVR = 256
CH = 1024
GROUPS = 8
GRID_W = 64


norm_eps = 1e-06
rope_base = 10000.0
far_below = -1e30


def padded_2(block, sides, width):
    for axis, dim in sides:
        count = lax.axis_size(axis)
        forward = [(i, i + 1) for i in range(count - 1)]
        backward = [(target, source) for source, target in forward]
        low = lax.ppermute(
            lax.slice_in_dim(block, block.shape[dim] - width, None, axis=dim), axis, forward
        )
        high = lax.ppermute(lax.slice_in_dim(block, 0, width, axis=dim), axis, backward)
        block = jnp.concatenate([low, block, high], axis=dim)
    return block


def rms_scale(values, scale_gain):
    inv_rms = lax.rsqrt(jnp.mean(values * values, axis=-1, keepdims=True) + norm_eps)
    return values * inv_rms * scale_gain.astype(jnp.float32)


def angles_for(positions, rope_size):
    quarter = rope_size // 4
    inverse = rope_base ** (-jnp.arange(quarter, dtype=jnp.float32) / quarter)
    grid_row = (positions // GRID_W).astype(jnp.float32)
    grid_col = (positions % GRID_W).astype(jnp.float32)
    return jnp.concatenate([grid_row[:, None] * inverse, grid_col[:, None] * inverse], axis=-1)


def rotate(values, angles):
    half_size = values.shape[-1] // 2
    front_half = values[..., :half_size]
    back_half = values[..., half_size:]
    cosine = jnp.cos(angles)
    sine_part = jnp.sin(angles)
    return jnp.concatenate(
        [front_half * cosine - back_half * sine_part, back_half * cosine + front_half * sine_part],
        axis=-1,
    )


def key_block(normed, latent_down, latent_gain, rope_down, positions):
    latent = jnp.dot(normed, latent_down, preferred_element_type=jnp.float32)
    latent = rms_scale(latent, latent_gain).astype(jnp.bfloat16)
    rope_key = jnp.dot(normed, rope_down, preferred_element_type=jnp.float32)
    rope_key = rotate(rope_key, angles_for(positions, rope_key.shape[-1])).astype(jnp.bfloat16)
    return jnp.concatenate([latent, rope_key], axis=1)


def per_device(
    tokens,
    norm_gain,
    query_down,
    query_gain,
    latent_down,
    latent_gain,
    rope_down,
    query_up,
    key_up,
    value_up,
    glu_value,
    glu_gate,
    conv_taps,
    group_gain,
    head_proj,
    channel_proj,
):
    tok_count = tokens.shape[0]
    reach_rows = conv_taps.shape[0] // 2
    head_count = key_up.shape[1] // NOPE
    normed = rms_scale(tokens.astype(jnp.float32), norm_gain).astype(jnp.bfloat16)
    offsets = lax.axis_index("sp") * tok_count + jnp.arange(tok_count, dtype=jnp.int32)
    query_latent = jnp.dot(
        normed,
        lax.all_gather(query_down, "sp", axis=0, tiled=True),
        preferred_element_type=jnp.float32,
    )
    value_in = jnp.dot(
        normed,
        lax.all_gather(glu_value, "sp", axis=0, tiled=True),
        preferred_element_type=jnp.float32,
    )
    gate_in = jnp.dot(
        normed,
        lax.all_gather(glu_gate, "sp", axis=0, tiled=True),
        preferred_element_type=jnp.float32,
    )
    latent_query = rms_scale(query_latent, query_gain).astype(jnp.bfloat16)
    query_all = jnp.dot(latent_query, query_up, preferred_element_type=jnp.float32).reshape(
        tok_count, head_count, NOPE + ROPE
    )
    query_plain = query_all[:, :, :NOPE].astype(jnp.bfloat16)
    query_rope = rotate(query_all[:, :, NOPE:], angles_for(offsets, ROPE)[:, None, :]).astype(
        jnp.bfloat16
    )
    absorbed = jnp.einsum(
        "thd,rhd->htr",
        query_plain,
        key_up.reshape(KVR, head_count, NOPE),
        preferred_element_type=jnp.float32,
    ).astype(jnp.bfloat16)
    queries = jnp.concatenate([absorbed, jnp.transpose(query_rope, (1, 0, 2))], axis=-1)
    score_scale = (NOPE + ROPE) ** (-0.5)
    half_rows = tok_count // lax.axis_size("tp")
    first_row = lax.axis_index("tp") * half_rows
    own_rows = lax.dynamic_slice_in_dim(normed, first_row, half_rows, 0)
    own_positions = lax.dynamic_slice_in_dim(offsets, first_row, half_rows, 0)
    own_keys = key_block(own_rows, latent_down, latent_gain, rope_down, own_positions)
    block_keys = lax.all_gather(own_keys, ("sp", "tp"), axis=0, tiled=True)
    row_max = jnp.full((head_count, tok_count), far_below, jnp.float32)
    scores = (
        jnp.einsum("hqc,kc->hqk", queries, block_keys, preferred_element_type=jnp.float32)
        * score_scale
    )
    new_max = jnp.maximum(row_max, jnp.max(scores, axis=2))
    weights = jnp.exp(scores - new_max[:, :, None])
    new_sum = jnp.sum(weights, axis=2)
    added = jnp.einsum(
        "hqk,kr->hqr",
        weights.astype(jnp.bfloat16),
        block_keys[:, :KVR],
        preferred_element_type=jnp.float32,
    )
    gated_rows = (value_in * jax.nn.sigmoid(gate_in)).astype(jnp.bfloat16)
    padded = padded_2(gated_rows, (("sp", 0),), reach_rows)
    filtered = padded[0:tok_count].astype(jnp.float32) * conv_taps[0].astype(jnp.float32)
    for tap_index in range(1, conv_taps.shape[0]):
        filtered = filtered + padded[tap_index : tap_index + tok_count].astype(
            jnp.float32
        ) * conv_taps[tap_index].astype(jnp.float32)
    grouped = filtered.reshape(tok_count, -1, CH // GROUPS)
    centred = grouped - jnp.mean(grouped, axis=-1, keepdims=True)
    spread = jnp.mean(centred * centred, axis=-1, keepdims=True)
    normal_groups = (centred * lax.rsqrt(spread + norm_eps)).reshape(tok_count, -1)
    conv_branch = jax.nn.silu(normal_groups * group_gain.astype(jnp.float32)).astype(jnp.bfloat16)
    attended = (added / new_sum[:, :, None]).astype(jnp.bfloat16)
    log_weight = new_max + jnp.log(new_sum)
    head_out = jnp.einsum(
        "htr,rhv->thv",
        attended,
        value_up.reshape(KVR, head_count, VDIM),
        preferred_element_type=jnp.float32,
    )
    head_out = head_out.reshape(tok_count, head_count * VDIM).astype(jnp.bfloat16)
    mixed_in = jnp.concatenate([head_out, conv_branch], axis=1)
    out_weight = jnp.concatenate([head_proj, channel_proj], axis=0)
    partial_terms = jnp.dot(
        mixed_in,
        lax.all_gather(out_weight, "sp", axis=1, tiled=True),
        preferred_element_type=jnp.float32,
    )
    mixed_out = lax.psum_scatter(
        partial_terms.astype(jnp.bfloat16), "tp", scatter_dimension=1, tiled=True
    )
    return (mixed_out, log_weight)


LANES = 128
MESH = pl.DeviceIdType.MESH
F32 = jnp.float32
BF16 = jnp.bfloat16
Q, K, H, C, G = range(5)
PIECES = 4
RING = 20


def rope_tables(length):
    quarter = ROPE // 4
    inverse = np.float32(rope_base) ** (-np.arange(quarter, dtype=np.float32) / np.float32(quarter))
    positions = np.arange(length)
    row = (positions // GRID_W).astype(np.float32)[:, None] * inverse
    col = (positions % GRID_W).astype(np.float32)[:, None] * inverse
    angles = np.concatenate([row, col], axis=1).astype(np.float32)
    cosine, sine = np.cos(angles), np.sin(angles)
    tables = np.zeros((3, length, LANES), np.float32)
    half = ROPE // 2
    tables[0, :, :half] = cosine
    tables[0, :, half:ROPE] = cosine
    tables[1, :, :half] = -sine
    tables[2, :, half:ROPE] = sine
    return tables


def dot(a, b):
    return jnp.dot(a, b, preferred_element_type=F32)


def row_of(ref):
    return ref[...].reshape(1, -1)


def dot_nt(a, b):
    return lax.dot_general(a, b, (((1,), (1,)), ((), ())), preferred_element_type=F32)


def fused_kernel(
    n_sp,
    tokens, norm_gain_in, query_down, query_gain_in, latent_down, latent_gain_in, rope_down, query_up,
    key_up, value_up, glu_value, glu_gate, taps_in, group_gain_in, head_proj, channel_proj, tables,
    placed, log_out,
    norm_gain, query_gain, latent_gain, conv_taps, group_gain, log_v,
    w_q, w_g, w_o, tok_v, lat_v, rope_v, qup_v, kup_v, vup_v, tab_v,
    normed, keys, rope_keys, key_tmp, q_out, q_lat, q_scr, g_acc, gated, low_rows, high_rows, padded,
    mixed, parts, w_full, mixed_o, part_o, edge_in, head_acc,
    load_sem, ring_sem, z_recv, pair_recv, n_recv, np_recv, q_recv, head_recv, halo_recv, halo_send,
    conv_recv, fin_recv, out_sem, up_recv, back_recv, back_send, nr_recv, corner_recv, edge_recv,
):
    z = lax.axis_index("sp")
    c = lax.axis_index("fs")
    t = lax.axis_index("tp")
    peer = 1 - t
    c_x = c + 1 - 2 * (c % 2)
    c_y = (c + 2) % 4
    c_d = 3 - c
    others = (c_x, c_y, c_d)
    n_fs = normed.shape[0]
    n_tp = 2
    rows, width = tokens.shape
    depth, q_cols = w_q.shape[1:]
    cols = w_g.shape[2] // 2
    heads = key_up.shape[1] // NOPE
    head_rows = head_proj.shape[0]
    out_rows, out_cols = w_o.shape[1:]
    half_width = width // n_tp
    per_core = n_fs // n_tp
    half_sp = n_sp // n_tp

    def lanes_at(index, size):
        return pl.ds(pl.multiple_of(index * size, LANES), size)

    barrier = pltpu.get_barrier_semaphore()
    sides = [{"fs": c_x}, {"fs": c_y}, {"tp": peer}]
    for partner in sides:
        pl.semaphore_signal(barrier, inc=1, device_id=partner, device_id_type=MESH)

    @pl.when(z > 0)
    def _():
        pl.semaphore_signal(barrier, inc=1, device_id={"sp": z - 1}, device_id_type=MESH)

    @pl.when(z < n_sp - 1)
    def _():
        pl.semaphore_signal(barrier, inc=1, device_id={"sp": z + 1}, device_id_type=MESH)

    loads = {}

    def load(name, slot, src, dst):
        copy = pltpu.make_async_copy(src, dst, load_sem.at[slot])
        copy.start()
        loads[name] = copy

    load("tok", 0, tokens, tok_v)
    load("ng", 1, norm_gain_in, norm_gain)
    load("wq", 2, query_down.at[:, lanes_at(c, q_cols)], w_q.at[z])
    load("wv", 3, glu_value.at[:, lanes_at(c, cols)], w_g.at[z, :, pl.ds(0, cols)])
    load("wt", 4, glu_gate.at[:, lanes_at(c, cols)], w_g.at[z, :, pl.ds(cols, cols)])
    load("lat", 5, latent_down, lat_v)
    load("rope", 6, rope_down, rope_v)
    load("tab", 7, tables.at[:, pl.ds(pl.multiple_of(z * rows, LANES), rows), :], tab_v)
    load("lg", 8, latent_gain_in, latent_gain)

    def load_rest():
        load("hp", 0, head_proj.at[:, lanes_at(c, out_cols)], w_o.at[z, pl.ds(0, head_rows), :])
        load("cp", 1, channel_proj.at[:, lanes_at(c, out_cols)], w_o.at[z, pl.ds(head_rows, out_rows - head_rows), :])
        load("qup", 2, query_up, qup_v)
        load("kup", 3, key_up, kup_v)
        load("vup", 4, value_up, vup_v)
        load("qg", 5, query_gain_in, query_gain)
        load("taps", 6, taps_in.at[:, lanes_at(c, cols)], conv_taps)
        load("gg", 7, group_gain_in, group_gain)
        load("hf", 8, head_proj, w_full.at[pl.ds(0, head_rows), :])
        load("cf", 9, channel_proj, w_full.at[pl.ds(head_rows, out_rows - head_rows), :])

    loads["tok"].wait()
    loads["ng"].wait()
    values = tok_v[...].astype(F32)
    normed[c] = rms_scale(values, row_of(norm_gain)).astype(BF16)
    for name in ("wq", "wv", "wt"):
        loads[name].wait()

    ends = (z == 0).astype(jnp.int32) + (z == n_sp - 1).astype(jnp.int32)
    pl.semaphore_wait(barrier, len(sides) + 2 - ends)

    sent = []

    def when(cond, action):
        if cond is None:
            action()
        else:
            pl.when(cond)(action)

    def both(first, second):
        return second if first is None else first & second

    def remote(src, dst, recv_sem, device):
        def make(send_sem):
            return pltpu.make_async_remote_copy(
                src_ref=src, dst_ref=dst, send_sem=send_sem, recv_sem=recv_sem,
                device_id=device, device_id_type=MESH,
            )

        return make

    def drain(entry):
        copy, cond = entry
        when(cond, copy.wait_send)

    def send(make, cond=None):
        slot = len(sent) % RING
        if len(sent) >= RING:
            drain(sent[-RING])
        copy = make(ring_sem.at[slot])
        when(cond, copy.start)
        sent.append((copy, cond))

    def arrive(make):
        make(ring_sem.at[0]).wait_recv()

    def arrive_all(like, recv_sem):
        arrive(remote(like, like, recv_sem, {"tp": peer}))

    q_half = depth // n_tp
    piece = depth // PIECES
    k_half = rows // n_tp
    inner = (z > 0) & (z < n_sp - 1)
    at_end = jnp.logical_not(inner)
    lower = 2 * z < n_sp
    outer = jnp.where(lower, 0, n_sp - 1)
    near = jnp.where(lower, 1, n_sp - 2)
    far = jnp.where(lower, n_sp - 2, 1)
    neighbour = jnp.where(lower, z + 1, z - 1)

    def half(first, size):
        return pl.ds(pl.multiple_of(first * size, 16), size)

    def block(u, shard, side=t):
        if u == Q:
            return w_q.at[shard, half(side, q_half), :]
        if u == K:
            return keys.at[shard, side]
        if u == H:
            return w_o.at[shard, pl.ds(0, head_rows), :]
        if u == C:
            return w_o.at[shard, pl.ds(head_rows, out_rows - head_rows), :]
        return w_g.at[shard, pl.ds((u - G) * piece, piece), :]

    def slot_of(shard, at):
        return shard - (shard > at).astype(jnp.int32)

    def z_copy(u, shard, target):
        ref = block(u, shard)
        return remote(ref, ref, z_recv.at[u, slot_of(shard, target)], {"sp": target})

    def z_arrive(u, shard):
        ref = block(u, shard)
        arrive(remote(ref, ref, z_recv.at[u, slot_of(shard, z)], {"sp": neighbour}))

    def send_own(u, cond=None):
        skip = 1 if u in (H, C) else 0
        send(z_copy(u, z, z - 1), both(cond, z > skip))
        send(z_copy(u, z, z + 1), both(cond, z < n_sp - 1 - skip))

    nearest = jnp.minimum(z, n_sp - 1 - z)
    arrivals = []
    for k in range(n_sp - 1):
        two_sided = k < 2 * nearest
        distance = jnp.where(two_sided, k // 2 + 1, k - nearest + 1)
        from_low = jnp.where(two_sided, 1 - k % 2, (2 * z > n_sp - 1).astype(jnp.int32))
        arrivals.append((z - distance * (2 * from_low - 1), z + 2 * from_low - 1))

    def pass_on(u, shard, target):
        when(inner, lambda: z_arrive(u, shard))
        send(z_copy(u, shard, target), inner)

    def relay(u, k):
        pass_on(u, *arrivals[k])

    def both_ways(u):
        pass_on(u, outer, far)
        pass_on(u, far, outer)

    def settle(u, k):
        when(at_end, lambda: z_arrive(u, arrivals[k][0]))

    def pair(u, shard, side):
        ref = block(u, shard, side)
        return remote(ref, ref, pair_recv.at[u], {"tp": peer})

    def share(u, k):
        settle(u, k)
        send(pair(u, arrivals[k][0], t))

    quarter_width = half_width // 2

    def n_block(owner, part):
        return normed.at[owner, :, lanes_at(2 * t + part, quarter_width)]

    def n_copy(i, part):
        ref = n_block(c, part)
        return remote(ref, ref, n_recv.at[i, part], {"fs": others[i]})

    def n_relay(i):
        ref = n_block(others[i], i)
        return remote(ref, ref, nr_recv.at[i], {"fs": others[1 - i]})

    def n_pair(i, side):
        ref = normed.at[others[i], :, lanes_at(side, half_width)]
        return remote(ref, ref, np_recv.at[0], {"tp": peer})

    def pass_normed(i):
        arrive(n_copy(i, i))
        send(n_relay(i))

    def share_normed(i):
        if i < 2:
            arrive(n_copy(i, 1 - i))
        else:
            for j in range(2):
                arrive(n_relay(j))
        send(n_pair(i, t))

    send_own(Q)
    for part in range(2):
        send(n_copy(0, part))
        send(n_copy(1, 1 - part))

    def rotate_lanes(v):
        step = ROPE // 2
        return (
            v * tab_v[0] + pltpu.roll(v, LANES - step, 1) * tab_v[1] + pltpu.roll(v, step, 1) * tab_v[2]
        )

    loads["lat"].wait()
    loads["lg"].wait()
    own_normed = normed[c]
    latent = rms_scale(dot(own_normed, lat_v[...]), row_of(latent_gain))
    keys[z, :, 0:k_half, :] = latent.astype(BF16).reshape(n_tp, k_half, KVR)
    loads["rope"].wait()
    loads["tab"].wait()
    key_tmp[...] = jnp.zeros_like(key_tmp)
    key_tmp[:, 0:ROPE] = dot_nt(own_normed, rope_v[...])
    rotated = rotate_lanes(key_tmp[...])
    fold = KVR // ROPE
    strip = k_half // fold
    for side in range(n_tp):
        for pair_of in range(fold // 2):
            first = side * k_half + 2 * pair_of * strip
            packed = rotated[first : first + strip, :] + pltpu.roll(
                rotated[first + strip : first + 2 * strip, :], ROPE, 1
            )
            keys[z, side, k_half : k_half + strip, pair_of * LANES : (pair_of + 1) * LANES] = packed.astype(BF16)
    send_own(K)
    send_own(G)
    send_own(G + 1)
    load_rest()

    last = n_sp - 2
    both_ways(Q)
    pass_normed(0)
    pass_normed(1)
    both_ways(K)
    share(Q, 0)
    send_own(G + 2)
    relay(Q, last)
    send_own(G + 3)
    both_ways(G)
    share_normed(0)
    share_normed(1)
    relay(K, last)
    both_ways(G + 1)
    for k in range(1, last):
        share(Q, k)
    share_normed(2)
    share(Q, last)
    for p in range(2, PIECES):
        both_ways(G + p)

    arrive_all(normed.at[pl.ds(0, n_fs - 1), :, lanes_at(peer, half_width)], np_recv.at[0])
    halo = low_rows.shape[1]
    edge_rows = pl.ds(pl.multiple_of(jnp.where(lower, rows - halo, 0), 16), halo)
    edge_half = edge_in.at[:, :, lanes_at(t, half_width)]
    edge_copy = remote(normed.at[:, edge_rows, lanes_at(t, half_width)], edge_half, edge_recv.at[0], {"sp": near})
    edge_pair = remote(edge_half, edge_half, edge_recv.at[1], {"tp": peer})
    arrive_all(w_q.at[pl.ds(0, n_sp - 1), half(peer, q_half), :], pair_recv.at[Q])
    seqs = normed[pl.ds(per_core * t, per_core)].reshape(per_core * rows, width)
    q_out[...] = dot(seqs, w_q[...].reshape(n_sp * depth, q_cols)).reshape(per_core, rows, q_cols)

    for i in range(per_core):
        seq = per_core * t + i
        for core in (peer, t):
            copy = remote(q_out.at[i], q_lat.at[c], q_recv.at[0], {"fs": seq, "tp": core})
            send(copy, None if core is peer else seq != c)

        @pl.when(seq == c)
        def _():
            q_lat[c] = q_out[i]

    for name in ("hp", "cp"):
        loads[name].wait()
    send_own(H, at_end)
    send(edge_copy, at_end)
    send_own(C, at_end)

    def add_shard(shard, first=False):
        rows_in = normed[:, :, lanes_at(shard, depth)].reshape(n_fs * rows, depth)
        term = dot(rows_in, w_g[shard])
        g_acc[...] = term if first else g_acc[...] + term

    up_copy = remote(
        gated.at[:, pl.ds(rows - halo, halo), :], low_rows, halo_recv.at[0], {"sp": z + 1}
    )(halo_send.at[0])
    down_copy = remote(
        gated.at[:, pl.ds(0, halo), :], high_rows, halo_recv.at[1], {"sp": z - 1}
    )(halo_send.at[1])

    def add_arrival(k):
        for p in range(PIECES):
            settle(G + p, k)
        add_shard(arrivals[k][0])

    def gate():
        gated[...] = gate_of(g_acc[...]).reshape(n_fs, rows, cols)

        @pl.when(inner)
        def _():
            up_copy.start()
            down_copy.start()

    def gate_of(acc):
        return (acc[:, 0:cols] * jax.nn.sigmoid(acc[:, cols : 2 * cols])).astype(BF16)

    def edge():
        arrive(edge_pair)
        acc = dot(edge_in[...].reshape(n_fs * halo, width), w_g[...].reshape(n_sp * depth, 2 * cols))
        values = gate_of(acc).astype(F32).reshape(n_fs, halo, cols)

        @pl.when(lower)
        def _():
            padded[:, 0:halo, :] = values

        @pl.when(jnp.logical_not(lower))
        def _():
            padded[:, halo + rows : 2 * halo + rows, :] = values

    for p in range(2):
        relay(G + p, last)
    for k in range(last):
        share(K, k)
    add_shard(z, True)
    for p in range(2, PIECES):
        relay(G + p, last)
    share(K, last)

    add_arrival(0)

    send_own(H, inner)

    @pl.when(inner)
    def _():
        for k in range(1, n_sp - 1):
            add_arrival(k)
        gate()

    send_own(C, inner)
    for name in ("qup", "kup", "vup", "qg", "taps", "gg"):
        loads[name].wait()

    here = t == c // per_core

    @pl.when(here)
    def _():
        arrive_all(q_lat.at[pl.ds(0, n_fs - 1)], q_recv.at[0])

    @pl.when(jnp.logical_not(here))
    def _():
        arrive_all(q_lat, q_recv.at[0])

    pass_on(H, outer, far)
    whole_q = jnp.concatenate([q_lat[i] for i in range(n_fs)], axis=1)
    latent_query = rms_scale(whole_q, row_of(query_gain)).astype(BF16)
    q_scr[...] = dot(latent_query, qup_v[...])
    arrive_all(keys.at[pl.ds(0, n_sp - 1), peer], pair_recv.at[K])

    key_lane = lax.broadcasted_iota(jnp.int32, (strip, LANES), 1)
    for shard in range(n_sp):
        for side in range(n_tp):
            for pair_of in range(fold // 2):
                packed = keys[
                    shard, side, k_half : k_half + strip, pair_of * LANES : (pair_of + 1) * LANES
                ].astype(F32)
                for part, values in enumerate((packed, pltpu.roll(packed, ROPE, 1))):
                    first = (shard * n_tp + side) * k_half + (2 * pair_of + part) * strip
                    rope_keys[first : first + strip, :] = jnp.where(key_lane < ROPE, values, 0.0).astype(BF16)

    def attend(h, shifted):
        start = h * (NOPE + ROPE)
        source = q_scr[...]
        if start % LANES:
            source, start = shifted, start - ROPE
        plain = source[:, start : start + NOPE].astype(BF16)
        rope_part = rotate_lanes(source[:, start + NOPE : start + NOPE + LANES]).astype(BF16)
        absorbed = dot_nt(plain, kup_v[:, h * NOPE : (h + 1) * NOPE]).astype(BF16)
        latents = keys[:, :, 0:k_half, :].reshape(n_sp * rows, KVR)
        scores = (dot_nt(absorbed, latents) + dot_nt(rope_part, rope_keys[...])) * (NOPE + ROPE) ** (-0.5)
        row_max = jnp.max(scores, axis=1, keepdims=True)
        weights = jnp.exp(scores - row_max)
        total = jnp.sum(weights, axis=1, keepdims=True)
        added = dot(weights.astype(BF16), latents)
        attended = (added / total).astype(BF16)
        head_out = dot(attended, vup_v[:, h * VDIM : (h + 1) * VDIM])
        mixed[c, :, h * VDIM : (h + 1) * VDIM] = head_out.astype(BF16)
        return row_max + jnp.log(total)

    def head_ref(owner, h):
        return mixed.at[owner, :, pl.ds(2 * h * VDIM, 2 * VDIM)]

    def head_copy(h, i):
        ref = head_ref(c, h)
        return remote(ref, ref, head_recv.at[h if h == i else 2], {"fs": others[i]})

    def head_relay(h):
        ref = head_ref(others[h], h)
        return remote(ref, ref, head_recv.at[2], {"fs": others[1 - h]})

    def pass_head(h, cond):
        when(cond, lambda: arrive(head_copy(h, h)))
        send(head_relay(h), cond)

    whole = q_scr[...]
    shifted = pltpu.roll(whole, whole.shape[1] - ROPE, 1)
    lane = lax.broadcasted_iota(jnp.int32, (rows, LANES), 1)
    logs = jnp.zeros((rows, LANES), F32)

    def to_near(group):
        lanes = lanes_at(group, cols) if isinstance(group, jax.Array) or group >= heads else pl.ds(2 * group * cols, 2 * cols)
        return remote(mixed.at[c, :, lanes], mixed_o.at[:, lanes], up_recv.at[0], {"sp": near})

    for h in range(heads):
        logs = jnp.where(lane == h, attend(h, shifted), logs)
        if h % 2:
            for i in range(2):
                send(head_copy(h // 2, i))
            send(to_near(h // 2), at_end)
        if h == 1:
            when(inner, lambda: arrive(edge_copy))
            send(edge_pair, inner)
    log_v[...] = jnp.transpose(logs)[0:heads, :]
    log_copy = pltpu.make_async_copy(log_v, log_out, out_sem.at[0])
    log_copy.start()
    pass_on(H, far, outer)

    @pl.when(at_end)
    def _():
        for k in range(1, last):
            add_arrival(k)

    for h in range(2):
        pass_head(h, at_end)

    @pl.when(at_end)
    def _():
        add_arrival(last)
        gate()

    @pl.when(inner)
    def _():
        edge()

    reach = conv_taps.shape[0] // 2
    padded[:, halo : halo + rows, :] = gated[...].astype(F32)

    @pl.when(z > 1)
    def _():
        up_copy.wait_recv()
        padded[:, 0:halo, :] = low_rows[...].astype(F32)

    @pl.when(z == 0)
    def _():
        padded[:, 0:halo, :] = jnp.zeros((n_fs, halo, cols), F32)

    @pl.when(z < n_sp - 2)
    def _():
        down_copy.wait_recv()
        padded[:, halo + rows : 2 * halo + rows, :] = high_rows[...].astype(F32)

    @pl.when(z == n_sp - 1)
    def _():
        padded[:, halo + rows : 2 * halo + rows, :] = jnp.zeros((n_fs, halo, cols), F32)

    def conv_ref(s, group):
        return mixed.at[s, :, pl.ds(pl.multiple_of(head_rows + group * cols, LANES), cols)]

    def conv_copy(s, i, slot=4):
        ref = conv_ref(s, c)
        return remote(ref, ref, conv_recv.at[slot], {"fs": others[i]})

    def conv_corner():
        ref = conv_ref(c_d, c)
        return remote(ref, ref, corner_recv.at[0], {"fs": c_d})

    def conv_corner_in():
        ref = conv_ref(c, c_d)
        return remote(ref, ref, corner_recv.at[0], {"fs": c_d})

    def conv_relay(s, i):
        ref = conv_ref(s, others[i])
        return remote(ref, ref, conv_recv.at[4], {"fs": others[1 - i]})

    taps = conv_taps[...].astype(F32)
    all_gains = row_of(group_gain).astype(F32)
    gains = all_gains[:, 0:cols]
    for i in range(1, n_fs):
        gains = jnp.where(c == i, all_gains[:, i * cols : (i + 1) * cols], gains)
    def conv_seq(s):
        filtered = jnp.zeros((rows, cols), F32)
        for j in range(conv_taps.shape[0]):
            first = halo - reach + j
            filtered = filtered + padded[s, first : first + rows, :] * taps[j : j + 1, :]
        centred = filtered - jnp.mean(filtered, axis=1, keepdims=True)
        spread = jnp.mean(centred * centred, axis=1, keepdims=True)
        branch = centred * lax.rsqrt(spread + norm_eps) * gains
        branch = branch * jax.nn.sigmoid(branch)
        mixed[s, :, pl.ds(pl.multiple_of(head_rows + c * cols, LANES), cols)] = branch.astype(BF16)

    conv_seq(c_d)
    send(conv_corner())
    conv_seq(c_x)
    send(conv_copy(c_x, 0, 0))
    conv_seq(c_y)
    send(conv_copy(c_y, 1, 2))
    conv_seq(c)
    send(to_near(heads + c), at_end)
    for s, i, slot in ((c, 0, 1), (c_d, 1, 4), (c_y, 0, 4), (c, 1, 4), (c_d, 0, 4), (c_x, 1, 3)):
        send(conv_copy(s, i, slot))
    pass_on(C, outer, far)
    pass_on(C, far, outer)
    for h in range(2):
        pass_head(h, inner)
    relay(H, last)
    arrive(conv_copy(c, 0, 0))
    send(to_near(heads + c_x), at_end)
    arrive(conv_copy(c, 1, 2))
    send(to_near(heads + c_y), at_end)
    send(conv_relay(c, 1))
    arrive(conv_corner_in())
    send(to_near(heads + c_d), at_end)
    for s, i, slot in ((c_x, 0, 1), (c_d, 1, 3)):
        arrive(conv_copy(s, i, slot))
        send(conv_relay(s, i))
    relay(C, last)
    arrive_all(parts.at[pl.ds(0, 2)], head_recv.at[2])

    def head_part(shard):
        head_acc[shard] = dot(mixed[:, :, 0:head_rows].reshape(n_fs * rows, head_rows), w_o[shard, 0:head_rows, :])

    head_part(z)
    settle(H, 1)
    head_part(arrivals[1][0])

    @pl.when(inner)
    def _():
        head_part(arrivals[0][0])
        for k in range(2, n_sp - 1):
            head_part(arrivals[k][0])

    rest = (2 * n_fs - 1) * rows
    arrive_all(w_o.at[0, pl.ds(0, rest), :], conv_recv.at[4])

    def place(core, shard):
        first = (shard % half_sp) * (n_fs * out_cols) + c * out_cols
        return placed.at[core, :, pl.ds(pl.multiple_of(first, LANES), out_cols)]

    def fin_copy(shard, j):
        seq = others[j] if j < len(others) else c
        return remote(
            parts.at[shard, pl.ds(pl.multiple_of(seq * rows, LANES), rows), :], place(t, shard),
            fin_recv.at[t, shard % half_sp], {"fs": seq, "tp": shard // half_sp},
        )

    def keep_copy(shard):
        ref = parts.at[shard, pl.ds(pl.multiple_of(c * rows, LANES), rows), :]
        return pltpu.make_async_copy(ref, place(t, shard), out_sem.at[1 + shard % half_sp])

    def add_part(shard, cond=None):
        def compute():
            part = head_acc[shard] + dot(
                mixed[:, :, head_rows:out_rows].reshape(n_fs * rows, out_rows - head_rows), w_o[shard, head_rows:out_rows, :]
            )
            parts[shard] = part.astype(BF16)

        when(cond, compute)
        for j in (2, 0, 1):
            send(fin_copy(shard, j), cond)
        mine = shard // half_sp == t
        send(fin_copy(shard, len(others)), both(cond, jnp.logical_not(mine)))
        when(both(cond, mine), lambda: keep_copy(shard).start())

    add_part(z)
    add_part(arrivals[0][0], inner)
    settle(C, 1)
    add_part(arrivals[1][0])
    for k in range(2, n_sp - 1):
        settle(H, k)

        @pl.when(at_end)
        def _():
            head_part(arrivals[k][0])

        settle(C, k)
        add_part(arrivals[k][0])

    back_lanes = lanes_at(z % half_sp, n_fs * out_cols)
    back_copy = remote(
        part_o, placed.at[t, :, back_lanes], back_recv.at[0], {"sp": outer, "tp": z // half_sp}
    )(back_send.at[0])
    for name in ("hf", "cf"):
        loads[name].wait()

    def neighbour_part():
        arrive_all(mixed_o, up_recv.at[0])
        part_o[...] = dot(mixed_o[...], w_full[...]).astype(BF16)
        back_copy.start()

    @pl.when(inner)
    def _():
        neighbour_part()

    for entry in sent[-RING:]:
        drain(entry)

    @pl.when(inner)
    def _():
        up_copy.wait_send()
        down_copy.wait_send()
        back_copy.wait_send()

    for i in range(half_sp):
        shard = t * half_sp + i
        computed = inner | (shard != near)

        @pl.when(computed)
        def _():
            arrive_all(parts.at[0, pl.ds(0, (n_fs - 1) * rows), :], fin_recv.at[t, i])
            arrive_all(parts.at[0], fin_recv.at[peer, i])
            keep_copy(shard).wait()

        @pl.when(jnp.logical_not(computed))
        def _():
            arrive_all(parts.at[pl.ds(0, n_tp)], back_recv.at[0])
    log_copy.wait()


def finish_kernel(placed, log_in, out, log_out, held, summed, log_v, load_sem, store_sem):
    span = out.shape[1] // 2
    logs = pltpu.make_async_copy(log_in, log_v, load_sem.at[2])
    loads = [
        pltpu.make_async_copy(placed.at[:, :, pl.ds(i * span, span)], held.at[i], load_sem.at[i]) for i in range(2)
    ]
    for copy in loads:
        copy.start()
    logs.start()
    stores = [
        pltpu.make_async_copy(summed.at[i], out.at[:, pl.ds(i * span, span)], store_sem.at[i]) for i in range(2)
    ]
    for i in range(2):
        loads[i].wait()
        summed[i] = (held[i, 0].astype(F32) + held[i, 1].astype(F32)).astype(BF16)
        stores[i].start()
    logs.wait()
    stores.append(pltpu.make_async_copy(log_v, log_out, store_sem.at[2]))
    stores[2].start()
    for copy in stores:
        copy.wait()


def fused_device(n_sp, n_fs, *args):
    (tokens, norm_gain, query_down, query_gain, latent_down, latent_gain, rope_down, query_up,
     key_up, value_up, glu_value, glu_gate, conv_taps, group_gain, head_proj, channel_proj) = args
    rows, width = tokens.shape
    depth, q_rank = query_down.shape
    cols = glu_value.shape[1] // n_fs
    heads = key_up.shape[1] // NOPE
    out_rows = head_proj.shape[0] + channel_proj.shape[0]
    out_cols = head_proj.shape[1] // n_fs
    q_cols = q_rank // n_fs
    halo = (conv_taps.shape[0] // 2 + 15) // 16 * 16
    tables = jnp.asarray(rope_tables(n_sp * rows))
    hbm = pl.BlockSpec(memory_space=pltpu.HBM)
    operands = [
        tokens, norm_gain, query_down, query_gain, latent_down, latent_gain, rope_down.T, query_up,
        key_up, value_up, glu_value, glu_gate, conv_taps, group_gain, head_proj, channel_proj, tables,
    ]
    like = lambda a: pltpu.VMEM(a.shape, a.dtype)
    dma = pltpu.SemaphoreType.DMA
    half_sp = n_sp // 2
    scratch = [
        like(norm_gain), like(query_gain), like(latent_gain), pltpu.VMEM((conv_taps.shape[0], cols), BF16), like(group_gain),
        pltpu.VMEM((heads, rows), F32),
        pltpu.VMEM((n_sp, depth, q_cols), BF16),
        pltpu.VMEM((n_sp, depth, 2 * cols), BF16),
        pltpu.VMEM((n_sp, out_rows, out_cols), BF16),
        like(tokens), like(latent_down), pltpu.VMEM(rope_down.shape[::-1], BF16), like(query_up), like(key_up), like(value_up),
        pltpu.VMEM((3, rows, LANES), F32),
        pltpu.VMEM((n_fs, rows, width), BF16),
        pltpu.VMEM((n_sp, 2, rows // 2 + rows // 2 * ROPE // KVR, KVR), BF16),
        pltpu.VMEM((n_sp * rows, LANES), BF16),
        pltpu.VMEM((rows, LANES), F32),
        pltpu.VMEM((n_fs // 2, rows, q_cols), F32),
        pltpu.VMEM((n_fs, rows, q_cols), F32),
        pltpu.VMEM((rows, query_up.shape[1]), F32),
        pltpu.VMEM((n_fs * rows, 2 * cols), F32),
        pltpu.VMEM((n_fs, rows, cols), BF16),
        pltpu.VMEM((n_fs, halo, cols), BF16),
        pltpu.VMEM((n_fs, halo, cols), BF16),
        pltpu.VMEM((n_fs, rows + 2 * halo, cols), F32),
        pltpu.VMEM((n_fs, rows, out_rows), BF16),
        pltpu.VMEM((n_sp, n_fs * rows, out_cols), BF16),
        pltpu.VMEM((out_rows, n_fs * out_cols), BF16),
        pltpu.VMEM((rows, out_rows), BF16),
        pltpu.VMEM((rows, n_fs * out_cols), BF16),
        pltpu.VMEM((n_fs, halo, width), BF16),
        pltpu.VMEM((n_sp, n_fs * rows, out_cols), F32),
        dma((10,)), dma((RING,)), dma((G + PIECES, n_sp - 1)), dma((2,)), dma((2, 2)), dma((1,)), dma((1,)),
        dma((3,)), dma((2,)), dma((2,)), dma((5,)), dma((2, half_sp)), dma((1 + half_sp,)),
        dma((1,)), dma((1,)), dma((1,)), dma((2,)), dma((1,)), dma((2,)),
    ]
    shapes = (
        jax.ShapeDtypeStruct((rows, half_sp * n_fs * out_cols), BF16),
        jax.ShapeDtypeStruct((heads, rows), F32),
    )
    placed, logs = pl.pallas_call(
        functools.partial(fused_kernel, n_sp),
        out_shape=(jax.ShapeDtypeStruct((2,) + shapes[0].shape, BF16), shapes[1]),
        in_specs=[hbm] * len(operands),
        out_specs=(hbm, hbm),
        scratch_shapes=scratch,
        compiler_params=pltpu.CompilerParams(
            collective_id=0, has_side_effects=True, vmem_limit_bytes=63 * 1024 * 1024
        ),
        name="fused_layer",
    )(*operands)
    span = shapes[0].shape[1] // 2
    return pl.pallas_call(
        finish_kernel,
        out_shape=shapes,
        in_specs=[hbm] * 2,
        out_specs=(hbm, hbm),
        scratch_shapes=[
            pltpu.VMEM((2, 2, rows, span), BF16), pltpu.VMEM((2, rows, span), BF16), pltpu.VMEM((heads, rows), F32),
            dma((3,)), dma((3,)),
        ],
        name="finish",
    )(placed, logs)


def solution(mesh):
    in_specs = (
        P(("fs", "sp"), None),
        P(),
        P("sp", None),
        P(),
        P(),
        P(),
        P(),
        P(None, "tp"),
        P(None, "tp"),
        P(None, "tp"),
        P("sp", "tp"),
        P("sp", "tp"),
        P(None, "tp"),
        P("tp"),
        P("tp", "sp"),
        P("tp", "sp"),
    )
    out_specs = (P(("fs", "sp"), "tp"), P("tp", ("fs", "sp")))
    body = per_device
    if mesh.shape["fs"] == 4 and mesh.shape["tp"] == 2 and mesh.shape["sp"] == 4:
        body = functools.partial(fused_device, mesh.shape["sp"], mesh.shape["fs"])
    return jax.shard_map(
        body, mesh=mesh, in_specs=in_specs, out_specs=out_specs, check_vma=False
    )
```

```python
import functools

import jax
import jax.numpy as jnp
import numpy as np
from jax import lax
from jax.experimental import pallas as pl
from jax.experimental.pallas import tpu as pltpu
from jax.sharding import PartitionSpec as P

NOPE = 128
ROPE = 64
VDIM = 128
KVR = 256
CH = 1024
GROUPS = 8
GRID_W = 64


norm_eps = 1e-06
rope_base = 10000.0
far_below = -1e30


def padded_2(block, sides, width):
    for axis, dim in sides:
        count = lax.axis_size(axis)
        forward = [(i, i + 1) for i in range(count - 1)]
        backward = [(target, source) for source, target in forward]
        low = lax.ppermute(
            lax.slice_in_dim(block, block.shape[dim] - width, None, axis=dim), axis, forward
        )
        high = lax.ppermute(lax.slice_in_dim(block, 0, width, axis=dim), axis, backward)
        block = jnp.concatenate([low, block, high], axis=dim)
    return block


def rms_scale(values, scale_gain):
    inv_rms = lax.rsqrt(jnp.mean(values * values, axis=-1, keepdims=True) + norm_eps)
    return values * inv_rms * scale_gain.astype(jnp.float32)


def angles_for(positions, rope_size):
    quarter = rope_size // 4
    inverse = rope_base ** (-jnp.arange(quarter, dtype=jnp.float32) / quarter)
    grid_row = (positions // GRID_W).astype(jnp.float32)
    grid_col = (positions % GRID_W).astype(jnp.float32)
    return jnp.concatenate([grid_row[:, None] * inverse, grid_col[:, None] * inverse], axis=-1)


def rotate(values, angles):
    half_size = values.shape[-1] // 2
    front_half = values[..., :half_size]
    back_half = values[..., half_size:]
    cosine = jnp.cos(angles)
    sine_part = jnp.sin(angles)
    return jnp.concatenate(
        [front_half * cosine - back_half * sine_part, back_half * cosine + front_half * sine_part],
        axis=-1,
    )


def key_block(normed, latent_down, latent_gain, rope_down, positions):
    latent = jnp.dot(normed, latent_down, preferred_element_type=jnp.float32)
    latent = rms_scale(latent, latent_gain).astype(jnp.bfloat16)
    rope_key = jnp.dot(normed, rope_down, preferred_element_type=jnp.float32)
    rope_key = rotate(rope_key, angles_for(positions, rope_key.shape[-1])).astype(jnp.bfloat16)
    return jnp.concatenate([latent, rope_key], axis=1)


def per_device(
    tokens,
    norm_gain,
    query_down,
    query_gain,
    latent_down,
    latent_gain,
    rope_down,
    query_up,
    key_up,
    value_up,
    glu_value,
    glu_gate,
    conv_taps,
    group_gain,
    head_proj,
    channel_proj,
):
    tok_count = tokens.shape[0]
    reach_rows = conv_taps.shape[0] // 2
    head_count = key_up.shape[1] // NOPE
    normed = rms_scale(tokens.astype(jnp.float32), norm_gain).astype(jnp.bfloat16)
    offsets = lax.axis_index("sp") * tok_count + jnp.arange(tok_count, dtype=jnp.int32)
    query_latent = jnp.dot(
        normed,
        lax.all_gather(query_down, "sp", axis=0, tiled=True),
        preferred_element_type=jnp.float32,
    )
    value_in = jnp.dot(
        normed,
        lax.all_gather(glu_value, "sp", axis=0, tiled=True),
        preferred_element_type=jnp.float32,
    )
    gate_in = jnp.dot(
        normed,
        lax.all_gather(glu_gate, "sp", axis=0, tiled=True),
        preferred_element_type=jnp.float32,
    )
    latent_query = rms_scale(query_latent, query_gain).astype(jnp.bfloat16)
    query_all = jnp.dot(latent_query, query_up, preferred_element_type=jnp.float32).reshape(
        tok_count, head_count, NOPE + ROPE
    )
    query_plain = query_all[:, :, :NOPE].astype(jnp.bfloat16)
    query_rope = rotate(query_all[:, :, NOPE:], angles_for(offsets, ROPE)[:, None, :]).astype(
        jnp.bfloat16
    )
    absorbed = jnp.einsum(
        "thd,rhd->htr",
        query_plain,
        key_up.reshape(KVR, head_count, NOPE),
        preferred_element_type=jnp.float32,
    ).astype(jnp.bfloat16)
    queries = jnp.concatenate([absorbed, jnp.transpose(query_rope, (1, 0, 2))], axis=-1)
    score_scale = (NOPE + ROPE) ** (-0.5)
    half_rows = tok_count // lax.axis_size("tp")
    first_row = lax.axis_index("tp") * half_rows
    own_rows = lax.dynamic_slice_in_dim(normed, first_row, half_rows, 0)
    own_positions = lax.dynamic_slice_in_dim(offsets, first_row, half_rows, 0)
    own_keys = key_block(own_rows, latent_down, latent_gain, rope_down, own_positions)
    block_keys = lax.all_gather(own_keys, ("sp", "tp"), axis=0, tiled=True)
    row_max = jnp.full((head_count, tok_count), far_below, jnp.float32)
    scores = (
        jnp.einsum("hqc,kc->hqk", queries, block_keys, preferred_element_type=jnp.float32)
        * score_scale
    )
    new_max = jnp.maximum(row_max, jnp.max(scores, axis=2))
    weights = jnp.exp(scores - new_max[:, :, None])
    new_sum = jnp.sum(weights, axis=2)
    added = jnp.einsum(
        "hqk,kr->hqr",
        weights.astype(jnp.bfloat16),
        block_keys[:, :KVR],
        preferred_element_type=jnp.float32,
    )
    gated_rows = (value_in * jax.nn.sigmoid(gate_in)).astype(jnp.bfloat16)
    padded = padded_2(gated_rows, (("sp", 0),), reach_rows)
    filtered = padded[0:tok_count].astype(jnp.float32) * conv_taps[0].astype(jnp.float32)
    for tap_index in range(1, conv_taps.shape[0]):
        filtered = filtered + padded[tap_index : tap_index + tok_count].astype(
            jnp.float32
        ) * conv_taps[tap_index].astype(jnp.float32)
    grouped = filtered.reshape(tok_count, -1, CH // GROUPS)
    centred = grouped - jnp.mean(grouped, axis=-1, keepdims=True)
    spread = jnp.mean(centred * centred, axis=-1, keepdims=True)
    normal_groups = (centred * lax.rsqrt(spread + norm_eps)).reshape(tok_count, -1)
    conv_branch = jax.nn.silu(normal_groups * group_gain.astype(jnp.float32)).astype(jnp.bfloat16)
    attended = (added / new_sum[:, :, None]).astype(jnp.bfloat16)
    log_weight = new_max + jnp.log(new_sum)
    head_out = jnp.einsum(
        "htr,rhv->thv",
        attended,
        value_up.reshape(KVR, head_count, VDIM),
        preferred_element_type=jnp.float32,
    )
    head_out = head_out.reshape(tok_count, head_count * VDIM).astype(jnp.bfloat16)
    mixed_in = jnp.concatenate([head_out, conv_branch], axis=1)
    out_weight = jnp.concatenate([head_proj, channel_proj], axis=0)
    partial_terms = jnp.dot(
        mixed_in,
        lax.all_gather(out_weight, "sp", axis=1, tiled=True),
        preferred_element_type=jnp.float32,
    )
    mixed_out = lax.psum_scatter(
        partial_terms.astype(jnp.bfloat16), "tp", scatter_dimension=1, tiled=True
    )
    return (mixed_out, log_weight)


LANES = 128
MESH = pl.DeviceIdType.MESH
F32 = jnp.float32
BF16 = jnp.bfloat16
Q, K, H, C, G = range(5)
PIECES = 4
RING = 28


def rope_tables(length):
    quarter = ROPE // 4
    inverse = np.float32(rope_base) ** (-np.arange(quarter, dtype=np.float32) / np.float32(quarter))
    positions = np.arange(length)
    row = (positions // GRID_W).astype(np.float32)[:, None] * inverse
    col = (positions % GRID_W).astype(np.float32)[:, None] * inverse
    angles = np.concatenate([row, col], axis=1).astype(np.float32)
    cosine, sine = np.cos(angles), np.sin(angles)
    tables = np.zeros((3, length, LANES), np.float32)
    half = ROPE // 2
    tables[0, :, :half] = cosine
    tables[0, :, half:ROPE] = cosine
    tables[1, :, :half] = -sine
    tables[2, :, half:ROPE] = sine
    return tables


def dot(a, b):
    return jnp.dot(a, b, preferred_element_type=F32)


def row_of(ref):
    return ref[...].reshape(1, -1)


def dot_nt(a, b):
    return lax.dot_general(a, b, (((1,), (1,)), ((), ())), preferred_element_type=F32)


def fused_kernel(
    n_sp,
    tokens, norm_gain_in, query_down, query_gain_in, latent_down, latent_gain_in, rope_down, query_up,
    key_up, value_up, glu_value, glu_gate, taps_in, group_gain_in, head_proj, channel_proj, tables,
    placed, log_out,
    norm_gain, query_gain, latent_gain, conv_taps, group_gain, log_v,
    w_q, w_g, w_o, tok_v, lat_v, rope_v, qup_v, kup_v, vup_v, tab_v,
    normed, keys, rope_keys, key_tmp, q_out, q_lat, q_scr, g_acc, gated, low_rows, high_rows, padded,
    mixed, parts, w_full, mixed_o, part_o, edge_in, head_acc,
    load_sem, ring_sem, z_recv, pair_recv, n_recv, np_recv, q_recv, head_recv, halo_recv, halo_send,
    conv_recv, fin_recv, out_sem, up_recv, back_recv, back_send, nr_recv, corner_recv, edge_recv,
):
    z = lax.axis_index("sp")
    c = lax.axis_index("fs")
    t = lax.axis_index("tp")
    peer = 1 - t
    c_x = c + 1 - 2 * (c % 2)
    c_y = (c + 2) % 4
    c_d = 3 - c
    others = (c_x, c_y, c_d)
    n_fs = normed.shape[0]
    n_tp = 2
    rows, width = tokens.shape
    depth, q_cols = w_q.shape[1:]
    cols = w_g.shape[2] // 2
    heads = key_up.shape[1] // NOPE
    head_rows = head_proj.shape[0]
    out_rows, out_cols = w_o.shape[1:]
    half_width = width // n_tp
    per_core = n_fs // n_tp
    half_sp = n_sp // n_tp

    def lanes_at(index, size):
        return pl.ds(pl.multiple_of(index * size, LANES), size)

    barrier = pltpu.get_barrier_semaphore()
    sides = [{"fs": c_x}, {"fs": c_y}, {"tp": peer}]
    for partner in sides:
        pl.semaphore_signal(barrier, inc=1, device_id=partner, device_id_type=MESH)

    @pl.when(z > 0)
    def _():
        pl.semaphore_signal(barrier, inc=1, device_id={"sp": z - 1}, device_id_type=MESH)

    @pl.when(z < n_sp - 1)
    def _():
        pl.semaphore_signal(barrier, inc=1, device_id={"sp": z + 1}, device_id_type=MESH)

    loads = {}

    def load(name, slot, src, dst):
        copy = pltpu.make_async_copy(src, dst, load_sem.at[slot])
        copy.start()
        loads[name] = copy

    load("tok", 0, tokens, tok_v)
    load("ng", 1, norm_gain_in, norm_gain)
    load("wq", 2, query_down.at[:, lanes_at(c, q_cols)], w_q.at[z])
    load("wv", 3, glu_value.at[:, lanes_at(c, cols)], w_g.at[z, :, pl.ds(0, cols)])
    load("wt", 4, glu_gate.at[:, lanes_at(c, cols)], w_g.at[z, :, pl.ds(cols, cols)])
    load("lat", 5, latent_down, lat_v)
    load("rope", 6, rope_down, rope_v)
    load("tab", 7, tables.at[:, pl.ds(pl.multiple_of(z * rows, LANES), rows), :], tab_v)
    load("lg", 8, latent_gain_in, latent_gain)

    def load_rest():
        load("hp", 0, head_proj.at[:, lanes_at(c, out_cols)], w_o.at[z, pl.ds(0, head_rows), :])
        load("cp", 1, channel_proj.at[:, lanes_at(c, out_cols)], w_o.at[z, pl.ds(head_rows, out_rows - head_rows), :])
        load("qup", 2, query_up, qup_v)
        load("kup", 3, key_up, kup_v)
        load("vup", 4, value_up, vup_v)
        load("qg", 5, query_gain_in, query_gain)
        load("taps", 6, taps_in.at[:, lanes_at(c, cols)], conv_taps)
        load("gg", 7, group_gain_in, group_gain)
        load("hf", 8, head_proj, w_full.at[pl.ds(0, head_rows), :])
        load("cf", 9, channel_proj, w_full.at[pl.ds(head_rows, out_rows - head_rows), :])

    loads["tok"].wait()
    loads["ng"].wait()
    values = tok_v[...].astype(F32)
    normed[c] = rms_scale(values, row_of(norm_gain)).astype(BF16)
    for name in ("wq", "wv", "wt"):
        loads[name].wait()

    ends = (z == 0).astype(jnp.int32) + (z == n_sp - 1).astype(jnp.int32)
    pl.semaphore_wait(barrier, len(sides) + 2 - ends)

    sent = []

    def when(cond, action):
        if cond is None:
            action()
        else:
            pl.when(cond)(action)

    def both(first, second):
        return second if first is None else first & second

    def remote(src, dst, recv_sem, device):
        def make(send_sem):
            return pltpu.make_async_remote_copy(
                src_ref=src, dst_ref=dst, send_sem=send_sem, recv_sem=recv_sem,
                device_id=device, device_id_type=MESH,
            )

        return make

    def drain(entry):
        copy, cond = entry
        when(cond, copy.wait_send)

    def send(make, cond=None):
        slot = len(sent) % RING
        if len(sent) >= RING:
            drain(sent[-RING])
        copy = make(ring_sem.at[slot])
        when(cond, copy.start)
        sent.append((copy, cond))

    def arrive(make):
        make(ring_sem.at[0]).wait_recv()

    def arrive_all(like, recv_sem):
        arrive(remote(like, like, recv_sem, {"tp": peer}))

    q_half = depth // n_tp
    piece = depth // PIECES
    k_half = rows // n_tp
    inner = (z > 0) & (z < n_sp - 1)
    at_end = jnp.logical_not(inner)
    lower = 2 * z < n_sp
    outer = jnp.where(lower, 0, n_sp - 1)
    near = jnp.where(lower, 1, n_sp - 2)
    far = jnp.where(lower, n_sp - 2, 1)
    neighbour = jnp.where(lower, z + 1, z - 1)

    def half(first, size):
        return pl.ds(pl.multiple_of(first * size, 16), size)

    def block(u, shard, side=t):
        if u == Q:
            return w_q.at[shard, half(side, q_half), :]
        if u == K:
            return keys.at[shard, side]
        if u == H:
            return w_o.at[shard, pl.ds(0, head_rows), :]
        if u == C:
            return w_o.at[shard, pl.ds(head_rows, out_rows - head_rows), :]
        return w_g.at[shard, pl.ds((u - G) * piece, piece), :]

    def slot_of(shard, at):
        return shard - (shard > at).astype(jnp.int32)

    def z_copy(u, shard, target):
        ref = block(u, shard)
        return remote(ref, ref, z_recv.at[u, slot_of(shard, target)], {"sp": target})

    def z_arrive(u, shard):
        ref = block(u, shard)
        arrive(remote(ref, ref, z_recv.at[u, slot_of(shard, z)], {"sp": neighbour}))

    def send_own(u, cond=None):
        skip = 1 if u in (H, C) else 0
        send(z_copy(u, z, z - 1), both(cond, z > skip))
        send(z_copy(u, z, z + 1), both(cond, z < n_sp - 1 - skip))

    nearest = jnp.minimum(z, n_sp - 1 - z)
    arrivals = []
    for k in range(n_sp - 1):
        two_sided = k < 2 * nearest
        distance = jnp.where(two_sided, k // 2 + 1, k - nearest + 1)
        from_low = jnp.where(two_sided, 1 - k % 2, (2 * z > n_sp - 1).astype(jnp.int32))
        arrivals.append((z - distance * (2 * from_low - 1), z + 2 * from_low - 1))

    def pass_on(u, shard, target):
        when(inner, lambda: z_arrive(u, shard))
        send(z_copy(u, shard, target), inner)

    def relay(u, k):
        pass_on(u, *arrivals[k])

    def both_ways(u):
        pass_on(u, outer, far)
        pass_on(u, far, outer)

    def settle(u, k):
        when(at_end, lambda: z_arrive(u, arrivals[k][0]))

    def pair(u, shard, side):
        ref = block(u, shard, side)
        return remote(ref, ref, pair_recv.at[u], {"tp": peer})

    def share(u, k):
        settle(u, k)
        send(pair(u, arrivals[k][0], t))

    quarter_width = half_width // 2

    def n_block(owner, part):
        return normed.at[owner, :, lanes_at(2 * t + part, quarter_width)]

    def n_copy(i, part):
        ref = n_block(c, part)
        return remote(ref, ref, n_recv.at[i, part], {"fs": others[i]})

    def n_relay(i):
        ref = n_block(others[i], i)
        return remote(ref, ref, nr_recv.at[i], {"fs": others[1 - i]})

    def n_pair(i, side):
        ref = normed.at[others[i], :, lanes_at(side, half_width)]
        return remote(ref, ref, np_recv.at[0], {"tp": peer})

    def pass_normed(i):
        arrive(n_copy(i, i))
        send(n_relay(i))

    def share_normed(i):
        if i < 2:
            arrive(n_copy(i, 1 - i))
        else:
            for j in range(2):
                arrive(n_relay(j))
        send(n_pair(i, t))

    send_own(Q)
    for part in range(2):
        send(n_copy(0, part))
        send(n_copy(1, 1 - part))

    def rotate_lanes(v):
        step = ROPE // 2
        return (
            v * tab_v[0] + pltpu.roll(v, LANES - step, 1) * tab_v[1] + pltpu.roll(v, step, 1) * tab_v[2]
        )

    loads["lat"].wait()
    loads["lg"].wait()
    own_normed = normed[c]
    latent = rms_scale(dot(own_normed, lat_v[...]), row_of(latent_gain))
    keys[z, :, 0:k_half, :] = latent.astype(BF16).reshape(n_tp, k_half, KVR)
    loads["rope"].wait()
    loads["tab"].wait()
    key_tmp[...] = jnp.zeros_like(key_tmp)
    key_tmp[:, 0:ROPE] = dot_nt(own_normed, rope_v[...])
    rotated = rotate_lanes(key_tmp[...])
    fold = KVR // ROPE
    strip = k_half // fold
    for side in range(n_tp):
        for pair_of in range(fold // 2):
            first = side * k_half + 2 * pair_of * strip
            packed = rotated[first : first + strip, :] + pltpu.roll(
                rotated[first + strip : first + 2 * strip, :], ROPE, 1
            )
            keys[z, side, k_half : k_half + strip, pair_of * LANES : (pair_of + 1) * LANES] = packed.astype(BF16)
    send_own(K)
    send_own(G)
    send_own(G + 1)
    load_rest()

    last = n_sp - 2
    both_ways(Q)
    pass_normed(0)
    pass_normed(1)
    both_ways(K)
    share(Q, 0)
    send_own(G + 2)
    relay(Q, last)
    send_own(G + 3)
    both_ways(G)
    share_normed(0)
    share_normed(1)
    relay(K, last)
    both_ways(G + 1)
    for k in range(1, last):
        share(Q, k)
    share_normed(2)
    share(Q, last)
    for p in range(2, PIECES):
        both_ways(G + p)

    arrive_all(normed.at[pl.ds(0, n_fs - 1), :, lanes_at(peer, half_width)], np_recv.at[0])
    halo = low_rows.shape[1]
    edge_rows = pl.ds(pl.multiple_of(jnp.where(lower, rows - halo, 0), 16), halo)
    edge_half = edge_in.at[:, :, lanes_at(t, half_width)]
    edge_copy = remote(normed.at[:, edge_rows, lanes_at(t, half_width)], edge_half, edge_recv.at[0], {"sp": near})
    edge_pair = remote(edge_half, edge_half, edge_recv.at[1], {"tp": peer})
    arrive_all(w_q.at[pl.ds(0, n_sp - 1), half(peer, q_half), :], pair_recv.at[Q])
    seqs = normed[pl.ds(per_core * t, per_core)].reshape(per_core * rows, width)
    q_out[...] = dot(seqs, w_q[...].reshape(n_sp * depth, q_cols)).reshape(per_core, rows, q_cols)

    for i in range(per_core):
        seq = per_core * t + i
        for core in (peer, t):
            copy = remote(q_out.at[i], q_lat.at[c], q_recv.at[0], {"fs": seq, "tp": core})
            send(copy, None if core is peer else seq != c)

        @pl.when(seq == c)
        def _():
            q_lat[c] = q_out[i]

    for name in ("hp", "cp"):
        loads[name].wait()
    send_own(H, at_end)
    send(edge_copy, at_end)
    send_own(C, at_end)

    def add_shard(shard, first=False):
        rows_in = normed[:, :, lanes_at(shard, depth)].reshape(n_fs * rows, depth)
        term = dot(rows_in, w_g[shard])
        g_acc[...] = term if first else g_acc[...] + term

    up_copy = remote(
        gated.at[:, pl.ds(rows - halo, halo), :], low_rows, halo_recv.at[0], {"sp": z + 1}
    )(halo_send.at[0])
    down_copy = remote(
        gated.at[:, pl.ds(0, halo), :], high_rows, halo_recv.at[1], {"sp": z - 1}
    )(halo_send.at[1])

    def add_arrival(k):
        for p in range(PIECES):
            settle(G + p, k)
        add_shard(arrivals[k][0])

    def gate():
        gated[...] = gate_of(g_acc[...]).reshape(n_fs, rows, cols)

        @pl.when(inner)
        def _():
            up_copy.start()
            down_copy.start()

    def gate_of(acc):
        return (acc[:, 0:cols] * jax.nn.sigmoid(acc[:, cols : 2 * cols])).astype(BF16)

    def edge():
        arrive(edge_pair)
        acc = dot(edge_in[...].reshape(n_fs * halo, width), w_g[...].reshape(n_sp * depth, 2 * cols))
        values = gate_of(acc).astype(F32).reshape(n_fs, halo, cols)

        @pl.when(lower)
        def _():
            padded[:, 0:halo, :] = values

        @pl.when(jnp.logical_not(lower))
        def _():
            padded[:, halo + rows : 2 * halo + rows, :] = values

    for p in range(2):
        relay(G + p, last)
    for k in range(last):
        share(K, k)
    add_shard(z, True)
    for p in range(2, PIECES):
        relay(G + p, last)
    share(K, last)

    add_arrival(0)

    send_own(H, inner)

    @pl.when(inner)
    def _():
        for k in range(1, n_sp - 1):
            add_arrival(k)
        gate()

    send_own(C, inner)
    for name in ("qup", "kup", "vup", "qg", "taps", "gg"):
        loads[name].wait()

    here = t == c // per_core

    @pl.when(here)
    def _():
        arrive_all(q_lat.at[pl.ds(0, n_fs - 1)], q_recv.at[0])

    @pl.when(jnp.logical_not(here))
    def _():
        arrive_all(q_lat, q_recv.at[0])

    pass_on(H, outer, far)
    whole_q = jnp.concatenate([q_lat[i] for i in range(n_fs)], axis=1)
    latent_query = rms_scale(whole_q, row_of(query_gain)).astype(BF16)
    q_scr[...] = dot(latent_query, qup_v[...])
    arrive_all(keys.at[pl.ds(0, n_sp - 1), peer], pair_recv.at[K])

    key_lane = lax.broadcasted_iota(jnp.int32, (strip, LANES), 1)
    for shard in range(n_sp):
        for side in range(n_tp):
            for pair_of in range(fold // 2):
                packed = keys[
                    shard, side, k_half : k_half + strip, pair_of * LANES : (pair_of + 1) * LANES
                ].astype(F32)
                for part, values in enumerate((packed, pltpu.roll(packed, ROPE, 1))):
                    first = (shard * n_tp + side) * k_half + (2 * pair_of + part) * strip
                    rope_keys[first : first + strip, :] = jnp.where(key_lane < ROPE, values, 0.0).astype(BF16)

    def attend(h, shifted):
        start = h * (NOPE + ROPE)
        source = q_scr[...]
        if start % LANES:
            source, start = shifted, start - ROPE
        plain = source[:, start : start + NOPE].astype(BF16)
        rope_part = rotate_lanes(source[:, start + NOPE : start + NOPE + LANES]).astype(BF16)
        absorbed = dot_nt(plain, kup_v[:, h * NOPE : (h + 1) * NOPE]).astype(BF16)
        latents = keys[:, :, 0:k_half, :].reshape(n_sp * rows, KVR)
        scores = (dot_nt(absorbed, latents) + dot_nt(rope_part, rope_keys[...])) * (NOPE + ROPE) ** (-0.5)
        row_max = jnp.max(scores, axis=1, keepdims=True)
        weights = jnp.exp(scores - row_max)
        total = jnp.sum(weights, axis=1, keepdims=True)
        added = dot(weights.astype(BF16), latents)
        attended = (added / total).astype(BF16)
        head_out = dot(attended, vup_v[:, h * VDIM : (h + 1) * VDIM])
        mixed[c, :, h * VDIM : (h + 1) * VDIM] = head_out.astype(BF16)
        return row_max + jnp.log(total)

    def head_ref(owner, h):
        return mixed.at[owner, :, pl.ds(2 * h * VDIM, 2 * VDIM)]

    def head_copy(h, i):
        ref = head_ref(c, h)
        return remote(ref, ref, head_recv.at[h if h == i else 2], {"fs": others[i]})

    def head_relay(h):
        ref = head_ref(others[h], h)
        return remote(ref, ref, head_recv.at[2], {"fs": others[1 - h]})

    def pass_head(h, cond):
        when(cond, lambda: arrive(head_copy(h, h)))
        send(head_relay(h), cond)

    whole = q_scr[...]
    shifted = pltpu.roll(whole, whole.shape[1] - ROPE, 1)
    lane = lax.broadcasted_iota(jnp.int32, (rows, LANES), 1)
    logs = jnp.zeros((rows, LANES), F32)

    def to_near(group):
        lanes = lanes_at(group, cols) if isinstance(group, jax.Array) or group >= heads else pl.ds(2 * group * cols, 2 * cols)
        return remote(mixed.at[c, :, lanes], mixed_o.at[:, lanes], up_recv.at[0], {"sp": near})

    for h in range(heads):
        logs = jnp.where(lane == h, attend(h, shifted), logs)
        if h % 2:
            for i in range(2):
                send(head_copy(h // 2, i))
            send(to_near(h // 2), at_end)
        if h == 1:
            when(inner, lambda: arrive(edge_copy))
            send(edge_pair, inner)
    log_v[...] = jnp.transpose(logs)[0:heads, :]
    log_copy = pltpu.make_async_copy(log_v, log_out, out_sem.at[0])
    log_copy.start()
    pass_on(H, far, outer)

    @pl.when(at_end)
    def _():
        for k in range(1, last):
            add_arrival(k)

    for h in range(2):
        pass_head(h, at_end)

    @pl.when(at_end)
    def _():
        add_arrival(last)
        gate()

    @pl.when(inner)
    def _():
        edge()

    reach = conv_taps.shape[0] // 2
    padded[:, halo : halo + rows, :] = gated[...].astype(F32)

    @pl.when(z > 1)
    def _():
        up_copy.wait_recv()
        padded[:, 0:halo, :] = low_rows[...].astype(F32)

    @pl.when(z == 0)
    def _():
        padded[:, 0:halo, :] = jnp.zeros((n_fs, halo, cols), F32)

    @pl.when(z < n_sp - 2)
    def _():
        down_copy.wait_recv()
        padded[:, halo + rows : 2 * halo + rows, :] = high_rows[...].astype(F32)

    @pl.when(z == n_sp - 1)
    def _():
        padded[:, halo + rows : 2 * halo + rows, :] = jnp.zeros((n_fs, halo, cols), F32)

    def conv_ref(s, group):
        return mixed.at[s, :, pl.ds(pl.multiple_of(head_rows + group * cols, LANES), cols)]

    def conv_copy(s, i, slot=4):
        ref = conv_ref(s, c)
        return remote(ref, ref, conv_recv.at[slot], {"fs": others[i]})

    def conv_corner():
        ref = conv_ref(c_d, c)
        return remote(ref, ref, corner_recv.at[0], {"fs": c_d})

    def conv_corner_in():
        ref = conv_ref(c, c_d)
        return remote(ref, ref, corner_recv.at[0], {"fs": c_d})

    def conv_relay(s, i):
        ref = conv_ref(s, others[i])
        return remote(ref, ref, conv_recv.at[4], {"fs": others[1 - i]})

    taps = conv_taps[...].astype(F32)
    all_gains = row_of(group_gain).astype(F32)
    gains = all_gains[:, 0:cols]
    for i in range(1, n_fs):
        gains = jnp.where(c == i, all_gains[:, i * cols : (i + 1) * cols], gains)
    def conv_seq(s):
        filtered = jnp.zeros((rows, cols), F32)
        for j in range(conv_taps.shape[0]):
            first = halo - reach + j
            filtered = filtered + padded[s, first : first + rows, :] * taps[j : j + 1, :]
        centred = filtered - jnp.mean(filtered, axis=1, keepdims=True)
        spread = jnp.mean(centred * centred, axis=1, keepdims=True)
        branch = centred * lax.rsqrt(spread + norm_eps) * gains
        branch = branch * jax.nn.sigmoid(branch)
        mixed[s, :, pl.ds(pl.multiple_of(head_rows + c * cols, LANES), cols)] = branch.astype(BF16)

    conv_seq(c_d)
    send(conv_corner())
    conv_seq(c_x)
    send(conv_copy(c_x, 0, 0))
    conv_seq(c_y)
    send(conv_copy(c_y, 1, 2))
    conv_seq(c)
    send(to_near(heads + c), at_end)
    for s, i, slot in ((c, 0, 1), (c_d, 1, 4), (c_y, 0, 4), (c, 1, 4), (c_d, 0, 4), (c_x, 1, 3)):
        send(conv_copy(s, i, slot))
    pass_on(C, outer, far)
    pass_on(C, far, outer)
    for h in range(2):
        pass_head(h, inner)
    relay(H, last)
    arrive(conv_copy(c, 0, 0))
    send(to_near(heads + c_x), at_end)
    arrive(conv_copy(c, 1, 2))
    send(to_near(heads + c_y), at_end)
    send(conv_relay(c, 1))
    arrive(conv_corner_in())
    send(to_near(heads + c_d), at_end)
    for s, i, slot in ((c_x, 0, 1), (c_d, 1, 3)):
        arrive(conv_copy(s, i, slot))
        send(conv_relay(s, i))
    relay(C, last)
    arrive_all(parts.at[pl.ds(0, 2)], head_recv.at[2])

    def head_part(shard):
        head_acc[shard] = dot(mixed[:, :, 0:head_rows].reshape(n_fs * rows, head_rows), w_o[shard, 0:head_rows, :])

    head_part(z)
    settle(H, 1)
    head_part(arrivals[1][0])

    @pl.when(inner)
    def _():
        head_part(arrivals[0][0])
        for k in range(2, n_sp - 1):
            head_part(arrivals[k][0])

    rest = (2 * n_fs - 1) * rows
    arrive_all(w_o.at[0, pl.ds(0, rest), :], conv_recv.at[4])

    def place(core, shard):
        first = (shard % half_sp) * (n_fs * out_cols) + c * out_cols
        return placed.at[core, :, pl.ds(pl.multiple_of(first, LANES), out_cols)]

    def fin_copy(shard, j):
        seq = others[j] if j < len(others) else c
        return remote(
            parts.at[shard, pl.ds(pl.multiple_of(seq * rows, LANES), rows), :], place(t, shard),
            fin_recv.at[t, shard % half_sp], {"fs": seq, "tp": shard // half_sp},
        )

    def keep_copy(shard):
        ref = parts.at[shard, pl.ds(pl.multiple_of(c * rows, LANES), rows), :]
        return pltpu.make_async_copy(ref, place(t, shard), out_sem.at[1 + shard % half_sp])

    def add_part(shard, cond=None):
        def compute():
            part = head_acc[shard] + dot(
                mixed[:, :, head_rows:out_rows].reshape(n_fs * rows, out_rows - head_rows), w_o[shard, head_rows:out_rows, :]
            )
            parts[shard] = part.astype(BF16)

        when(cond, compute)
        for j in (2, 0, 1):
            send(fin_copy(shard, j), cond)
        mine = shard // half_sp == t
        send(fin_copy(shard, len(others)), both(cond, jnp.logical_not(mine)))
        when(both(cond, mine), lambda: keep_copy(shard).start())

    add_part(z)
    add_part(arrivals[0][0], inner)
    settle(C, 1)
    add_part(arrivals[1][0])
    for k in range(2, n_sp - 1):
        settle(H, k)

        @pl.when(at_end)
        def _():
            head_part(arrivals[k][0])

        settle(C, k)
        add_part(arrivals[k][0])

    back_lanes = lanes_at(z % half_sp, n_fs * out_cols)
    back_copy = remote(
        part_o, placed.at[t, :, back_lanes], back_recv.at[0], {"sp": outer, "tp": z // half_sp}
    )(back_send.at[0])
    for name in ("hf", "cf"):
        loads[name].wait()

    def neighbour_part():
        arrive_all(mixed_o, up_recv.at[0])
        part_o[...] = dot(mixed_o[...], w_full[...]).astype(BF16)
        back_copy.start()

    @pl.when(inner)
    def _():
        neighbour_part()

    for entry in sent[-RING:]:
        drain(entry)

    @pl.when(inner)
    def _():
        up_copy.wait_send()
        down_copy.wait_send()
        back_copy.wait_send()

    for i in range(half_sp):
        shard = t * half_sp + i
        computed = inner | (shard != near)

        @pl.when(computed)
        def _():
            arrive_all(parts.at[0, pl.ds(0, (n_fs - 1) * rows), :], fin_recv.at[t, i])
            arrive_all(parts.at[0], fin_recv.at[peer, i])
            keep_copy(shard).wait()

        @pl.when(jnp.logical_not(computed))
        def _():
            arrive_all(parts.at[pl.ds(0, n_tp)], back_recv.at[0])
    log_copy.wait()


def finish_kernel(placed, log_in, out, log_out, held, summed, log_v, load_sem, store_sem):
    span = out.shape[1] // 2
    logs = pltpu.make_async_copy(log_in, log_v, load_sem.at[2])
    loads = [
        pltpu.make_async_copy(placed.at[:, :, pl.ds(i * span, span)], held.at[i], load_sem.at[i]) for i in range(2)
    ]
    for copy in loads:
        copy.start()
    logs.start()
    stores = [
        pltpu.make_async_copy(summed.at[i], out.at[:, pl.ds(i * span, span)], store_sem.at[i]) for i in range(2)
    ]
    for i in range(2):
        loads[i].wait()
        summed[i] = (held[i, 0].astype(F32) + held[i, 1].astype(F32)).astype(BF16)
        stores[i].start()
    logs.wait()
    stores.append(pltpu.make_async_copy(log_v, log_out, store_sem.at[2]))
    stores[2].start()
    for copy in stores:
        copy.wait()


def fused_device(n_sp, n_fs, *args):
    (tokens, norm_gain, query_down, query_gain, latent_down, latent_gain, rope_down, query_up,
     key_up, value_up, glu_value, glu_gate, conv_taps, group_gain, head_proj, channel_proj) = args
    rows, width = tokens.shape
    depth, q_rank = query_down.shape
    cols = glu_value.shape[1] // n_fs
    heads = key_up.shape[1] // NOPE
    out_rows = head_proj.shape[0] + channel_proj.shape[0]
    out_cols = head_proj.shape[1] // n_fs
    q_cols = q_rank // n_fs
    halo = (conv_taps.shape[0] // 2 + 15) // 16 * 16
    tables = jnp.asarray(rope_tables(n_sp * rows))
    hbm = pl.BlockSpec(memory_space=pltpu.HBM)
    operands = [
        tokens, norm_gain, query_down, query_gain, latent_down, latent_gain, rope_down.T, query_up,
        key_up, value_up, glu_value, glu_gate, conv_taps, group_gain, head_proj, channel_proj, tables,
    ]
    like = lambda a: pltpu.VMEM(a.shape, a.dtype)
    dma = pltpu.SemaphoreType.DMA
    half_sp = n_sp // 2
    scratch = [
        like(norm_gain), like(query_gain), like(latent_gain), pltpu.VMEM((conv_taps.shape[0], cols), BF16), like(group_gain),
        pltpu.VMEM((heads, rows), F32),
        pltpu.VMEM((n_sp, depth, q_cols), BF16),
        pltpu.VMEM((n_sp, depth, 2 * cols), BF16),
        pltpu.VMEM((n_sp, out_rows, out_cols), BF16),
        like(tokens), like(latent_down), pltpu.VMEM(rope_down.shape[::-1], BF16), like(query_up), like(key_up), like(value_up),
        pltpu.VMEM((3, rows, LANES), F32),
        pltpu.VMEM((n_fs, rows, width), BF16),
        pltpu.VMEM((n_sp, 2, rows // 2 + rows // 2 * ROPE // KVR, KVR), BF16),
        pltpu.VMEM((n_sp * rows, LANES), BF16),
        pltpu.VMEM((rows, LANES), F32),
        pltpu.VMEM((n_fs // 2, rows, q_cols), F32),
        pltpu.VMEM((n_fs, rows, q_cols), F32),
        pltpu.VMEM((rows, query_up.shape[1]), F32),
        pltpu.VMEM((n_fs * rows, 2 * cols), F32),
        pltpu.VMEM((n_fs, rows, cols), BF16),
        pltpu.VMEM((n_fs, halo, cols), BF16),
        pltpu.VMEM((n_fs, halo, cols), BF16),
        pltpu.VMEM((n_fs, rows + 2 * halo, cols), F32),
        pltpu.VMEM((n_fs, rows, out_rows), BF16),
        pltpu.VMEM((n_sp, n_fs * rows, out_cols), BF16),
        pltpu.VMEM((out_rows, n_fs * out_cols), BF16),
        pltpu.VMEM((rows, out_rows), BF16),
        pltpu.VMEM((rows, n_fs * out_cols), BF16),
        pltpu.VMEM((n_fs, halo, width), BF16),
        pltpu.VMEM((n_sp, n_fs * rows, out_cols), F32),
        dma((10,)), dma((RING,)), dma((G + PIECES, n_sp - 1)), dma((2,)), dma((2, 2)), dma((1,)), dma((1,)),
        dma((3,)), dma((2,)), dma((2,)), dma((5,)), dma((2, half_sp)), dma((1 + half_sp,)),
        dma((1,)), dma((1,)), dma((1,)), dma((2,)), dma((1,)), dma((2,)),
    ]
    shapes = (
        jax.ShapeDtypeStruct((rows, half_sp * n_fs * out_cols), BF16),
        jax.ShapeDtypeStruct((heads, rows), F32),
    )
    placed, logs = pl.pallas_call(
        functools.partial(fused_kernel, n_sp),
        out_shape=(jax.ShapeDtypeStruct((2,) + shapes[0].shape, BF16), shapes[1]),
        in_specs=[hbm] * len(operands),
        out_specs=(hbm, hbm),
        scratch_shapes=scratch,
        compiler_params=pltpu.CompilerParams(
            collective_id=0, has_side_effects=True, vmem_limit_bytes=63 * 1024 * 1024
        ),
        name="fused_layer",
    )(*operands)
    span = shapes[0].shape[1] // 2
    return pl.pallas_call(
        finish_kernel,
        out_shape=shapes,
        in_specs=[hbm] * 2,
        out_specs=(hbm, hbm),
        scratch_shapes=[
            pltpu.VMEM((2, 2, rows, span), BF16), pltpu.VMEM((2, rows, span), BF16), pltpu.VMEM((heads, rows), F32),
            dma((3,)), dma((3,)),
        ],
        name="finish",
    )(placed, logs)


def solution(mesh):
    in_specs = (
        P(("fs", "sp"), None),
        P(),
        P("sp", None),
        P(),
        P(),
        P(),
        P(),
        P(None, "tp"),
        P(None, "tp"),
        P(None, "tp"),
        P("sp", "tp"),
        P("sp", "tp"),
        P(None, "tp"),
        P("tp"),
        P("tp", "sp"),
        P("tp", "sp"),
    )
    out_specs = (P(("fs", "sp"), "tp"), P("tp", ("fs", "sp")))
    body = per_device
    if mesh.shape["fs"] == 4 and mesh.shape["tp"] == 2 and mesh.shape["sp"] == 4:
        body = functools.partial(fused_device, mesh.shape["sp"], mesh.shape["fs"])
    return jax.shard_map(
        body, mesh=mesh, in_specs=in_specs, out_specs=out_specs, check_vma=False
    )
```

```python
import functools

import jax
import jax.numpy as jnp
import numpy as np
from jax import lax
from jax.experimental import pallas as pl
from jax.experimental.pallas import tpu as pltpu
from jax.sharding import PartitionSpec as P

NOPE = 128
ROPE = 64
VDIM = 128
KVR = 256
CH = 1024
GROUPS = 8
GRID_W = 64


norm_eps = 1e-06
rope_base = 10000.0
far_below = -1e30


def padded_2(block, sides, width):
    for axis, dim in sides:
        count = lax.axis_size(axis)
        forward = [(i, i + 1) for i in range(count - 1)]
        backward = [(target, source) for source, target in forward]
        low = lax.ppermute(
            lax.slice_in_dim(block, block.shape[dim] - width, None, axis=dim), axis, forward
        )
        high = lax.ppermute(lax.slice_in_dim(block, 0, width, axis=dim), axis, backward)
        block = jnp.concatenate([low, block, high], axis=dim)
    return block


def rms_scale(values, scale_gain):
    inv_rms = lax.rsqrt(jnp.mean(values * values, axis=-1, keepdims=True) + norm_eps)
    return values * inv_rms * scale_gain.astype(jnp.float32)


def angles_for(positions, rope_size):
    quarter = rope_size // 4
    inverse = rope_base ** (-jnp.arange(quarter, dtype=jnp.float32) / quarter)
    grid_row = (positions // GRID_W).astype(jnp.float32)
    grid_col = (positions % GRID_W).astype(jnp.float32)
    return jnp.concatenate([grid_row[:, None] * inverse, grid_col[:, None] * inverse], axis=-1)


def rotate(values, angles):
    half_size = values.shape[-1] // 2
    front_half = values[..., :half_size]
    back_half = values[..., half_size:]
    cosine = jnp.cos(angles)
    sine_part = jnp.sin(angles)
    return jnp.concatenate(
        [front_half * cosine - back_half * sine_part, back_half * cosine + front_half * sine_part],
        axis=-1,
    )


def key_block(normed, latent_down, latent_gain, rope_down, positions):
    latent = jnp.dot(normed, latent_down, preferred_element_type=jnp.float32)
    latent = rms_scale(latent, latent_gain).astype(jnp.bfloat16)
    rope_key = jnp.dot(normed, rope_down, preferred_element_type=jnp.float32)
    rope_key = rotate(rope_key, angles_for(positions, rope_key.shape[-1])).astype(jnp.bfloat16)
    return jnp.concatenate([latent, rope_key], axis=1)


def per_device(
    tokens,
    norm_gain,
    query_down,
    query_gain,
    latent_down,
    latent_gain,
    rope_down,
    query_up,
    key_up,
    value_up,
    glu_value,
    glu_gate,
    conv_taps,
    group_gain,
    head_proj,
    channel_proj,
):
    tok_count = tokens.shape[0]
    reach_rows = conv_taps.shape[0] // 2
    head_count = key_up.shape[1] // NOPE
    normed = rms_scale(tokens.astype(jnp.float32), norm_gain).astype(jnp.bfloat16)
    offsets = lax.axis_index("sp") * tok_count + jnp.arange(tok_count, dtype=jnp.int32)
    query_latent = jnp.dot(
        normed,
        lax.all_gather(query_down, "sp", axis=0, tiled=True),
        preferred_element_type=jnp.float32,
    )
    value_in = jnp.dot(
        normed,
        lax.all_gather(glu_value, "sp", axis=0, tiled=True),
        preferred_element_type=jnp.float32,
    )
    gate_in = jnp.dot(
        normed,
        lax.all_gather(glu_gate, "sp", axis=0, tiled=True),
        preferred_element_type=jnp.float32,
    )
    latent_query = rms_scale(query_latent, query_gain).astype(jnp.bfloat16)
    query_all = jnp.dot(latent_query, query_up, preferred_element_type=jnp.float32).reshape(
        tok_count, head_count, NOPE + ROPE
    )
    query_plain = query_all[:, :, :NOPE].astype(jnp.bfloat16)
    query_rope = rotate(query_all[:, :, NOPE:], angles_for(offsets, ROPE)[:, None, :]).astype(
        jnp.bfloat16
    )
    absorbed = jnp.einsum(
        "thd,rhd->htr",
        query_plain,
        key_up.reshape(KVR, head_count, NOPE),
        preferred_element_type=jnp.float32,
    ).astype(jnp.bfloat16)
    queries = jnp.concatenate([absorbed, jnp.transpose(query_rope, (1, 0, 2))], axis=-1)
    score_scale = (NOPE + ROPE) ** (-0.5)
    half_rows = tok_count // lax.axis_size("tp")
    first_row = lax.axis_index("tp") * half_rows
    own_rows = lax.dynamic_slice_in_dim(normed, first_row, half_rows, 0)
    own_positions = lax.dynamic_slice_in_dim(offsets, first_row, half_rows, 0)
    own_keys = key_block(own_rows, latent_down, latent_gain, rope_down, own_positions)
    block_keys = lax.all_gather(own_keys, ("sp", "tp"), axis=0, tiled=True)
    row_max = jnp.full((head_count, tok_count), far_below, jnp.float32)
    scores = (
        jnp.einsum("hqc,kc->hqk", queries, block_keys, preferred_element_type=jnp.float32)
        * score_scale
    )
    new_max = jnp.maximum(row_max, jnp.max(scores, axis=2))
    weights = jnp.exp(scores - new_max[:, :, None])
    new_sum = jnp.sum(weights, axis=2)
    added = jnp.einsum(
        "hqk,kr->hqr",
        weights.astype(jnp.bfloat16),
        block_keys[:, :KVR],
        preferred_element_type=jnp.float32,
    )
    gated_rows = (value_in * jax.nn.sigmoid(gate_in)).astype(jnp.bfloat16)
    padded = padded_2(gated_rows, (("sp", 0),), reach_rows)
    filtered = padded[0:tok_count].astype(jnp.float32) * conv_taps[0].astype(jnp.float32)
    for tap_index in range(1, conv_taps.shape[0]):
        filtered = filtered + padded[tap_index : tap_index + tok_count].astype(
            jnp.float32
        ) * conv_taps[tap_index].astype(jnp.float32)
    grouped = filtered.reshape(tok_count, -1, CH // GROUPS)
    centred = grouped - jnp.mean(grouped, axis=-1, keepdims=True)
    spread = jnp.mean(centred * centred, axis=-1, keepdims=True)
    normal_groups = (centred * lax.rsqrt(spread + norm_eps)).reshape(tok_count, -1)
    conv_branch = jax.nn.silu(normal_groups * group_gain.astype(jnp.float32)).astype(jnp.bfloat16)
    attended = (added / new_sum[:, :, None]).astype(jnp.bfloat16)
    log_weight = new_max + jnp.log(new_sum)
    head_out = jnp.einsum(
        "htr,rhv->thv",
        attended,
        value_up.reshape(KVR, head_count, VDIM),
        preferred_element_type=jnp.float32,
    )
    head_out = head_out.reshape(tok_count, head_count * VDIM).astype(jnp.bfloat16)
    mixed_in = jnp.concatenate([head_out, conv_branch], axis=1)
    out_weight = jnp.concatenate([head_proj, channel_proj], axis=0)
    partial_terms = jnp.dot(
        mixed_in,
        lax.all_gather(out_weight, "sp", axis=1, tiled=True),
        preferred_element_type=jnp.float32,
    )
    mixed_out = lax.psum_scatter(
        partial_terms.astype(jnp.bfloat16), "tp", scatter_dimension=1, tiled=True
    )
    return (mixed_out, log_weight)


LANES = 128
MESH = pl.DeviceIdType.MESH
F32 = jnp.float32
BF16 = jnp.bfloat16
Q, K, H, C, G = range(5)
PIECES = 4
RING = 28


def rope_tables(length):
    quarter = ROPE // 4
    inverse = np.float32(rope_base) ** (-np.arange(quarter, dtype=np.float32) / np.float32(quarter))
    positions = np.arange(length)
    row = (positions // GRID_W).astype(np.float32)[:, None] * inverse
    col = (positions % GRID_W).astype(np.float32)[:, None] * inverse
    angles = np.concatenate([row, col], axis=1).astype(np.float32)
    cosine, sine = np.cos(angles), np.sin(angles)
    tables = np.zeros((3, length, LANES), np.float32)
    half = ROPE // 2
    tables[0, :, :half] = cosine
    tables[0, :, half:ROPE] = cosine
    tables[1, :, :half] = -sine
    tables[2, :, half:ROPE] = sine
    return tables


def dot(a, b):
    return jnp.dot(a, b, preferred_element_type=F32)


def row_of(ref):
    return ref[...].reshape(1, -1)


def dot_nt(a, b):
    return lax.dot_general(a, b, (((1,), (1,)), ((), ())), preferred_element_type=F32)


def fused_kernel(
    n_sp,
    tokens, norm_gain_in, query_down, query_gain_in, latent_down, latent_gain_in, rope_down, query_up,
    key_up, value_up, glu_value, glu_gate, taps_in, group_gain_in, head_proj, channel_proj, tables,
    placed, log_out,
    norm_gain, query_gain, latent_gain, conv_taps, group_gain, log_v,
    w_q, w_g, w_o, tok_v, lat_v, rope_v, qup_v, kup_v, vup_v, tab_v,
    normed, keys, rope_keys, key_tmp, q_out, q_lat, q_scr, g_acc, gated, low_rows, high_rows, padded,
    mixed, parts, w_full, mixed_o, part_o, edge_in, head_acc,
    load_sem, ring_sem, z_recv, pair_recv, n_recv, np_recv, q_recv, head_recv, halo_recv, halo_send,
    conv_recv, fin_recv, out_sem, up_recv, back_recv, back_send, nr_recv, corner_recv, edge_recv,
):
    z = lax.axis_index("sp")
    c = lax.axis_index("fs")
    t = lax.axis_index("tp")
    peer = 1 - t
    c_x = c + 1 - 2 * (c % 2)
    c_y = (c + 2) % 4
    c_d = 3 - c
    others = (c_x, c_y, c_d)
    n_fs = normed.shape[0]
    n_tp = 2
    rows, width = tokens.shape
    depth, q_cols = w_q.shape[1:]
    cols = w_g.shape[2] // 2
    heads = key_up.shape[1] // NOPE
    head_rows = head_proj.shape[0]
    out_rows, out_cols = w_o.shape[1:]
    half_width = width // n_tp
    per_core = n_fs // n_tp
    half_sp = n_sp // n_tp

    def lanes_at(index, size):
        return pl.ds(pl.multiple_of(index * size, LANES), size)

    barrier = pltpu.get_barrier_semaphore()
    sides = [{"fs": c_x}, {"fs": c_y}, {"tp": peer}]
    for partner in sides:
        pl.semaphore_signal(barrier, inc=1, device_id=partner, device_id_type=MESH)

    @pl.when(z > 0)
    def _():
        pl.semaphore_signal(barrier, inc=1, device_id={"sp": z - 1}, device_id_type=MESH)

    @pl.when(z < n_sp - 1)
    def _():
        pl.semaphore_signal(barrier, inc=1, device_id={"sp": z + 1}, device_id_type=MESH)

    loads = {}

    def load(name, slot, src, dst):
        copy = pltpu.make_async_copy(src, dst, load_sem.at[slot])
        copy.start()
        loads[name] = copy

    load("tok", 0, tokens, tok_v)
    load("ng", 1, norm_gain_in, norm_gain)
    load("wq", 2, query_down.at[:, lanes_at(c, q_cols)], w_q.at[z])
    load("wv", 3, glu_value.at[:, lanes_at(c, cols)], w_g.at[z, :, pl.ds(0, cols)])
    load("wt", 4, glu_gate.at[:, lanes_at(c, cols)], w_g.at[z, :, pl.ds(cols, cols)])
    load("lat", 5, latent_down, lat_v)
    load("rope", 6, rope_down, rope_v)
    load("tab", 7, tables.at[:, pl.ds(pl.multiple_of(z * rows, LANES), rows), :], tab_v)
    load("lg", 8, latent_gain_in, latent_gain)

    def load_rest():
        load("hp", 0, head_proj.at[:, lanes_at(c, out_cols)], w_o.at[z, pl.ds(0, head_rows), :])
        load("cp", 1, channel_proj.at[:, lanes_at(c, out_cols)], w_o.at[z, pl.ds(head_rows, out_rows - head_rows), :])
        load("qup", 2, query_up, qup_v)
        load("kup", 3, key_up, kup_v)
        load("vup", 4, value_up, vup_v)
        load("qg", 5, query_gain_in, query_gain)
        load("taps", 6, taps_in.at[:, lanes_at(c, cols)], conv_taps)
        load("gg", 7, group_gain_in, group_gain)
        load("hf", 8, head_proj, w_full.at[pl.ds(0, head_rows), :])
        load("cf", 9, channel_proj, w_full.at[pl.ds(head_rows, out_rows - head_rows), :])

    loads["tok"].wait()
    loads["ng"].wait()
    values = tok_v[...].astype(F32)
    normed[c] = rms_scale(values, row_of(norm_gain)).astype(BF16)
    for name in ("wq", "wv", "wt"):
        loads[name].wait()

    ends = (z == 0).astype(jnp.int32) + (z == n_sp - 1).astype(jnp.int32)
    pl.semaphore_wait(barrier, len(sides) + 2 - ends)

    sent = []

    def when(cond, action):
        if cond is None:
            action()
        else:
            pl.when(cond)(action)

    def both(first, second):
        return second if first is None else first & second

    def remote(src, dst, recv_sem, device):
        def make(send_sem):
            return pltpu.make_async_remote_copy(
                src_ref=src, dst_ref=dst, send_sem=send_sem, recv_sem=recv_sem,
                device_id=device, device_id_type=MESH,
            )

        return make

    def drain(entry):
        copy, cond = entry
        when(cond, copy.wait_send)

    def send(make, cond=None):
        slot = len(sent) % RING
        if len(sent) >= RING:
            drain(sent[-RING])
        copy = make(ring_sem.at[slot])
        when(cond, copy.start)
        sent.append((copy, cond))

    def arrive(make):
        make(ring_sem.at[0]).wait_recv()

    def arrive_all(like, recv_sem):
        arrive(remote(like, like, recv_sem, {"tp": peer}))

    q_half = depth // n_tp
    piece = depth // PIECES
    k_half = rows // n_tp
    inner = (z > 0) & (z < n_sp - 1)
    at_end = jnp.logical_not(inner)
    lower = 2 * z < n_sp
    outer = jnp.where(lower, 0, n_sp - 1)
    near = jnp.where(lower, 1, n_sp - 2)
    far = jnp.where(lower, n_sp - 2, 1)
    neighbour = jnp.where(lower, z + 1, z - 1)

    def half(first, size):
        return pl.ds(pl.multiple_of(first * size, 16), size)

    def block(u, shard, side=t):
        if u == Q:
            return w_q.at[shard, half(side, q_half), :]
        if u == K:
            return keys.at[shard, side]
        if u == H:
            return w_o.at[shard, pl.ds(0, head_rows), :]
        if u == C:
            return w_o.at[shard, pl.ds(head_rows, out_rows - head_rows), :]
        return w_g.at[shard, pl.ds((u - G) * piece, piece), :]

    def slot_of(shard, at):
        return shard - (shard > at).astype(jnp.int32)

    def z_copy(u, shard, target):
        ref = block(u, shard)
        return remote(ref, ref, z_recv.at[u, slot_of(shard, target)], {"sp": target})

    def z_arrive(u, shard):
        ref = block(u, shard)
        arrive(remote(ref, ref, z_recv.at[u, slot_of(shard, z)], {"sp": neighbour}))

    def send_own(u, cond=None):
        skip = 1 if u in (H, C) else 0
        send(z_copy(u, z, z - 1), both(cond, z > skip))
        send(z_copy(u, z, z + 1), both(cond, z < n_sp - 1 - skip))

    nearest = jnp.minimum(z, n_sp - 1 - z)
    arrivals = []
    for k in range(n_sp - 1):
        two_sided = k < 2 * nearest
        distance = jnp.where(two_sided, k // 2 + 1, k - nearest + 1)
        from_low = jnp.where(two_sided, 1 - k % 2, (2 * z > n_sp - 1).astype(jnp.int32))
        arrivals.append((z - distance * (2 * from_low - 1), z + 2 * from_low - 1))

    def pass_on(u, shard, target):
        when(inner, lambda: z_arrive(u, shard))
        send(z_copy(u, shard, target), inner)

    def relay(u, k):
        pass_on(u, *arrivals[k])

    def both_ways(u):
        pass_on(u, outer, far)
        pass_on(u, far, outer)

    def settle(u, k):
        when(at_end, lambda: z_arrive(u, arrivals[k][0]))

    def pair(u, shard, side):
        ref = block(u, shard, side)
        return remote(ref, ref, pair_recv.at[u], {"tp": peer})

    def share(u, k):
        settle(u, k)
        send(pair(u, arrivals[k][0], t))

    quarter_width = half_width // 2

    def n_block(owner, part):
        return normed.at[owner, :, lanes_at(2 * t + part, quarter_width)]

    def n_copy(i, part):
        ref = n_block(c, part)
        return remote(ref, ref, n_recv.at[i, part], {"fs": others[i]})

    def n_relay(i):
        ref = n_block(others[i], i)
        return remote(ref, ref, nr_recv.at[i], {"fs": others[1 - i]})

    def n_pair(i, side):
        ref = normed.at[others[i], :, lanes_at(side, half_width)]
        return remote(ref, ref, np_recv.at[0], {"tp": peer})

    def pass_normed(i):
        arrive(n_copy(i, i))
        send(n_relay(i))

    def share_normed(i):
        if i < 2:
            arrive(n_copy(i, 1 - i))
        else:
            for j in range(2):
                arrive(n_relay(j))
        send(n_pair(i, t))

    send_own(Q)
    for part in range(2):
        send(n_copy(0, part))
        send(n_copy(1, 1 - part))

    def rotate_lanes(v):
        step = ROPE // 2
        return (
            v * tab_v[0] + pltpu.roll(v, LANES - step, 1) * tab_v[1] + pltpu.roll(v, step, 1) * tab_v[2]
        )

    loads["lat"].wait()
    loads["lg"].wait()
    own_normed = normed[c]
    latent = rms_scale(dot(own_normed, lat_v[...]), row_of(latent_gain))
    keys[z, :, 0:k_half, :] = latent.astype(BF16).reshape(n_tp, k_half, KVR)
    loads["rope"].wait()
    loads["tab"].wait()
    key_tmp[...] = jnp.zeros_like(key_tmp)
    key_tmp[:, 0:ROPE] = dot_nt(own_normed, rope_v[...])
    rotated = rotate_lanes(key_tmp[...])
    fold = KVR // ROPE
    strip = k_half // fold
    for side in range(n_tp):
        for pair_of in range(fold // 2):
            first = side * k_half + 2 * pair_of * strip
            packed = rotated[first : first + strip, :] + pltpu.roll(
                rotated[first + strip : first + 2 * strip, :], ROPE, 1
            )
            keys[z, side, k_half : k_half + strip, pair_of * LANES : (pair_of + 1) * LANES] = packed.astype(BF16)
    send_own(K)
    send_own(G)
    send_own(G + 1)
    load_rest()

    last = n_sp - 2
    both_ways(Q)
    pass_normed(0)
    pass_normed(1)
    both_ways(K)
    share(Q, 0)
    send_own(G + 2)
    relay(Q, last)
    send_own(G + 3)
    both_ways(G)
    share_normed(0)
    share_normed(1)
    relay(K, last)
    both_ways(G + 1)
    for k in range(1, last):
        share(Q, k)
    share_normed(2)
    share(Q, last)
    for p in range(2, PIECES):
        both_ways(G + p)

    arrive_all(normed.at[pl.ds(0, n_fs - 1), :, lanes_at(peer, half_width)], np_recv.at[0])
    halo = low_rows.shape[1]
    edge_rows = pl.ds(pl.multiple_of(jnp.where(lower, rows - halo, 0), 16), halo)
    edge_half = edge_in.at[:, :, lanes_at(t, half_width)]
    edge_copy = remote(normed.at[:, edge_rows, lanes_at(t, half_width)], edge_half, edge_recv.at[0], {"sp": near})
    edge_pair = remote(edge_half, edge_half, edge_recv.at[1], {"tp": peer})
    arrive_all(w_q.at[pl.ds(0, n_sp - 1), half(peer, q_half), :], pair_recv.at[Q])
    seqs = normed[pl.ds(per_core * t, per_core)].reshape(per_core * rows, width)
    q_out[...] = dot(seqs, w_q[...].reshape(n_sp * depth, q_cols)).reshape(per_core, rows, q_cols)

    for i in range(per_core):
        seq = per_core * t + i
        for core in (peer, t):
            copy = remote(q_out.at[i], q_lat.at[c], q_recv.at[0], {"fs": seq, "tp": core})
            send(copy, None if core is peer else seq != c)

        @pl.when(seq == c)
        def _():
            q_lat[c] = q_out[i]

    for name in ("hp", "cp"):
        loads[name].wait()
    send_own(H, at_end)
    send(edge_copy, at_end)
    send_own(C, at_end)

    def add_shard(shard, first=False):
        rows_in = normed[:, :, lanes_at(shard, depth)].reshape(n_fs * rows, depth)
        term = dot(rows_in, w_g[shard])
        g_acc[...] = term if first else g_acc[...] + term

    up_copy = remote(
        gated.at[:, pl.ds(rows - halo, halo), :], low_rows, halo_recv.at[0], {"sp": z + 1}
    )(halo_send.at[0])
    down_copy = remote(
        gated.at[:, pl.ds(0, halo), :], high_rows, halo_recv.at[1], {"sp": z - 1}
    )(halo_send.at[1])

    def add_arrival(k):
        for p in range(PIECES):
            settle(G + p, k)
        add_shard(arrivals[k][0])

    def gate():
        gated[...] = gate_of(g_acc[...]).reshape(n_fs, rows, cols)

        @pl.when(inner)
        def _():
            up_copy.start()
            down_copy.start()

    def gate_of(acc):
        return (acc[:, 0:cols] * jax.nn.sigmoid(acc[:, cols : 2 * cols])).astype(BF16)

    def edge():
        arrive(edge_pair)
        acc = dot(edge_in[...].reshape(n_fs * halo, width), w_g[...].reshape(n_sp * depth, 2 * cols))
        values = gate_of(acc).astype(F32).reshape(n_fs, halo, cols)

        @pl.when(lower)
        def _():
            padded[:, 0:halo, :] = values

        @pl.when(jnp.logical_not(lower))
        def _():
            padded[:, halo + rows : 2 * halo + rows, :] = values

    for p in range(2):
        relay(G + p, last)
    for k in range(last):
        share(K, k)
    add_shard(z, True)
    for p in range(2, PIECES):
        relay(G + p, last)
    share(K, last)

    add_arrival(0)

    send_own(H, inner)

    @pl.when(inner)
    def _():
        for k in range(1, n_sp - 1):
            add_arrival(k)
        gate()

    send_own(C, inner)
    for name in ("qup", "kup", "vup", "qg", "taps", "gg"):
        loads[name].wait()

    here = t == c // per_core

    @pl.when(here)
    def _():
        arrive_all(q_lat.at[pl.ds(0, n_fs - 1)], q_recv.at[0])

    @pl.when(jnp.logical_not(here))
    def _():
        arrive_all(q_lat, q_recv.at[0])

    pass_on(H, outer, far)
    whole_q = jnp.concatenate([q_lat[i] for i in range(n_fs)], axis=1)
    latent_query = rms_scale(whole_q, row_of(query_gain)).astype(BF16)
    q_scr[...] = dot(latent_query, qup_v[...])
    arrive_all(keys.at[pl.ds(0, n_sp - 1), peer], pair_recv.at[K])

    key_lane = lax.broadcasted_iota(jnp.int32, (strip, LANES), 1)
    for shard in range(n_sp):
        for side in range(n_tp):
            for pair_of in range(fold // 2):
                packed = keys[
                    shard, side, k_half : k_half + strip, pair_of * LANES : (pair_of + 1) * LANES
                ].astype(F32)
                for part, values in enumerate((packed, pltpu.roll(packed, ROPE, 1))):
                    first = (shard * n_tp + side) * k_half + (2 * pair_of + part) * strip
                    rope_keys[first : first + strip, :] = jnp.where(key_lane < ROPE, values, 0.0).astype(BF16)

    def attend(h, shifted):
        start = h * (NOPE + ROPE)
        source = q_scr[...]
        if start % LANES:
            source, start = shifted, start - ROPE
        plain = source[:, start : start + NOPE].astype(BF16)
        rope_part = rotate_lanes(source[:, start + NOPE : start + NOPE + LANES]).astype(BF16)
        absorbed = dot_nt(plain, kup_v[:, h * NOPE : (h + 1) * NOPE]).astype(BF16)
        latents = keys[:, :, 0:k_half, :].reshape(n_sp * rows, KVR)
        scores = (dot_nt(absorbed, latents) + dot_nt(rope_part, rope_keys[...])) * (NOPE + ROPE) ** (-0.5)
        row_max = jnp.max(scores, axis=1, keepdims=True)
        weights = jnp.exp(scores - row_max)
        total = jnp.sum(weights, axis=1, keepdims=True)
        added = dot(weights.astype(BF16), latents)
        attended = (added / total).astype(BF16)
        head_out = dot(attended, vup_v[:, h * VDIM : (h + 1) * VDIM])
        mixed[c, :, h * VDIM : (h + 1) * VDIM] = head_out.astype(BF16)
        return row_max + jnp.log(total)

    def head_ref(owner, h):
        return mixed.at[owner, :, pl.ds(2 * h * VDIM, 2 * VDIM)]

    def head_copy(h, i):
        ref = head_ref(c, h)
        return remote(ref, ref, head_recv.at[h if h == i else 2], {"fs": others[i]})

    def head_relay(h):
        ref = head_ref(others[h], h)
        return remote(ref, ref, head_recv.at[2], {"fs": others[1 - h]})

    def pass_head(h, cond):
        when(cond, lambda: arrive(head_copy(h, h)))
        send(head_relay(h), cond)

    whole = q_scr[...]
    shifted = pltpu.roll(whole, whole.shape[1] - ROPE, 1)
    lane = lax.broadcasted_iota(jnp.int32, (rows, LANES), 1)
    logs = jnp.zeros((rows, LANES), F32)

    def to_near(group):
        lanes = lanes_at(group, cols) if isinstance(group, jax.Array) or group >= heads else pl.ds(2 * group * cols, 2 * cols)
        return remote(mixed.at[c, :, lanes], mixed_o.at[:, lanes], up_recv.at[0], {"sp": near})

    for h in range(heads):
        logs = jnp.where(lane == h, attend(h, shifted), logs)
        if h % 2:
            for i in range(2):
                send(head_copy(h // 2, i))
            send(to_near(h // 2), at_end)
        if h == 1:
            when(inner, lambda: arrive(edge_copy))
            send(edge_pair, inner)
    log_v[...] = jnp.transpose(logs)[0:heads, :]
    log_copy = pltpu.make_async_copy(log_v, log_out, out_sem.at[0])
    log_copy.start()
    pass_on(H, far, outer)

    @pl.when(at_end)
    def _():
        for k in range(1, last):
            add_arrival(k)


    @pl.when(at_end)
    def _():
        add_arrival(last)
        gate()

    @pl.when(inner)
    def _():
        edge()

    reach = conv_taps.shape[0] // 2
    padded[:, halo : halo + rows, :] = gated[...].astype(F32)

    @pl.when(z > 1)
    def _():
        up_copy.wait_recv()
        padded[:, 0:halo, :] = low_rows[...].astype(F32)

    @pl.when(z == 0)
    def _():
        padded[:, 0:halo, :] = jnp.zeros((n_fs, halo, cols), F32)

    @pl.when(z < n_sp - 2)
    def _():
        down_copy.wait_recv()
        padded[:, halo + rows : 2 * halo + rows, :] = high_rows[...].astype(F32)

    @pl.when(z == n_sp - 1)
    def _():
        padded[:, halo + rows : 2 * halo + rows, :] = jnp.zeros((n_fs, halo, cols), F32)

    def conv_ref(s, group):
        return mixed.at[s, :, pl.ds(pl.multiple_of(head_rows + group * cols, LANES), cols)]

    def conv_copy(s, i, slot=4):
        ref = conv_ref(s, c)
        return remote(ref, ref, conv_recv.at[slot], {"fs": others[i]})

    def conv_corner():
        ref = conv_ref(c_d, c)
        return remote(ref, ref, corner_recv.at[0], {"fs": c_d})

    def conv_corner_in():
        ref = conv_ref(c, c_d)
        return remote(ref, ref, corner_recv.at[0], {"fs": c_d})

    def conv_relay(s, i):
        ref = conv_ref(s, others[i])
        return remote(ref, ref, conv_recv.at[4], {"fs": others[1 - i]})

    taps = conv_taps[...].astype(F32)
    all_gains = row_of(group_gain).astype(F32)
    gains = all_gains[:, 0:cols]
    for i in range(1, n_fs):
        gains = jnp.where(c == i, all_gains[:, i * cols : (i + 1) * cols], gains)
    def conv_seq(s):
        filtered = jnp.zeros((rows, cols), F32)
        for j in range(conv_taps.shape[0]):
            first = halo - reach + j
            filtered = filtered + padded[s, first : first + rows, :] * taps[j : j + 1, :]
        centred = filtered - jnp.mean(filtered, axis=1, keepdims=True)
        spread = jnp.mean(centred * centred, axis=1, keepdims=True)
        branch = centred * lax.rsqrt(spread + norm_eps) * gains
        branch = branch * jax.nn.sigmoid(branch)
        mixed[s, :, pl.ds(pl.multiple_of(head_rows + c * cols, LANES), cols)] = branch.astype(BF16)

    conv_seq(c_d)
    send(conv_corner())
    conv_seq(c_x)
    send(conv_copy(c_x, 0, 0))
    conv_seq(c_y)
    send(conv_copy(c_y, 1, 2))
    conv_seq(c)
    send(to_near(heads + c), at_end)
    for s, i, slot in ((c, 0, 1), (c_d, 1, 4), (c_y, 0, 4), (c, 1, 4), (c_d, 0, 4), (c_x, 1, 3)):
        send(conv_copy(s, i, slot))
    pass_on(C, far, outer)
    pass_on(C, outer, far)
    for h in range(2):
        pass_head(h, None)
    relay(H, last)
    arrive(conv_copy(c, 0, 0))
    send(to_near(heads + c_x), at_end)
    arrive(conv_copy(c, 1, 2))
    send(to_near(heads + c_y), at_end)
    send(conv_relay(c, 1))
    arrive(conv_corner_in())
    send(to_near(heads + c_d), at_end)
    for s, i, slot in ((c_x, 0, 1), (c_d, 1, 3)):
        arrive(conv_copy(s, i, slot))
        send(conv_relay(s, i))
    relay(C, last)
    arrive_all(parts.at[pl.ds(0, 2)], head_recv.at[2])

    def head_part(shard):
        head_acc[shard] = dot(mixed[:, :, 0:head_rows].reshape(n_fs * rows, head_rows), w_o[shard, 0:head_rows, :])

    head_part(z)
    settle(H, 1)
    head_part(arrivals[1][0])

    @pl.when(inner)
    def _():
        head_part(arrivals[0][0])
        for k in range(2, n_sp - 1):
            head_part(arrivals[k][0])

    rest = (2 * n_fs - 1) * rows
    arrive_all(w_o.at[0, pl.ds(0, rest), :], conv_recv.at[4])

    def place(core, shard):
        first = (shard % half_sp) * (n_fs * out_cols) + c * out_cols
        return placed.at[core, :, pl.ds(pl.multiple_of(first, LANES), out_cols)]

    def fin_copy(shard, j):
        seq = others[j] if j < len(others) else c
        return remote(
            parts.at[shard, pl.ds(pl.multiple_of(seq * rows, LANES), rows), :], place(t, shard),
            fin_recv.at[t, shard % half_sp], {"fs": seq, "tp": shard // half_sp},
        )

    def keep_copy(shard):
        ref = parts.at[shard, pl.ds(pl.multiple_of(c * rows, LANES), rows), :]
        return pltpu.make_async_copy(ref, place(t, shard), out_sem.at[1 + shard % half_sp])

    def add_part(shard, cond=None):
        def compute():
            part = head_acc[shard] + dot(
                mixed[:, :, head_rows:out_rows].reshape(n_fs * rows, out_rows - head_rows), w_o[shard, head_rows:out_rows, :]
            )
            parts[shard] = part.astype(BF16)

        when(cond, compute)
        for j in (2, 0, 1):
            send(fin_copy(shard, j), cond)
        mine = shard // half_sp == t
        send(fin_copy(shard, len(others)), both(cond, jnp.logical_not(mine)))
        when(both(cond, mine), lambda: keep_copy(shard).start())

    add_part(z)
    add_part(arrivals[0][0], inner)
    settle(C, 1)
    add_part(arrivals[1][0])
    for k in range(2, n_sp - 1):
        settle(H, k)

        @pl.when(at_end)
        def _():
            head_part(arrivals[k][0])

        settle(C, k)
        add_part(arrivals[k][0])

    back_lanes = lanes_at(z % half_sp, n_fs * out_cols)
    back_copy = remote(
        part_o, placed.at[t, :, back_lanes], back_recv.at[0], {"sp": outer, "tp": z // half_sp}
    )(back_send.at[0])
    for name in ("hf", "cf"):
        loads[name].wait()

    def neighbour_part():
        arrive_all(mixed_o, up_recv.at[0])
        part_o[...] = dot(mixed_o[...], w_full[...]).astype(BF16)
        back_copy.start()

    @pl.when(inner)
    def _():
        neighbour_part()

    for entry in sent[-RING:]:
        drain(entry)

    @pl.when(inner)
    def _():
        up_copy.wait_send()
        down_copy.wait_send()
        back_copy.wait_send()

    for i in range(half_sp):
        shard = t * half_sp + i
        computed = inner | (shard != near)

        @pl.when(computed)
        def _():
            arrive_all(parts.at[0, pl.ds(0, (n_fs - 1) * rows), :], fin_recv.at[t, i])
            arrive_all(parts.at[0], fin_recv.at[peer, i])
            keep_copy(shard).wait()

        @pl.when(jnp.logical_not(computed))
        def _():
            arrive_all(parts.at[pl.ds(0, n_tp)], back_recv.at[0])
    log_copy.wait()


def finish_kernel(placed, log_in, out, log_out, held, summed, log_v, load_sem, store_sem):
    span = out.shape[1] // 2
    logs = pltpu.make_async_copy(log_in, log_v, load_sem.at[2])
    loads = [
        pltpu.make_async_copy(placed.at[:, :, pl.ds(i * span, span)], held.at[i], load_sem.at[i]) for i in range(2)
    ]
    for copy in loads:
        copy.start()
    logs.start()
    stores = [
        pltpu.make_async_copy(summed.at[i], out.at[:, pl.ds(i * span, span)], store_sem.at[i]) for i in range(2)
    ]
    for i in range(2):
        loads[i].wait()
        summed[i] = (held[i, 0].astype(F32) + held[i, 1].astype(F32)).astype(BF16)
        stores[i].start()
    logs.wait()
    stores.append(pltpu.make_async_copy(log_v, log_out, store_sem.at[2]))
    stores[2].start()
    for copy in stores:
        copy.wait()


def fused_device(n_sp, n_fs, *args):
    (tokens, norm_gain, query_down, query_gain, latent_down, latent_gain, rope_down, query_up,
     key_up, value_up, glu_value, glu_gate, conv_taps, group_gain, head_proj, channel_proj) = args
    rows, width = tokens.shape
    depth, q_rank = query_down.shape
    cols = glu_value.shape[1] // n_fs
    heads = key_up.shape[1] // NOPE
    out_rows = head_proj.shape[0] + channel_proj.shape[0]
    out_cols = head_proj.shape[1] // n_fs
    q_cols = q_rank // n_fs
    halo = (conv_taps.shape[0] // 2 + 15) // 16 * 16
    tables = jnp.asarray(rope_tables(n_sp * rows))
    hbm = pl.BlockSpec(memory_space=pltpu.HBM)
    operands = [
        tokens, norm_gain, query_down, query_gain, latent_down, latent_gain, rope_down.T, query_up,
        key_up, value_up, glu_value, glu_gate, conv_taps, group_gain, head_proj, channel_proj, tables,
    ]
    like = lambda a: pltpu.VMEM(a.shape, a.dtype)
    dma = pltpu.SemaphoreType.DMA
    half_sp = n_sp // 2
    scratch = [
        like(norm_gain), like(query_gain), like(latent_gain), pltpu.VMEM((conv_taps.shape[0], cols), BF16), like(group_gain),
        pltpu.VMEM((heads, rows), F32),
        pltpu.VMEM((n_sp, depth, q_cols), BF16),
        pltpu.VMEM((n_sp, depth, 2 * cols), BF16),
        pltpu.VMEM((n_sp, out_rows, out_cols), BF16),
        like(tokens), like(latent_down), pltpu.VMEM(rope_down.shape[::-1], BF16), like(query_up), like(key_up), like(value_up),
        pltpu.VMEM((3, rows, LANES), F32),
        pltpu.VMEM((n_fs, rows, width), BF16),
        pltpu.VMEM((n_sp, 2, rows // 2 + rows // 2 * ROPE // KVR, KVR), BF16),
        pltpu.VMEM((n_sp * rows, LANES), BF16),
        pltpu.VMEM((rows, LANES), F32),
        pltpu.VMEM((n_fs // 2, rows, q_cols), F32),
        pltpu.VMEM((n_fs, rows, q_cols), F32),
        pltpu.VMEM((rows, query_up.shape[1]), F32),
        pltpu.VMEM((n_fs * rows, 2 * cols), F32),
        pltpu.VMEM((n_fs, rows, cols), BF16),
        pltpu.VMEM((n_fs, halo, cols), BF16),
        pltpu.VMEM((n_fs, halo, cols), BF16),
        pltpu.VMEM((n_fs, rows + 2 * halo, cols), F32),
        pltpu.VMEM((n_fs, rows, out_rows), BF16),
        pltpu.VMEM((n_sp, n_fs * rows, out_cols), BF16),
        pltpu.VMEM((out_rows, n_fs * out_cols), BF16),
        pltpu.VMEM((rows, out_rows), BF16),
        pltpu.VMEM((rows, n_fs * out_cols), BF16),
        pltpu.VMEM((n_fs, halo, width), BF16),
        pltpu.VMEM((n_sp, n_fs * rows, out_cols), F32),
        dma((10,)), dma((RING,)), dma((G + PIECES, n_sp - 1)), dma((2,)), dma((2, 2)), dma((1,)), dma((1,)),
        dma((3,)), dma((2,)), dma((2,)), dma((5,)), dma((2, half_sp)), dma((1 + half_sp,)),
        dma((1,)), dma((1,)), dma((1,)), dma((2,)), dma((1,)), dma((2,)),
    ]
    shapes = (
        jax.ShapeDtypeStruct((rows, half_sp * n_fs * out_cols), BF16),
        jax.ShapeDtypeStruct((heads, rows), F32),
    )
    placed, logs = pl.pallas_call(
        functools.partial(fused_kernel, n_sp),
        out_shape=(jax.ShapeDtypeStruct((2,) + shapes[0].shape, BF16), shapes[1]),
        in_specs=[hbm] * len(operands),
        out_specs=(hbm, hbm),
        scratch_shapes=scratch,
        compiler_params=pltpu.CompilerParams(
            collective_id=0, has_side_effects=True, vmem_limit_bytes=63 * 1024 * 1024
        ),
        name="fused_layer",
    )(*operands)
    span = shapes[0].shape[1] // 2
    return pl.pallas_call(
        finish_kernel,
        out_shape=shapes,
        in_specs=[hbm] * 2,
        out_specs=(hbm, hbm),
        scratch_shapes=[
            pltpu.VMEM((2, 2, rows, span), BF16), pltpu.VMEM((2, rows, span), BF16), pltpu.VMEM((heads, rows), F32),
            dma((3,)), dma((3,)),
        ],
        name="finish",
    )(placed, logs)


def solution(mesh):
    in_specs = (
        P(("fs", "sp"), None),
        P(),
        P("sp", None),
        P(),
        P(),
        P(),
        P(),
        P(None, "tp"),
        P(None, "tp"),
        P(None, "tp"),
        P("sp", "tp"),
        P("sp", "tp"),
        P(None, "tp"),
        P("tp"),
        P("tp", "sp"),
        P("tp", "sp"),
    )
    out_specs = (P(("fs", "sp"), "tp"), P("tp", ("fs", "sp")))
    body = per_device
    if mesh.shape["fs"] == 4 and mesh.shape["tp"] == 2 and mesh.shape["sp"] == 4:
        body = functools.partial(fused_device, mesh.shape["sp"], mesh.shape["fs"])
    return jax.shard_map(
        body, mesh=mesh, in_specs=in_specs, out_specs=out_specs, check_vma=False
    )
```
